32 devices in a mesh: ep: 8 (over z, x), tp: 4 (over y, core).
Axes of the slice: x: 2, y: 2, z: 4, core: 2. Of those that a mesh axis runs over, the one named last changes fastest.
Arguments:
- queries: bfloat16 [2048, 4096], P('ep', 'tp'), may hold values from -6 to 6
- key_rows: bfloat16 [2048, 4096], P('ep', 'tp'), may hold values from -6 to 6
- value_rows: bfloat16 [2048, 4096], P('ep', 'tp'), may hold values from -6 to 6
- lambdas: float32 [16], P('tp'), may hold values from 0.3 to 0.8
- head_gain: float32 [256], replicated, may hold values from 0.1 to 1.9
- out_proj: bfloat16 [4096, 2048], P('tp'), may hold values from -0.09375 to 0.09375
- moe_input: bfloat16 [1024, 2048], P('ep'), may hold values from -6 to 6
- moe_gain: float32 [2048], replicated, may hold values from 0.1 to 1.9
- routes: int32 [1024, 2], P('ep'), may hold values from 0 to 7, all different within a row; in each aligned block of 32 rows (0 to 31, 32 to 63, ...) at most 16 rows name the same one
- route_weights: float32 [1024, 2], P('ep'), may hold values from 0.2 to 1.2
- expert_gate: bfloat16 [8, 2048, 1024], P('ep', None, 'tp'), may hold values from -0.125 to 0.125
- expert_up: bfloat16 [8, 2048, 1024], P('ep', None, 'tp'), may hold values from -0.125 to 0.125
- expert_down: bfloat16 [8, 1024, 2048], P('ep', 'tp'), may hold values from -0.1875 to 0.1875
- shared_gate: bfloat16 [2048, 1024], P(None, 'tp'), may hold values from -0.125 to 0.125
- shared_up: bfloat16 [2048, 1024], P(None, 'tp'), may hold values from -0.125 to 0.125
- shared_down: bfloat16 [1024, 2048], P('tp'), may hold values from -0.1875 to 0.1875
Outputs:
- mixer_out: bfloat16 [2048, 2048], P(('ep', 'tp'))
- moe_out: bfloat16 [1024, 2048], P(('ep', 'tp'))
The draws below stay inside these ranges and needn't reach their ends.
Inputs may be any that keep to these rules, and one draw needn't show every extreme that they name: `routes`: each row names 2 different experts. The rows of one index of ep fall into 4 aligned blocks of equal size; no expert is named by more than 16 rows of one block, and in every draw some expert is named by exactly 16 rows of some block.
All inputs are finite; a program needn't handle non-finite values.
Results may differ from the reference program's by a relative error of at most 0.02.
Values may be sent and summed in bfloat16 or wider, within the bound.
A program may use at most 128 MiB of HBM per device.

```python
import math
import jax
import jax.numpy as jnp
import numpy as np
from jax import lax

D = 2048
HEADS = 16
HEAD_DIM = 128
DE = 1024
TOP = 2
TOK2_DEV = 128
TOKENS1 = 2048
TOKENS2 = 1024
EXPERTS = 8
CAP = 16
N_EP = 8
N_TP = 4


def draw_common(key, salt):
    own_key = jax.random.fold_in(key, salt)
    base = jax.random.normal(own_key, (TOKENS1, HEADS * 2 * HEAD_DIM), jnp.float32) * 1.3
    return jnp.clip(base, -6.0, 6.0).astype(jnp.bfloat16)


def draw_queries(key, part):
    return draw_common(key, 11)


def draw_key_rows(key, part):
    return draw_common(key, 12)


def block_levels(rng, shape, pieces, smallest, high):
    def one(axis_at, shards_of):
        steps = jax.random.uniform(jax.random.fold_in(jax.random.fold_in(rng, 6), axis_at), (shards_of,), jnp.float32, smallest / len(pieces), high / len(pieces))
        return jnp.repeat(jnp.exp(steps), shape[axis_at] // shards_of).reshape((-1,) + (1,) * (len(shape) - axis_at - 1))

    level = one(*pieces[0])
    for cut in pieces[1:]:
        level = level * one(*cut)
    return level


def assign_block(rng, own, number, rows, number_of, top, most, skew):
    order = jax.random.permutation(rng, number_of)
    crowded, ordinary = load_shares(number_of, rows * top, most, skew, True), load_shares(number_of, rows * top, most, skew, False)
    places = jnp.arange(number_of)

    def named(sizes, turn):
        used = int((sizes > 0).sum())
        fixed = max(1, used // 4)
        passed = fixed + (places - fixed + turn * (used - fixed)) % max(1, number_of - fixed)
        return jnp.zeros((number_of,), jnp.int32).at[order[jnp.where(places < fixed, places, passed)]].set(jnp.asarray(sizes, jnp.int32))

    sizes = jnp.where(number % 4 == 0, named(crowded, number // 4), named(ordinary, number - number // 4 - 1))
    mixed = jax.random.permutation(jax.random.fold_in(own, 3), number_of)
    giver, receiver = mixed[0:number_of // 2 * 2:2], mixed[1:number_of // 2 * 2:2]
    room = jnp.minimum(sizes[giver] - 1, most - sizes[receiver]) // 2
    room = jnp.where((giver == order[0]) | (receiver == order[0]) | (sizes[receiver] == 0), 0, jnp.maximum(room, 0))
    passed = jax.random.randint(jax.random.fold_in(own, 4), (number_of // 2,), 0, 1 << 20) % (room + 1)
    sizes = sizes.at[giver].add(-passed).at[receiver].add(passed)
    labels = jnp.searchsorted(jnp.cumsum(sizes), jnp.arange(rows * top), side="right").astype(jnp.int32)
    listing = labels.reshape(top, rows).T
    listing = listing[jax.random.permutation(jax.random.fold_in(own, 1), rows)]
    turn = jax.random.randint(jax.random.fold_in(own, 2), (rows, 1), 0, top)
    return jnp.take_along_axis(listing, (jnp.arange(top)[None, :] + turn) % top, axis=1)


def load_shares(amount, total, limit, slope, full):
    weights = [(1 << 20) // math.isqrt(standing ** slope) + 1 for standing in range(1, amount + 1)]
    largest = limit if full else min(limit, max(-(-total // amount), total * weights[0] // sum(weights)))
    least = 1 if total - largest >= amount - 1 else 0
    holding, spare = [largest] + [least] * (amount - 1), total - largest - least * (amount - 1)
    while spare > 0:
        movable = [i for i in range(1, amount) if holding[i] < largest] or [i for i in range(1, amount) if holding[i] < limit]
        mass, budget = sum([weights[i] for i in movable]), spare
        for i in movable:
            addition = min(limit - holding[i], max(1, budget * weights[i] // mass), spare)
            holding[i] = holding[i] + addition
            spare = spare - addition
    return np.array(holding)


def normal_values(key, dims, scale, reach, shards=(), held_as=jnp.bfloat16):
    result = jax.random.normal(key, dims, jnp.float32) * scale
    if len(shards) > 0:
        result = block_levels(key, dims, shards, -0.22, 0.18) * result
    return jnp.clip(result, min=-reach, max=reach).astype(held_as)


def setup_inputs(seed: int = 0) -> dict:
    splits = jax.random.split(jax.random.key(seed), 17)
    queries = draw_queries(jax.random.fold_in(splits[16], 71), 0)
    key_rows = draw_key_rows(jax.random.fold_in(splits[16], 71), 0)
    value_rows = normal_values(splits[2], (TOKENS1, HEADS * 2 * HEAD_DIM), 1.0, 6.0, ((0, 8), (1, 4)))
    lambdas = jnp.clip(0.3 + 0.5 * jax.random.uniform(splits[3], (HEADS,), jnp.float32) ** block_levels(splits[3], (HEADS,), ((0, 4),), -0.2, 0.2), 0.3, 0.8)
    head_gain = jnp.clip(1.0 + 0.18 * jax.random.normal(splits[4], (2 * HEAD_DIM,), jnp.float32), 0.1, 1.9)
    out_proj = normal_values(splits[5], (HEADS * 2 * HEAD_DIM, D), (HEADS * 2 * HEAD_DIM) ** -0.5, 0.09375, ((0, 4),))
    moe_input = normal_values(splits[6], (TOKENS2, D), 1.0, 6.0, ((0, 8),))
    moe_gain = jnp.clip(1.0 + 0.18 * jax.random.normal(splits[7], (D,), jnp.float32), 0.1, 1.9)
    routes_keys = jax.random.split(jax.random.fold_in(splits[8], 1), TOKENS2 // (TOK2_DEV // N_TP))
    routes_turns = jax.random.permutation(jax.random.fold_in(splits[8], 3), TOKENS2 // (TOK2_DEV // N_TP))
    routes = jax.vmap(lambda own, number: assign_block(jax.random.fold_in(splits[8], 2), own, number, TOK2_DEV // N_TP, EXPERTS, TOP, CAP, 2))(routes_keys, routes_turns).reshape((TOKENS2, TOP))
    route_weights = jnp.clip(0.2 + 1 * jax.random.uniform(splits[9], (TOKENS2, TOP), jnp.float32) ** block_levels(splits[9], (TOKENS2, TOP), ((0, 8),), -0.2, 0.2), 0.2, 1.2)
    expert_gate = normal_values(splits[10], (EXPERTS, D, DE), D ** -0.5, 0.125, ((0, 8), (2, 4)))
    expert_up = normal_values(splits[11], (EXPERTS, D, DE), D ** -0.5, 0.125, ((0, 8), (2, 4)))
    expert_down = normal_values(splits[12], (EXPERTS, DE, D), DE ** -0.5, 0.1875, ((0, 8), (1, 4)))
    shared_gate = normal_values(splits[13], (D, DE), D ** -0.5, 0.125, ((1, 4),))
    shared_up = normal_values(splits[14], (D, DE), D ** -0.5, 0.125, ((1, 4),))
    shared_down = normal_values(splits[15], (DE, D), DE ** -0.5, 0.1875, ((0, 4),))
    return dict(queries=queries, key_rows=key_rows, value_rows=value_rows, lambdas=lambdas, head_gain=head_gain, out_proj=out_proj, moe_input=moe_input, moe_gain=moe_gain, routes=routes, route_weights=route_weights, expert_gate=expert_gate, expert_up=expert_up, expert_down=expert_down, shared_gate=shared_gate, shared_up=shared_up, shared_down=shared_down)


theta_base = 500000.0
norm_eps = 1e-06
head_eps = 1e-05

def rotate(matrix, positions, head_dim):
    row_count = matrix.shape[0]
    shaped = matrix.reshape(row_count, -1, head_dim).astype(jnp.float32)
    half_dim = head_dim // 2
    frequency = jnp.power(theta_base, -jnp.arange(half_dim, dtype=jnp.float32) * 2.0 / head_dim)
    angles = positions.astype(jnp.float32)[:, None] * frequency[None, :]
    cosine = jnp.cos(angles)[:, None, :]
    sines = jnp.sin(angles)[:, None, :]
    front_half = shaped[..., :half_dim]
    second = shaped[..., half_dim:]
    turned = jnp.concatenate([front_half * cosine - second * sines, second * cosine + front_half * sines], axis=-1)
    return turned.reshape(matrix.shape).astype(jnp.bfloat16)

def rms_rows(values, gain):
    widened = values.astype(jnp.float32)
    mean_square = lax.optimization_barrier(jnp.mean(widened * widened, axis=-1, keepdims=True))
    return (widened * lax.rsqrt(mean_square + norm_eps) * gain).astype(jnp.bfloat16)

def gated_hidden(rows_in, gate_weight, up_weight):
    gate_part = jnp.dot(rows_in, gate_weight, preferred_element_type=jnp.float32)
    up_part = jnp.dot(rows_in, up_weight, preferred_element_type=jnp.float32)
    return (jax.nn.silu(gate_part) * up_part).astype(jnp.bfloat16)

def grouped_sum(rows_in, weight, groups):
    width = rows_in.shape[1] // groups
    groups_in = jnp.transpose(rows_in.reshape(rows_in.shape[0], groups, width), (1, 0, 2))
    groups_weight = weight.reshape(groups, width, weight.shape[1])

    def add_group(running, operands):
        partial_value = jnp.dot(operands[0], operands[1], preferred_element_type=jnp.float32)
        return (running + lax.optimization_barrier(partial_value.astype(jnp.bfloat16)).astype(jnp.float32), None)
    initial = jnp.zeros((rows_in.shape[0], weight.shape[1]), jnp.float32)
    running, _ = lax.scan(add_group, initial, (groups_in, groups_weight))
    return running

def reference(queries, key_rows, value_rows, lambdas, head_gain, out_proj, moe_input, moe_gain, routes, route_weights, expert_gate, expert_up, expert_down, shared_gate, shared_up, shared_down):
    head_dim = HEAD_DIM
    seq_total = queries.shape[0]
    positions = jnp.arange(seq_total, dtype=jnp.int32)
    rot_query = rotate(queries, positions, head_dim)
    rot_keys = rotate(key_rows, positions, head_dim)
    query_heads = jnp.transpose(rot_query.reshape(seq_total, HEADS, 2, head_dim), (1, 0, 2, 3))
    key_heads = jnp.transpose(rot_keys.reshape(seq_total, HEADS, 2, head_dim), (1, 0, 2, 3))
    value_heads = jnp.transpose(value_rows.reshape(seq_total, HEADS, 2 * head_dim), (1, 0, 2))
    block_rows = 512 if seq_total % 512 == 0 else seq_total

    def one_head(operands):
        head_query, head_keys, head_values, head_lambda = operands
        keys_wide = head_keys.astype(jnp.float32)
        values_wide = head_values.astype(jnp.float32)

        def one_block(block_query):
            scores = jnp.einsum('qmd,kmd->mqk', block_query.astype(jnp.float32), keys_wide) * head_dim ** (-0.5)
            shifted = jnp.exp(scores - lax.optimization_barrier(jnp.max(scores, axis=-1, keepdims=True)))
            denominator = lax.optimization_barrier(jnp.sum(shifted, axis=-1))
            rounded = lax.optimization_barrier(shifted.astype(jnp.bfloat16)).astype(jnp.float32)
            weighted = jnp.einsum('mqk,ke->mqe', rounded, values_wide)
            ratio = weighted / denominator[..., None]
            mixed_heads = ratio[0] - head_lambda * ratio[1]
            mean_square = lax.optimization_barrier(jnp.mean(mixed_heads * mixed_heads, axis=-1, keepdims=True))
            return (mixed_heads * lax.rsqrt(mean_square + head_eps) * head_gain).astype(jnp.bfloat16)
        blocks_out = lax.map(one_block, head_query.reshape(-1, block_rows, 2, head_dim))
        return blocks_out.reshape(seq_total, 2 * head_dim)
    head_out = lax.map(one_head, (query_heads, key_heads, value_heads, lambdas))
    head_out = jnp.transpose(head_out, (1, 0, 2)).reshape(seq_total, HEADS * 2 * head_dim)
    mixer_out = grouped_sum(head_out, out_proj, N_TP).astype(jnp.bfloat16)
    normed = rms_rows(moe_input, moe_gain)
    shared_hidden = gated_hidden(normed, shared_gate, shared_up)
    shared_sum = grouped_sum(shared_hidden, shared_down, N_TP)
    flat_experts = routes.reshape(-1).astype(jnp.int32)
    route_total = flat_experts.shape[0]
    sorted_order = jnp.argsort(flat_experts, stable=True).astype(jnp.int32)
    counts = lax.optimization_barrier(jnp.sum((flat_experts[:, None] == jnp.arange(EXPERTS, dtype=jnp.int32)[None, :]).astype(jnp.int32), axis=0))
    starts = jnp.cumsum(counts) - counts
    sorted_experts = flat_experts[sorted_order]
    slot_place = jnp.zeros((route_total,), jnp.int32).at[sorted_order].set(jnp.arange(route_total, dtype=jnp.int32) - starts[sorted_experts])
    load_bound = N_EP * N_TP * CAP
    table_index = jnp.clip(starts[:, None] + jnp.arange(load_bound, dtype=jnp.int32)[None, :], 0, route_total - 1)
    table_route = sorted_order[table_index]

    def one_expert(operands):
        gate_weight, up_weight, down_weight, route_ids = operands
        rows_in = normed[route_ids // TOP]
        hidden = gated_hidden(rows_in, gate_weight, up_weight)
        return grouped_sum(hidden, down_weight, N_TP).astype(jnp.bfloat16)
    expert_rows = lax.map(one_expert, (expert_gate, expert_up, expert_down, table_route))
    picked = expert_rows[flat_experts, slot_place].reshape(routes.shape[0], TOP, D)
    combined = shared_sum + lax.optimization_barrier(jnp.sum(route_weights[..., None] * picked.astype(jnp.float32), axis=1))
    return (mixer_out, combined.astype(jnp.bfloat16))
```

```python
import functools
import jax
import jax.numpy as jnp
from jax import lax
from jax.experimental import pallas as pl
from jax.experimental.pallas import tpu as pltpu
from jax.sharding import PartitionSpec as P

theta_base = 500000.0
norm_eps = 1e-06
head_eps = 1e-05
MESH = pl.DeviceIdType.MESH
log2_e = 1.4426950408889634


def rotate(matrix, positions, head_dim):
    row_count = matrix.shape[0]
    shaped = matrix.reshape(row_count, -1, head_dim).astype(jnp.float32)
    half_dim = head_dim // 2
    frequency = jnp.power(theta_base, -jnp.arange(half_dim, dtype=jnp.float32) * 2.0 / head_dim)
    angles = positions.astype(jnp.float32)[:, None] * frequency[None, :]
    cosine = jnp.cos(angles)[:, None, :]
    sines = jnp.sin(angles)[:, None, :]
    front_half = shaped[..., :half_dim]
    second = shaped[..., half_dim:]
    turned = jnp.concatenate(
        [front_half * cosine - second * sines, second * cosine + front_half * sines], axis=-1
    )
    return turned.reshape(matrix.shape).astype(jnp.bfloat16)


def rms_rows(values, gain):
    widened = values.astype(jnp.float32)
    mean_square = jnp.mean(widened * widened, axis=-1, keepdims=True)
    return (widened * lax.rsqrt(mean_square + norm_eps) * gain).astype(jnp.bfloat16)


def gated_hidden(rows_in, gate_weight, up_weight):
    gate_part = jnp.dot(rows_in, gate_weight, preferred_element_type=jnp.float32)
    up_part = jnp.dot(rows_in, up_weight, preferred_element_type=jnp.float32)
    return (jax.nn.silu(gate_part) * up_part).astype(jnp.bfloat16)


def slot_hidden(slot_rows, gate_weight, up_weight):
    gate_part = jnp.einsum(
        "xnsd,xdf->xnsf", slot_rows, gate_weight, preferred_element_type=jnp.float32
    )
    up_part = jnp.einsum("xnsd,xdf->xnsf", slot_rows, up_weight, preferred_element_type=jnp.float32)
    return (jax.nn.silu(gate_part) * up_part).astype(jnp.bfloat16)


def key_block_size(piece_rows):
    for candidate in (1024, 512):
        return candidate
    return piece_rows


def fold_keys(state_in, pieces, rot_query, head_count, head_dim):
    keys_piece, values_piece = pieces
    piece_rows = keys_piece.shape[0]
    block_rows = key_block_size(piece_rows)
    block_count = piece_rows // block_rows
    query_view = rot_query.reshape(rot_query.shape[0], head_count, 2, head_dim)
    score_scale = head_dim ** (-0.5)

    def one_block(running, key_block):
        running_max, denominator, numerator = running
        key_view = key_block[0].reshape(block_rows, head_count, 2, head_dim)
        value_view = key_block[1].reshape(block_rows, head_count, 2 * head_dim)
        scores = (
            jnp.einsum("qhmd,khmd->hmqk", query_view, key_view, preferred_element_type=jnp.float32)
            * score_scale
        )
        newest = jnp.maximum(running_max, jnp.max(scores, axis=-1))
        weights = jnp.exp(scores - newest[..., None])
        shrink = jnp.exp(running_max - newest)
        denominator = denominator * shrink + jnp.sum(weights, axis=-1)
        weighted = jnp.einsum(
            "hmqk,khe->hmqe",
            weights.astype(jnp.bfloat16),
            value_view,
            preferred_element_type=jnp.float32,
        )
        numerator = numerator * shrink[..., None] + weighted
        return ((newest, denominator, numerator), None)

    blocks = (
        keys_piece.reshape(block_count, block_rows, -1),
        values_piece.reshape(block_count, block_rows, -1),
    )
    result, _ = lax.scan(one_block, state_in, blocks)
    return result


def slot_table(route_block, expert_count, capacity):
    flat_routes = route_block.reshape(-1)
    route_total = flat_routes.shape[0]
    top_count = route_block.shape[1]
    experts_iota = jnp.arange(expert_count, dtype=jnp.int32)
    onehot = (flat_routes[:, None] == experts_iota[None, :]).astype(jnp.int32)
    before = jnp.cumsum(onehot, axis=0) - onehot
    slot_rank = jnp.sum(before * onehot, axis=1)
    slot_iota = jnp.arange(capacity, dtype=jnp.int32)
    matches = (flat_routes[None, None, :] == experts_iota[:, None, None]) & (
        slot_rank[None, None, :] == slot_iota[None, :, None]
    )
    source_row = jnp.arange(route_total, dtype=jnp.int32) // top_count
    source = jnp.sum(jnp.where(matches, source_row[None, None, :], 0), axis=2)
    filled = jnp.any(matches, axis=2)
    return (source, filled, slot_rank.reshape(route_block.shape))


def fill_slots(rows_src, source, filled):
    taken = jnp.take(rows_src, source.reshape(-1), axis=0).reshape(
        source.shape + (rows_src.shape[1],)
    )
    return jnp.where(filled[..., None], taken, jnp.zeros_like(taken))


def rotation_tables(positions, head_dim):
    half_dim = head_dim // 2
    frequency = jnp.power(theta_base, -jnp.arange(half_dim, dtype=jnp.float32) * 2.0 / head_dim)
    angles = positions.astype(jnp.float32)[:, None] * frequency[None, :]
    cosine, sines = jnp.cos(angles), jnp.sin(angles)
    return (
        jnp.concatenate([cosine, cosine], axis=1),
        jnp.concatenate([-sines, sines], axis=1),
    )


def mixer_kernel(
    ep_count,
    tp_count,
    cos_ref,
    sin_ref,
    lam_ref,
    gain_hbm,
    mgain_hbm,
    routes_hbm,
    scale_hbm,
    rows_hbm,
    q_hbm,
    k_hbm,
    v_hbm,
    proj_hbm,
    gate_hbm,
    up_hbm,
    down_hbm,
    sgate_hbm,
    sup_hbm,
    sdown_hbm,
    out_ref,
    moe_ref,
    gain_ref,
    mgain_ref,
    routes_ref,
    scale_ref,
    rows_ref,
    small_sem,
    norm_ref,
    slot_ref,
    mix_ref,
    raw,
    pack_ref,
    q_sem,
    proj_ref,
    gate_ref,
    up_ref,
    down_ref,
    sgate_ref,
    sup_ref,
    sdown_ref,
    xbuf,
    hidden,
    pair_out,
    pair_own,
    pair_in,
    far_in,
    shared_sum,
    ret_out,
    ret_in,
    w_sem,
    d_send,
    d_recv,
    g_send,
    g_recv,
    h_send,
    h_recv,
    p_sem,
    y_send,
    y_recv,
    v_send,
    v_recv,
    qbuf,
    kbuf,
    vbuf,
    lam_own,
    lam_other,
    obuf,
    heads,
    sum_out,
    sum_in,
    kept,
    block_out,
    block_in,
    s_send,
    s_recv,
    s_local,
    f_send,
    f_recv,
    l_sem,
    o_send,
    o_recv,
    r_send,
    r_recv,
    b_send,
    b_recv,
):
    head_count = pack_ref.shape[1]
    half, width = pack_ref.shape[3], pack_ref.shape[4]
    head_dim = width // 2
    e = lax.axis_index("ep")
    t = lax.axis_index("tp")
    y, c = t // 2, lax.rem(t, 2)
    partner = y * 2 + 1 - c
    s_me, h_me = e // head_count, lax.rem(e, head_count)
    y_count = tp_count // 2
    share = half // y_count

    barrier = pltpu.get_barrier_semaphore()

    def greet(where):
        pl.semaphore_signal(barrier, inc=1, device_id=where, device_id_type=MESH)

    def greet_row(j, carry):
        there = lax.rem(e + j, ep_count)
        for core in range(2):
            greet((there, y * 2 + core))
        return carry

    lax.fori_loop(1, ep_count, greet_row, 0)
    greet((e, partner))
    for step in range(1, y_count):
        greet((e, lax.rem(y + step, y_count) * 2 + c))

    def remote(src, dst, send, recv, where):
        return pltpu.make_async_remote_copy(
            src_ref=src,
            dst_ref=dst,
            send_sem=send,
            recv_sem=recv,
            device_id=where,
            device_id_type=MESH,
        )

    small_copies = [
        pltpu.make_async_copy(a, b, small_sem.at[at])
        for at, (a, b) in enumerate(
            (
                (rows_hbm, rows_ref),
                (mgain_hbm, mgain_ref),
                (routes_hbm, routes_ref),
                (scale_hbm, scale_ref),
                (gain_hbm, gain_ref),
            )
        )
    ]
    for copy in small_copies:
        copy.start()
    raw_copies = [
        pltpu.make_async_copy(ref, raw.at[at], q_sem.at[at])
        for at, ref in enumerate((q_hbm, k_hbm, v_hbm))
    ]
    for copy in raw_copies:
        copy.start()
    weight_copies = [
        pltpu.make_async_copy(a, b, w_sem.at[at])
        for at, (a, b) in enumerate(
            (
                (sgate_hbm, sgate_ref),
                (sup_hbm, sup_ref),
                (sdown_hbm, sdown_ref),
                (gate_hbm.at[0], gate_ref),
                (up_hbm.at[0], up_ref),
                (down_hbm.at[0], down_ref),
                (proj_hbm, proj_ref),
            )
        )
    ]
    for copy in weight_copies:
        copy.start()

    def landing(which, side, source):
        if which == 0:
            return qbuf.at[source]
        return (kbuf, vbuf)[which - 1].at[pl.ds((side * ep_count + source) * half, half)]

    def first_copy(which, h, side):
        return remote(
            pack_ref.at[which, h, side],
            landing(which, side, e),
            s_send.at[which, h, side],
            s_recv.at[which, e],
            (c * head_count + h, y * 2 + side),
        )

    def own_copy(which):
        return pltpu.make_async_copy(
            pack_ref.at[which, h_me, c], landing(which, c, e), s_local.at[which]
        )

    def forward(which, source):
        place = landing(which, c, source)
        return remote(
            place, place, f_send.at[which - 1, source], f_recv.at[which - 1, source], (e, partner)
        )

    capacity = xbuf.shape[2]
    own_rows = moe_ref.shape[0]
    slots = ep_count * capacity
    batch_rows = rows_ref.shape[0]

    for copy in small_copies[:4]:
        copy.wait()
    widened = rows_ref[...].astype(jnp.float32)
    mean_square = jnp.mean(widened * widened, axis=-1, keepdims=True)
    norm_ref[...] = (widened * lax.rsqrt(mean_square + norm_eps) * mgain_ref[...]).astype(
        jnp.bfloat16
    )
    slot_at = lax.broadcasted_iota(jnp.int32, (slots, batch_rows), 0)
    slot_expert, slot_rank = slot_at // capacity, lax.rem(slot_at, capacity)
    hits = [routes_ref[k : k + 1, :] == slot_expert for k in range(routes_ref.shape[0])]
    named = sum(hit.astype(jnp.float32) for hit in hits).astype(jnp.bfloat16)
    other_at = lax.broadcasted_iota(jnp.int32, (batch_rows, batch_rows), 0)
    row_at = lax.broadcasted_iota(jnp.int32, (batch_rows, batch_rows), 1)
    earlier = jnp.logical_and(other_at < row_at, other_at // own_rows == row_at // own_rows)
    before = jnp.dot(
        named, earlier.astype(jnp.float32).astype(jnp.bfloat16), preferred_element_type=jnp.float32
    ).astype(jnp.int32)
    chosen = [jnp.logical_and(hit, before == slot_rank).astype(jnp.float32) for hit in hits]
    token_block = lax.broadcasted_iota(jnp.int32, (slots, batch_rows), 1) // own_rows
    picked = jnp.where(token_block == t, sum(chosen), 0.0).astype(jnp.bfloat16)
    slot_ref[...] = jnp.dot(
        picked, norm_ref[...], preferred_element_type=jnp.float32
    ).astype(jnp.bfloat16)
    mixing = sum(scale_ref[k : k + 1, :] * chosen[k] for k in range(len(chosen)))
    mix_ref[...] = jnp.transpose(mixing)
    lam_own[...] = jnp.full(lam_own.shape, lam_ref[h_me], jnp.float32)

    for copy in raw_copies:
        copy.wait()

    def pack_head(h, carry):
        cosine = cos_ref[...]
        sines = sin_ref[...]
        for which in range(2):
            for m in range(2):
                at = pl.multiple_of(h * width + m * head_dim, head_dim)
                part = raw[which, :, pl.ds(at, head_dim)].astype(jnp.float32)
                turned = part * cosine + pltpu.roll(part, head_dim // 2, 1) * sines
                turned = turned.astype(jnp.bfloat16)
                for v in range(y_count):
                    for side in range(2):
                        block = v * 2 + side
                        pack_ref[
                            which,
                            h,
                            side,
                            v * share : (v + 1) * share,
                            m * head_dim : (m + 1) * head_dim,
                        ] = turned[block * share : (block + 1) * share]
        at = pl.multiple_of(h * width, width)
        for v in range(y_count):
            for side in range(2):
                block = v * 2 + side
                pack_ref[2, h, side, v * share : (v + 1) * share] = raw[
                    2, block * share : (block + 1) * share, pl.ds(at, width)
                ]
        return carry

    lax.fori_loop(0, head_count, pack_head, 0)

    pl.semaphore_wait(barrier, (ep_count - 1) * 2 + 1 + (y_count - 1))

    def dispatch(target):
        rows = pl.ds(pl.multiple_of(target * capacity, capacity), capacity)
        return remote(
            slot_ref.at[rows], xbuf.at[t, e], d_send.at[target], d_recv.at[e], (target, t)
        )

    own_slots = pl.ds(pl.multiple_of(e * capacity, capacity), capacity)
    own_dispatch = pltpu.make_async_copy(slot_ref.at[own_slots], xbuf.at[t, e], d_recv.at[e])

    def start_dispatch(j, carry):
        dispatch(lax.rem(e + ep_count // 2 + j, ep_count)).start()
        return carry

    lax.fori_loop(0, ep_count // 2, start_dispatch, 0)

    def start_late(j, carry):
        dispatch(lax.rem(e + 1 + j, ep_count)).start()
        return carry

    lax.fori_loop(0, ep_count // 2 - 1, start_late, 0)

    mine = s_me == c

    def each_send(whiches, act):
        def body(j, carry):
            h = lax.rem(h_me + 1 + j, head_count)
            for k in range(2):
                side = lax.rem(c + 1 + k, 2)
                own = jnp.logical_and(c * head_count + h == e, side == c)
                act(whiches, h, side, own)
            return carry

        lax.fori_loop(0, head_count, body, 0)

    def start_send(whiches, h, side, own):
        @pl.when(jnp.logical_not(own))
        def _():
            for which in whiches:
                first_copy(which, h, side).start()

    each_send((1, 2), start_send)
    each_send((0,), start_send)
    lam_copy = remote(lam_own, lam_other, l_sem.at[0], l_sem.at[1], (e, partner))
    lam_copy.start()
    own_dispatch.start()

    @pl.when(mine)
    def _():
        for which in range(3):
            own_copy(which).start()

    for copy in weight_copies[:3]:
        copy.wait()
    normed = norm_ref[...]
    gate_part = jnp.dot(normed, sgate_ref[...], preferred_element_type=jnp.float32)
    up_part = jnp.dot(normed, sup_ref[...], preferred_element_type=jnp.float32)
    shared_hidden = (gate_part / (1.0 + jnp.exp(-gate_part)) * up_part).astype(jnp.bfloat16)
    shared_part = jnp.dot(
        shared_hidden, sdown_ref[...], preferred_element_type=jnp.float32
    ).astype(jnp.bfloat16)
    for v in range(y_count):
        for core in range(2):
            block = shared_part[(v * 2 + core) * own_rows : (v * 2 + core + 1) * own_rows]

            @pl.when(c == core)
            def _():
                pair_own[v, :own_rows, :] = block

            @pl.when(c != core)
            def _():
                pair_out[v, :own_rows, :] = block

    def spread(place, source, far):
        if far == 0:
            sends, recvs, where = g_send.at[source, 0], g_recv.at[source, 0], (e, partner)
        else:
            there = lax.rem(y + far, y_count)
            sends, recvs = g_send.at[source, far], g_recv.at[source, far]
            where = (e, there * 2 + c)
        return remote(place, place, sends, recvs, where)

    def arrive_slots(j, carry):
        source = lax.rem(e + j, ep_count)
        place = xbuf.at[t, source]

        @pl.when(source == e)
        def _():
            own_dispatch.wait()

        @pl.when(source != e)
        def _():
            remote(
                place, place, d_send.at[source], d_recv.at[source], (e, partner)
            ).wait_recv()

        for far in range(1, y_count):
            spread(place, source, far).start()
        spread(place, source, 0).start()
        return carry

    lax.fori_loop(0, ep_count, arrive_slots, 0)

    def relay(source, far, core):
        from_y = lax.rem(y + y_count - far, y_count)
        place = xbuf.at[from_y * 2 + core, source]
        return remote(
            place, place, h_send.at[source, far - 1], h_recv.at[source, far - 1], (e, partner)
        )

    def arrive_far(j, carry):
        source = lax.rem(e + j, ep_count)
        for far in range(1, y_count):
            from_y = lax.rem(y + y_count - far, y_count)
            spread(xbuf.at[from_y * 2 + c, source], source, far).wait_recv()
            relay(source, far, c).start()
        return carry

    lax.fori_loop(0, ep_count, arrive_far, 0)

    def arrive_relay(j, carry):
        source = lax.rem(e + j, ep_count)
        spread(xbuf.at[partner, source], source, 0).wait_recv()
        for far in range(1, y_count):
            relay(source, far, 1 - c).wait_recv()
        return carry

    lax.fori_loop(0, ep_count, arrive_relay, 0)

    for copy in weight_copies[3:6]:
        copy.wait()
    rows_in = xbuf[...].reshape(tp_count * slots, xbuf.shape[3])
    gate_part = jnp.dot(rows_in, gate_ref[...], preferred_element_type=jnp.float32)
    up_part = jnp.dot(rows_in, up_ref[...], preferred_element_type=jnp.float32)
    hidden[...] = (
        (gate_part / (1.0 + jnp.exp(-gate_part)) * up_part).astype(jnp.bfloat16)
    ).reshape(hidden.shape)

    def down_part(core, into):
        rows = jnp.concatenate([hidden[v * 2 + core] for v in range(y_count)], axis=0)
        product = jnp.dot(rows, down_ref[...], preferred_element_type=jnp.float32)
        product = product.astype(jnp.bfloat16)
        for v in range(y_count):
            into[v, own_rows:, :] = product[v * slots : (v + 1) * slots]

    down_part(1 - c, pair_out)
    near_copy = remote(pair_out, pair_in, p_sem.at[0], p_sem.at[1], (e, partner))
    near_copy.start()
    down_part(c, pair_own)
    near_copy.wait()
    pair_own[...] = (
        pair_own[...].astype(jnp.float32) + pair_in[...].astype(jnp.float32)
    ).astype(jnp.bfloat16)

    def far_copy(step):
        target = lax.rem(y + step, y_count)
        return remote(
            pair_own.at[target],
            far_in.at[step - 1],
            y_send.at[step - 1],
            y_recv.at[step - 1],
            (e, target * 2 + c),
        )

    for step in range(1, y_count):
        far_copy(step).start()

    def arrived(which, source):
        own = jnp.logical_and(source == e, mine)

        @pl.when(own)
        def _():
            own_copy(which).wait()

        @pl.when(jnp.logical_not(own))
        def _():
            place = landing(which, c, source)
            remote(
                place, place, f_send.at[0, source], s_recv.at[which, source], (e, partner)
            ).wait_recv()

    def arrive(j, carry):
        source = lax.rem(e + j, ep_count)
        for which in (1, 2):
            arrived(which, source)
            forward(which, source).start()
        return carry

    lax.fori_loop(0, ep_count, arrive, 0)

    def give_back(target):
        return remote(
            ret_out.at[target], ret_in.at[e], v_send.at[target], v_recv.at[e], (target, t)
        )

    own_back = pltpu.make_async_copy(ret_out.at[e], ret_in.at[e], v_recv.at[e])

    for step in range(1, y_count):
        far_copy(step).wait_recv()
    expert_sum = pair_own[y].astype(jnp.float32)
    for step in range(1, y_count):
        expert_sum = expert_sum + far_in[step - 1].astype(jnp.float32)
    shared_sum[...] = expert_sum[:own_rows]
    ret_out[...] = expert_sum[own_rows:].astype(jnp.bfloat16).reshape(ret_out.shape)

    def start_back(j, carry):
        give_back(lax.rem(e + 1 + j, ep_count)).start()
        return carry

    lax.fori_loop(0, ep_count - 1, start_back, 0)
    own_back.start()

    def arrive_forward(j, carry):
        source = lax.rem(e + j, ep_count)
        for which in (1, 2):
            place = landing(which, 1 - c, source)
            remote(
                place,
                place,
                f_send.at[which - 1, source],
                f_recv.at[which - 1, source],
                (e, partner),
            ).wait_recv()
        return carry

    lax.fori_loop(0, ep_count, arrive_forward, 0)
    lam_copy.wait()
    small_copies[4].wait()

    lam = jnp.where(mine, lam_own[...], lam_other[...])[0:1, 0:1]
    gain = gain_ref[...]
    factor = head_dim ** (-0.5) * log2_e

    def back_place(v):
        return heads.at[h_me, v, c]

    def back_copy(target, v):
        return remote(
            obuf.at[target, v],
            back_place(v),
            o_send.at[target, v],
            o_recv.at[h_me, v, c],
            (target, y * 2 + s_me),
        )

    def back_own(v):
        return pltpu.make_async_copy(obuf.at[e, v], back_place(v), o_recv.at[h_me, v, c])

    pair_count = ep_count // 2
    pair_me = e // 2

    def attend(j, carry):
        v = lax.rem(y + 1 + j // pair_count, y_count)
        at = lax.rem(pair_me + pair_count // 2 + lax.rem(j, pair_count), pair_count)
        targets = (at * 2, at * 2 + 1)

        @pl.when(j < pair_count)
        def _():
            for target in targets:
                arrived(0, target)

        rows = pl.ds(pl.multiple_of(v * share, share), share)
        block = jnp.concatenate([qbuf[target, rows, :] for target in targets], axis=0)
        ratios = []
        for m in range(2):
            columns = slice(m * head_dim, (m + 1) * head_dim)
            scores = lax.dot_general(
                block[:, columns],
                kbuf[:, columns],
                (((1,), (1,)), ((), ())),
                preferred_element_type=jnp.float32,
            )
            top = jnp.max(scores, axis=-1, keepdims=True)
            weights = jnp.exp2((scores - top) * factor)
            denominator = jnp.sum(weights, axis=-1, keepdims=True)
            weighted = jnp.dot(
                weights.astype(jnp.bfloat16), vbuf[...], preferred_element_type=jnp.float32
            )
            ratios.append(weighted / denominator)
        mixed = ratios[0] - lam * ratios[1]
        mean_square = jnp.mean(mixed * mixed, axis=-1, keepdims=True)
        done = (mixed * lax.rsqrt(mean_square + head_eps) * gain).astype(jnp.bfloat16)
        for k, target in enumerate(targets):
            obuf[target, v] = done[k * share : (k + 1) * share]
        for target in targets:
            own = jnp.logical_and(target == e, mine)

            @pl.when(jnp.logical_not(own))
            def _():
                back_copy(target, v).start()

            @pl.when(own)
            def _():
                back_own(v).start()

        return carry

    lax.fori_loop(0, pair_count * y_count, attend, 0)

    weight_copies[6].wait()

    def pair_copy(at):
        return remote(sum_out.at[at], sum_in.at[at], r_send.at[at], r_recv.at[at], (e, partner))

    def project(at):
        v = lax.rem(y + 1 + at, y_count)

        def arrive_heads(h, carry):
            for side in range(2):
                own = jnp.logical_and(
                    jnp.logical_and(c * head_count + h == e, side == c), h == h_me
                )
                place = heads.at[h, v, side]

                @pl.when(own)
                def _():
                    back_own(v).wait()

                @pl.when(jnp.logical_not(own))
                def _():
                    remote(
                        place, place, o_send.at[0, 0], o_recv.at[h, v, side], (e, partner)
                    ).wait_recv()

            return carry

        lax.fori_loop(0, head_count, arrive_heads, 0)
        total = None
        for h in range(head_count):
            rows = jnp.concatenate([heads[h, v, 1 - c], heads[h, v, c]], axis=0)
            term = jnp.dot(
                rows,
                proj_ref[h * width : (h + 1) * width, :],
                preferred_element_type=jnp.float32,
            )
            total = term if total is None else total + term
        total = total.astype(jnp.bfloat16)
        sum_out[at] = total[:share]
        kept[at] = total[share:]
        pair_copy(at).start()

    def block_copy(step):
        target = lax.rem(y + step, y_count)
        return remote(
            block_out.at[step - 1],
            block_in.at[step - 1],
            b_send.at[step - 1],
            b_recv.at[step - 1],
            (e, target * 2 + c),
        )

    for step in range(1, y_count):
        project(step - 1)
        pair_copy(step - 1).wait()
        block_out[step - 1] = (
            kept[step - 1].astype(jnp.float32) + sum_in[step - 1].astype(jnp.float32)
        ).astype(jnp.bfloat16)
        block_copy(step).start()
    project(y_count - 1)

    own_back.wait()

    def arrive_back(j, carry):
        source = lax.rem(e + 1 + j, ep_count)
        place = ret_in.at[source]
        remote(place, place, v_send.at[source], v_recv.at[source], (e, partner)).wait_recv()
        return carry

    lax.fori_loop(0, ep_count - 1, arrive_back, 0)
    mix = mix_ref[pl.ds(pl.multiple_of(t * own_rows, own_rows), own_rows), :]
    coarse = mix.astype(jnp.bfloat16)
    fine = (mix - coarse.astype(jnp.float32)).astype(jnp.bfloat16)
    returned = ret_in[...].reshape(slots, ret_in.shape[2])
    combined = jnp.dot(coarse, returned, preferred_element_type=jnp.float32)
    combined = combined + jnp.dot(fine, returned, preferred_element_type=jnp.float32)
    moe_ref[...] = (shared_sum[...] + combined).astype(jnp.bfloat16)

    pair_copy(y_count - 1).wait()
    total = (
        kept[y_count - 1].astype(jnp.float32) + sum_in[y_count - 1].astype(jnp.float32)
    ).astype(jnp.bfloat16)
    total = total.astype(jnp.float32)
    for step in range(1, y_count):
        block_copy(step).wait()
        total = total + block_in[step - 1].astype(jnp.float32)
    out_ref[...] = total.astype(jnp.bfloat16)

    def end_send(whiches, h, side, own):
        @pl.when(jnp.logical_not(own))
        def _():
            for which in whiches:
                first_copy(which, h, side).wait_send()

    each_send((0, 1, 2), end_send)

    for step in range(1, y_count):
        far_copy(step).wait_send()

    def end_rest(source, carry):
        for far in range(y_count):
            spread(xbuf.at[t, source], source, far).wait_send()
        for far in range(1, y_count):
            relay(source, far, c).wait_send()

        @pl.when(source != e)
        def _():
            dispatch(source).wait_send()
            give_back(source).wait_send()

        for which in (1, 2):
            forward(which, source).wait_send()

        @pl.when(jnp.logical_not(jnp.logical_and(source == e, mine)))
        def _():
            for v in range(y_count):
                back_copy(source, v).wait_send()

        return carry

    lax.fori_loop(0, ep_count, end_rest, 0)


def mixer(
    tables,
    sequence,
    lambdas,
    head_gain,
    out_proj,
    moe_inputs,
    expert_weights,
    ep_count,
    tp_count,
    capacity,
):
    moe_input, moe_gain, routes, route_weights = moe_inputs
    head_count = lambdas.shape[0]
    half = sequence[0].shape[0] // 2
    width = sequence[0].shape[1] // head_count
    slots = ep_count * capacity
    batch_rows, model = moe_input.shape
    own_rows = batch_rows // tp_count
    top_count = routes.shape[1]
    hidden_width = expert_weights[0].shape[2]
    shared_width = expert_weights[3].shape[1]
    tokens = ep_count * 2 * half
    share = 2 * half // tp_count
    y_count = tp_count // 2
    dma = pltpu.SemaphoreType.DMA
    bf16 = jnp.bfloat16
    return pl.pallas_call(
        functools.partial(mixer_kernel, ep_count, tp_count),
        out_shape=(
            jax.ShapeDtypeStruct((share, model), bf16),
            jax.ShapeDtypeStruct((own_rows, model), bf16),
        ),
        in_specs=[pl.BlockSpec(memory_space=pltpu.VMEM)] * 2
        + [pl.BlockSpec(memory_space=pltpu.SMEM)]
        + [pl.BlockSpec(memory_space=pltpu.HBM)] * 15,
        out_specs=[pl.BlockSpec(memory_space=pltpu.VMEM)] * 2,
        scratch_shapes=[
            pltpu.VMEM((1, width), jnp.float32),
            pltpu.VMEM((1, model), jnp.float32),
            pltpu.VMEM((top_count, batch_rows), jnp.int32),
            pltpu.VMEM((top_count, batch_rows), jnp.float32),
            pltpu.VMEM((batch_rows, model), bf16),
            dma((5,)),
            pltpu.VMEM((batch_rows, model), bf16),
            pltpu.VMEM((slots, model), bf16),
            pltpu.VMEM((batch_rows, slots), jnp.float32),
            pltpu.VMEM((3,) + sequence[0].shape, bf16),
            pltpu.VMEM((3, head_count, 2, half, width), bf16),
            dma((3,)),
            pltpu.VMEM(out_proj.shape, bf16),
            pltpu.VMEM((model, hidden_width), bf16),
            pltpu.VMEM((model, hidden_width), bf16),
            pltpu.VMEM((hidden_width, model), bf16),
            pltpu.VMEM((model, shared_width), bf16),
            pltpu.VMEM((model, shared_width), bf16),
            pltpu.VMEM((shared_width, model), bf16),
            pltpu.VMEM((tp_count, ep_count, capacity, model), bf16),
            pltpu.VMEM((tp_count, slots, hidden_width), bf16),
            pltpu.VMEM((y_count, own_rows + slots, model), bf16),
            pltpu.VMEM((y_count, own_rows + slots, model), bf16),
            pltpu.VMEM((y_count, own_rows + slots, model), bf16),
            pltpu.VMEM((max(1, y_count - 1), own_rows + slots, model), bf16),
            pltpu.VMEM((own_rows, model), jnp.float32),
            pltpu.VMEM((ep_count, capacity, model), bf16),
            pltpu.VMEM((ep_count, capacity, model), bf16),
            dma((7,)),
            dma((ep_count,)),
            dma((ep_count,)),
            dma((ep_count, y_count)),
            dma((ep_count, y_count)),
            dma((ep_count, max(1, y_count - 1))),
            dma((ep_count, max(1, y_count - 1))),
            dma((2,)),
            dma((max(1, y_count - 1),)),
            dma((max(1, y_count - 1),)),
            dma((ep_count,)),
            dma((ep_count,)),
            pltpu.VMEM((ep_count, half, width), bf16),
            pltpu.VMEM((tokens, width), bf16),
            pltpu.VMEM((tokens, width), bf16),
            pltpu.VMEM((8, 128), jnp.float32),
            pltpu.VMEM((8, 128), jnp.float32),
            pltpu.VMEM((ep_count, y_count, share, width), bf16),
            pltpu.VMEM((head_count, y_count, 2, share, width), bf16),
            pltpu.VMEM((y_count, share, model), bf16),
            pltpu.VMEM((y_count, share, model), bf16),
            pltpu.VMEM((y_count, share, model), bf16),
            pltpu.VMEM((max(1, y_count - 1), share, model), bf16),
            pltpu.VMEM((max(1, y_count - 1), share, model), bf16),
            dma((3, head_count, 2)),
            dma((3, ep_count)),
            dma((3,)),
            dma((2, ep_count)),
            dma((2, ep_count)),
            dma((2,)),
            dma((ep_count, y_count)),
            dma((head_count, y_count, 2)),
            dma((y_count,)),
            dma((y_count,)),
            dma((max(1, y_count - 1),)),
            dma((max(1, y_count - 1),)),
        ],
        compiler_params=pltpu.CompilerParams(
            has_side_effects=True, vmem_limit_bytes=67043328, collective_id=0
        ),
        name="mixer",
    )(
        *tables,
        lambdas,
        head_gain[None, :],
        moe_gain[None, :],
        jnp.transpose(routes),
        jnp.transpose(route_weights),
        moe_input,
        *sequence,
        out_proj,
        *expert_weights,
    )


def local(
    queries,
    key_rows,
    value_rows,
    lambdas,
    head_gain,
    out_proj,
    moe_input,
    moe_gain,
    routes,
    route_weights,
    expert_gate,
    expert_up,
    expert_down,
    shared_gate,
    shared_up,
    shared_down,
):
    query_rows = queries.shape[0]
    head_count = lambdas.shape[0]
    head_dim = queries.shape[1] // (2 * head_count)
    tp_count = lax.axis_size("tp")
    ep_count = lax.axis_size("ep")
    tp_place = lax.axis_index("tp")
    ep_place = lax.axis_index("ep")
    positions = ep_place * query_rows + jnp.arange(query_rows, dtype=jnp.int32)
    batch_rows = moe_input.shape[0]
    top_count = routes.shape[1]
    own_rows = batch_rows // tp_count
    local_experts = expert_gate.shape[0]
    expert_count = local_experts * ep_count
    capacity = (2 * own_rows * top_count + expert_count - 1) // expert_count
    one_head_each = ep_count == 2 * head_count and tp_count % 2 == 0 and local_experts == 1 and ep_count % 4 == 0
    if one_head_each:
        tables = rotation_tables(positions, head_dim)
        sequence = (queries, key_rows, value_rows)
        weights = (expert_gate, expert_up, expert_down, shared_gate, shared_up, shared_down)
        return mixer(
            tables,
            sequence,
            lambdas,
            head_gain,
            out_proj,
            (moe_input, moe_gain, routes, route_weights),
            weights,
            ep_count,
            tp_count,
            capacity,
        )
    else:
        rot_query = rotate(queries, positions, head_dim)
        rot_keys = rotate(key_rows, positions, head_dim)
        initial = (
            jnp.full((head_count, 2, query_rows), -1e30, jnp.float32),
            jnp.zeros((head_count, 2, query_rows), jnp.float32),
            jnp.zeros((head_count, 2, query_rows, 2 * head_dim), jnp.float32),
        )
        running_max, denominator, numerator = fold_keys(
            initial,
            (
                lax.all_gather(rot_keys, "ep", axis=0, tiled=True),
                lax.all_gather(value_rows, "ep", axis=0, tiled=True),
            ),
            rot_query,
            head_count,
            head_dim,
        )
        ratio = numerator / denominator[..., None]
        mixed_heads = ratio[:, 0] - lambdas[:, None, None] * ratio[:, 1]
        mean_square = jnp.mean(mixed_heads * mixed_heads, axis=-1, keepdims=True)
        normed_heads = (mixed_heads * lax.rsqrt(mean_square + head_eps) * head_gain).astype(
            jnp.bfloat16
        )
        head_out = jnp.transpose(normed_heads, (1, 0, 2)).reshape(query_rows, head_count * 2 * head_dim)
    normed = rms_rows(moe_input, moe_gain)
    shared_hidden = gated_hidden(normed, shared_gate, shared_up)
    own_routes = lax.dynamic_slice_in_dim(routes, tp_place * own_rows, own_rows, 0)
    own_weights = lax.dynamic_slice_in_dim(route_weights, tp_place * own_rows, own_rows, 0)
    own_source, own_filled, own_rank = slot_table(own_routes, expert_count, capacity)
    own_normed = lax.dynamic_slice_in_dim(normed, tp_place * own_rows, own_rows, 0)
    outgoing = fill_slots(own_normed, own_source, own_filled)
    arrived = lax.all_to_all(outgoing[:, None], "ep", split_axis=0, concat_axis=2, tiled=True)
    hidden = slot_hidden(lax.all_gather(arrived, "tp", axis=1, tiled=True), expert_gate, expert_up)
    slot_rows = local_experts * ep_count * capacity
    mixer_share = query_rows // tp_count
    expert_share = own_rows + slot_rows
    if not one_head_each:
        block_count = lax.axis_size("tp") * mixer_share // mixer_share
        product = jnp.dot(head_out, out_proj, preferred_element_type=jnp.float32)
        mixer_out = lax.psum_scatter(
            product.reshape(block_count, mixer_share, -1)
            .reshape(lax.axis_size("tp") * mixer_share, -1)
            .astype(jnp.bfloat16),
            "tp",
            scatter_dimension=0,
            tiled=True,
        )
    block_count = lax.axis_size("tp") * expert_share // expert_share
    shared_part = jnp.dot(shared_hidden, shared_down, preferred_element_type=jnp.float32).reshape(
        block_count, own_rows, -1
    )
    routed_part = jnp.einsum(
        "xnsf,xfd->nxsd", hidden, expert_down, preferred_element_type=jnp.float32
    )
    routed_part = routed_part.reshape(block_count, slot_rows, -1)
    expert_sum = lax.psum_scatter(
        jnp.concatenate([shared_part, routed_part], axis=1)
        .reshape(lax.axis_size("tp") * expert_share, -1)
        .astype(jnp.bfloat16),
        "tp",
        scatter_dimension=0,
        tiled=True,
    ).astype(jnp.float32)
    shared_sum = expert_sum[:own_rows]
    routed = (
        expert_sum[own_rows:].reshape(local_experts, ep_count * capacity, -1).astype(jnp.bfloat16)
    )
    returned = lax.all_to_all(routed, "ep", split_axis=1, concat_axis=0, tiled=True)
    flat_index = (own_routes * capacity + own_rank).reshape(-1)
    picked = jnp.take(returned.reshape(expert_count * capacity, -1), flat_index, axis=0).reshape(
        own_rows, top_count, -1
    )
    combined = shared_sum + jnp.sum(own_weights[..., None] * picked.astype(jnp.float32), axis=1)
    return (mixer_out, combined.astype(jnp.bfloat16))


def solution(mesh):
    in_specs = (
        P("ep", "tp"),
        P("ep", "tp"),
        P("ep", "tp"),
        P("tp"),
        P(),
        P("tp", None),
        P("ep", None),
        P(),
        P("ep", None),
        P("ep", None),
        P("ep", None, "tp"),
        P("ep", None, "tp"),
        P("ep", "tp", None),
        P(None, "tp"),
        P(None, "tp"),
        P("tp", None),
    )
    out_specs = (P(("ep", "tp"), None), P(("ep", "tp"), None))
    return jax.shard_map(local, mesh=mesh, in_specs=in_specs, out_specs=out_specs, check_vma=False)
```

```python
import functools
import jax
import jax.numpy as jnp
import numpy as np
from jax import lax
from jax.experimental import pallas as pl
from jax.experimental.pallas import tpu as pltpu
from jax.sharding import PartitionSpec as P

theta_base = 500000.0
norm_eps = 1e-06
head_eps = 1e-05
MESH = pl.DeviceIdType.MESH
log2_e = 1.4426950408889634


def rotate(matrix, positions, head_dim):
    row_count = matrix.shape[0]
    shaped = matrix.reshape(row_count, -1, head_dim).astype(jnp.float32)
    half_dim = head_dim // 2
    frequency = jnp.power(theta_base, -jnp.arange(half_dim, dtype=jnp.float32) * 2.0 / head_dim)
    angles = positions.astype(jnp.float32)[:, None] * frequency[None, :]
    cosine = jnp.cos(angles)[:, None, :]
    sines = jnp.sin(angles)[:, None, :]
    front_half = shaped[..., :half_dim]
    second = shaped[..., half_dim:]
    turned = jnp.concatenate(
        [front_half * cosine - second * sines, second * cosine + front_half * sines], axis=-1
    )
    return turned.reshape(matrix.shape).astype(jnp.bfloat16)


def rms_rows(values, gain):
    widened = values.astype(jnp.float32)
    mean_square = jnp.mean(widened * widened, axis=-1, keepdims=True)
    return (widened * lax.rsqrt(mean_square + norm_eps) * gain).astype(jnp.bfloat16)


def gated_hidden(rows_in, gate_weight, up_weight):
    gate_part = jnp.dot(rows_in, gate_weight, preferred_element_type=jnp.float32)
    up_part = jnp.dot(rows_in, up_weight, preferred_element_type=jnp.float32)
    return (jax.nn.silu(gate_part) * up_part).astype(jnp.bfloat16)


def slot_hidden(slot_rows, gate_weight, up_weight):
    gate_part = jnp.einsum(
        "xnsd,xdf->xnsf", slot_rows, gate_weight, preferred_element_type=jnp.float32
    )
    up_part = jnp.einsum("xnsd,xdf->xnsf", slot_rows, up_weight, preferred_element_type=jnp.float32)
    return (jax.nn.silu(gate_part) * up_part).astype(jnp.bfloat16)


def key_block_size(piece_rows):
    for candidate in (1024, 512):
        return candidate
    return piece_rows


def fold_keys(state_in, pieces, rot_query, head_count, head_dim):
    keys_piece, values_piece = pieces
    piece_rows = keys_piece.shape[0]
    block_rows = key_block_size(piece_rows)
    block_count = piece_rows // block_rows
    query_view = rot_query.reshape(rot_query.shape[0], head_count, 2, head_dim)
    score_scale = head_dim ** (-0.5)

    def one_block(running, key_block):
        running_max, denominator, numerator = running
        key_view = key_block[0].reshape(block_rows, head_count, 2, head_dim)
        value_view = key_block[1].reshape(block_rows, head_count, 2 * head_dim)
        scores = (
            jnp.einsum("qhmd,khmd->hmqk", query_view, key_view, preferred_element_type=jnp.float32)
            * score_scale
        )
        newest = jnp.maximum(running_max, jnp.max(scores, axis=-1))
        weights = jnp.exp(scores - newest[..., None])
        shrink = jnp.exp(running_max - newest)
        denominator = denominator * shrink + jnp.sum(weights, axis=-1)
        weighted = jnp.einsum(
            "hmqk,khe->hmqe",
            weights.astype(jnp.bfloat16),
            value_view,
            preferred_element_type=jnp.float32,
        )
        numerator = numerator * shrink[..., None] + weighted
        return ((newest, denominator, numerator), None)

    blocks = (
        keys_piece.reshape(block_count, block_rows, -1),
        values_piece.reshape(block_count, block_rows, -1),
    )
    result, _ = lax.scan(one_block, state_in, blocks)
    return result


def slot_table(route_block, expert_count, capacity):
    flat_routes = route_block.reshape(-1)
    route_total = flat_routes.shape[0]
    top_count = route_block.shape[1]
    experts_iota = jnp.arange(expert_count, dtype=jnp.int32)
    onehot = (flat_routes[:, None] == experts_iota[None, :]).astype(jnp.int32)
    before = jnp.cumsum(onehot, axis=0) - onehot
    slot_rank = jnp.sum(before * onehot, axis=1)
    slot_iota = jnp.arange(capacity, dtype=jnp.int32)
    matches = (flat_routes[None, None, :] == experts_iota[:, None, None]) & (
        slot_rank[None, None, :] == slot_iota[None, :, None]
    )
    source_row = jnp.arange(route_total, dtype=jnp.int32) // top_count
    source = jnp.sum(jnp.where(matches, source_row[None, None, :], 0), axis=2)
    filled = jnp.any(matches, axis=2)
    return (source, filled, slot_rank.reshape(route_block.shape))


def fill_slots(rows_src, source, filled):
    taken = jnp.take(rows_src, source.reshape(-1), axis=0).reshape(
        source.shape + (rows_src.shape[1],)
    )
    return jnp.where(filled[..., None], taken, jnp.zeros_like(taken))


def rotation_tables(row_count, block_count, head_dim):
    half_dim = head_dim // 2
    frequency = np.power(theta_base, -np.arange(half_dim) * 2.0 / head_dim)

    def table(positions):
        angles = positions[:, None] * frequency[None, :]
        cosine, sines = np.cos(angles), np.sin(angles)
        both = (np.concatenate([cosine, cosine], 1), np.concatenate([-sines, sines], 1))
        return np.stack(both).astype(np.float32)

    return (
        jnp.asarray(table(np.arange(row_count))),
        jnp.asarray(table(np.arange(block_count) * row_count)),
    )


def mixer_kernel(
    ep_count,
    tp_count,
    lam_ref,
    turn_hbm,
    base_hbm,
    gain_hbm,
    mgain_hbm,
    routes_hbm,
    scale_hbm,
    rows_hbm,
    q_hbm,
    k_hbm,
    v_hbm,
    proj_hbm,
    gate_hbm,
    up_hbm,
    down_hbm,
    sgate_hbm,
    sup_hbm,
    sdown_hbm,
    out_ref,
    moe_ref,
    turn_ref,
    base_ref,
    cos_ref,
    sin_ref,
    gain_ref,
    mgain_ref,
    routes_ref,
    scale_ref,
    rows_ref,
    small_sem,
    norm_ref,
    slot_ref,
    mix_ref,
    ext_out,
    ext_in,
    rel_slots,
    gathered,
    part_out,
    part_in,
    raw,
    pack_ref,
    q_sem,
    proj_ref,
    gate_ref,
    up_ref,
    down_ref,
    sgate_ref,
    sup_ref,
    sdown_ref,
    xbuf,
    hidden,
    pair_out,
    pair_own,
    pair_in,
    far_in,
    shared_sum,
    ret_out,
    ret_in,
    w_sem,
    d_send,
    d_recv,
    c_sem,
    k_send,
    u_send,
    u_recv,
    m_sem,
    g_send,
    g_recv,
    h_send,
    h_recv,
    p_sem,
    y_send,
    y_recv,
    v_send,
    v_recv,
    qbuf,
    kbuf,
    vbuf,
    lam_own,
    lam_other,
    obuf,
    heads,
    sum_out,
    sum_in,
    kept,
    block_out,
    block_in,
    s_send,
    s_recv,
    s_local,
    f_send,
    f_recv,
    l_sem,
    o_send,
    o_recv,
    r_send,
    r_recv,
    b_send,
    b_recv,
):
    head_count = pack_ref.shape[1]
    half, width = pack_ref.shape[3], pack_ref.shape[4]
    head_dim = width // 2
    e = lax.axis_index("ep")
    t = lax.axis_index("tp")
    y, c = t // 2, lax.rem(t, 2)
    partner = y * 2 + 1 - c
    s_me, h_me = e // head_count, lax.rem(e, head_count)
    y_count = tp_count // 2
    share = half // y_count

    barrier = pltpu.get_barrier_semaphore()

    def greet(where):
        pl.semaphore_signal(barrier, inc=1, device_id=where, device_id_type=MESH)

    def greet_row(j, carry):
        there = lax.rem(e + j, ep_count)
        for core in range(2):
            greet((there, y * 2 + core))
        return carry

    lax.fori_loop(1, ep_count, greet_row, 0)
    greet((e, partner))
    for step in range(1, y_count):
        greet((e, lax.rem(y + step, y_count) * 2 + c))

    def remote(src, dst, send, recv, where):
        return pltpu.make_async_remote_copy(
            src_ref=src,
            dst_ref=dst,
            send_sem=send,
            recv_sem=recv,
            device_id=where,
            device_id_type=MESH,
        )

    small_copies = [
        pltpu.make_async_copy(a, b, small_sem.at[at])
        for at, (a, b) in enumerate(
            (
                (routes_hbm, routes_ref),
                (scale_hbm, scale_ref),
                (mgain_hbm, mgain_ref),
                (rows_hbm, rows_ref),
                (base_hbm, base_ref),
                (turn_hbm, turn_ref),
                (gain_hbm, gain_ref),
            )
        )
    ]
    for copy in small_copies:
        copy.start()
    raw_copies = [
        pltpu.make_async_copy(ref, raw.at[at], q_sem.at[at])
        for at, ref in enumerate((q_hbm, k_hbm, v_hbm))
    ]
    for copy in raw_copies:
        copy.start()
    weight_copies = [
        pltpu.make_async_copy(a, b, w_sem.at[at])
        for at, (a, b) in enumerate(
            (
                (sgate_hbm, sgate_ref),
                (sup_hbm, sup_ref),
                (sdown_hbm, sdown_ref),
                (gate_hbm.at[0], gate_ref),
                (up_hbm.at[0], up_ref),
                (down_hbm.at[0], down_ref),
                (proj_hbm, proj_ref),
            )
        )
    ]
    def landing(which, side, source):
        if which == 0:
            return qbuf.at[source]
        return (kbuf, vbuf)[which - 1].at[pl.ds((side * ep_count + source) * half, half)]

    def first_copy(which, h, side):
        return remote(
            pack_ref.at[which, h, side],
            landing(which, side, e),
            s_send.at[which, h, side],
            s_recv.at[which, e],
            (c * head_count + h, y * 2 + side),
        )

    def own_copy(which):
        return pltpu.make_async_copy(
            pack_ref.at[which, h_me, c], landing(which, c, e), s_local.at[which]
        )

    def forward(which, source):
        place = landing(which, c, source)
        return remote(
            place, place, f_send.at[which - 1, source], f_recv.at[which - 1, source], (e, partner)
        )

    capacity = xbuf.shape[2]
    own_rows = moe_ref.shape[0]
    slots = ep_count * capacity
    batch_rows = rows_ref.shape[0]
    model = rows_ref.shape[1]
    half_count = ep_count // 2
    half_slots = half_count * capacity
    across = lax.rem(e + half_count, ep_count)
    near_first = s_me * half_count
    place_me = lax.rem(e, half_count)

    def near(j):
        return near_first + lax.rem(place_me + j, half_count)

    for copy in small_copies[:4]:
        copy.wait()
    widened = rows_ref[...].astype(jnp.float32)
    mean_square = jnp.mean(widened * widened, axis=-1, keepdims=True)
    norm_ref[...] = (widened * lax.rsqrt(mean_square + norm_eps) * mgain_ref[...]).astype(
        jnp.bfloat16
    )
    slot_at = lax.broadcasted_iota(jnp.int32, (slots, batch_rows), 0)
    slot_expert, slot_rank = slot_at // capacity, lax.rem(slot_at, capacity)
    hits = [routes_ref[k : k + 1, :] == slot_expert for k in range(routes_ref.shape[0])]
    named = sum(hit.astype(jnp.float32) for hit in hits).astype(jnp.bfloat16)
    other_at = lax.broadcasted_iota(jnp.int32, (batch_rows, batch_rows), 0)
    row_at = lax.broadcasted_iota(jnp.int32, (batch_rows, batch_rows), 1)
    earlier = jnp.logical_and(other_at < row_at, other_at // own_rows == row_at // own_rows)
    before = jnp.dot(
        named, earlier.astype(jnp.float32).astype(jnp.bfloat16), preferred_element_type=jnp.float32
    ).astype(jnp.int32)
    chosen = [jnp.logical_and(hit, before == slot_rank).astype(jnp.float32) for hit in hits]
    token_block = lax.broadcasted_iota(jnp.int32, (slots, batch_rows), 1) // own_rows
    picked = jnp.where(token_block == t, sum(chosen), 0.0).astype(jnp.bfloat16)
    slot_ref[...] = jnp.dot(
        picked, norm_ref[...], preferred_element_type=jnp.float32
    ).astype(jnp.bfloat16)
    mixing = sum(scale_ref[k : k + 1, :] * chosen[k] for k in range(len(chosen)))
    mix_ref[...] = jnp.transpose(mixing)
    lam_own[...] = jnp.full(lam_own.shape, lam_ref[h_me], jnp.float32)

    def fold(wide):
        return jnp.where(s_me == 0, wide[:, half_slots:], wide[:, :half_slots])

    own_span = pl.ds(pl.multiple_of(t * own_rows, own_rows), own_rows)
    away = fold(mix_ref[own_span, :])
    away_coarse = away.astype(jnp.bfloat16)
    away_fine = (away - away_coarse.astype(jnp.float32)).astype(jnp.bfloat16)
    ext_out[:, :model] = norm_ref[own_span, :]
    ext_out[:, model:] = jnp.concatenate([away_coarse, away_fine], axis=1)

    for copy in small_copies[4:6]:
        copy.wait()
    base_cos, base_sin = base_ref[0, pl.ds(e, 1), :], base_ref[1, pl.ds(e, 1), :]
    cos_ref[...] = base_cos * turn_ref[0] - base_sin * turn_ref[1]
    sin_ref[...] = base_sin * turn_ref[0] + base_cos * turn_ref[1]
    for copy in raw_copies:
        copy.wait()

    def pack_head(h, carry):
        cosine = cos_ref[...]
        sines = sin_ref[...]
        for which in range(2):
            for m in range(2):
                at = pl.multiple_of(h * width + m * head_dim, head_dim)
                part = raw[which, :, pl.ds(at, head_dim)].astype(jnp.float32)
                turned = part * cosine + pltpu.roll(part, head_dim // 2, 1) * sines
                turned = turned.astype(jnp.bfloat16)
                for v in range(y_count):
                    for side in range(2):
                        block = v * 2 + side
                        pack_ref[
                            which,
                            h,
                            side,
                            v * share : (v + 1) * share,
                            m * head_dim : (m + 1) * head_dim,
                        ] = turned[block * share : (block + 1) * share]
        at = pl.multiple_of(h * width, width)
        for v in range(y_count):
            for side in range(2):
                block = v * 2 + side
                pack_ref[2, h, side, v * share : (v + 1) * share] = raw[
                    2, block * share : (block + 1) * share, pl.ds(at, width)
                ]
        return carry

    lax.fori_loop(0, head_count, pack_head, 0)

    pl.semaphore_wait(barrier, (ep_count - 1) * 2 + 1 + (y_count - 1))

    for copy in weight_copies:
        copy.start()

    def dispatch(target):
        rows = pl.ds(pl.multiple_of(target * capacity, capacity), capacity)
        return remote(
            slot_ref.at[rows], xbuf.at[t, e], d_send.at[target], d_recv.at[e], (target, t)
        )

    cross_copy = remote(ext_out, ext_in, c_sem.at[0], c_sem.at[1], (across, t))
    cross_copy.start()

    def start_dispatch(j, carry):
        dispatch(near(j)).start()
        return carry

    lax.fori_loop(1, half_count, start_dispatch, 0)

    mine = s_me == c

    def each_send(whiches, act):
        def body(j, carry):
            h = lax.rem(h_me + 1 + j, head_count)
            for k in range(2):
                side = lax.rem(c + 1 + k, 2)
                own = jnp.logical_and(c * head_count + h == e, side == c)
                act(whiches, h, side, own)
            return carry

        lax.fori_loop(0, head_count, body, 0)

    def start_send(whiches, h, side, own):
        @pl.when(jnp.logical_not(own))
        def _():
            for which in whiches:
                first_copy(which, h, side).start()

    pair_count = ep_count // 2
    pair_me = e // 2
    near_pairs = pair_count // 2
    beside = jnp.logical_or(pair_me == near_pairs - 1, pair_me == near_pairs)
    at_once = jnp.logical_and(jnp.logical_not(mine), beside)

    @pl.when(at_once)
    def _():
        each_send((1, 2), start_send)
        each_send((0,), start_send)

    lam_copy = remote(lam_own, lam_other, l_sem.at[0], l_sem.at[1], (e, partner))
    lam_copy.start()
    xbuf[t, e] = slot_ref[pl.ds(pl.multiple_of(e * capacity, capacity), capacity), :]

    for copy in weight_copies[:3]:
        copy.wait()
    normed = norm_ref[...]
    gate_part = jnp.dot(normed, sgate_ref[...], preferred_element_type=jnp.float32)
    up_part = jnp.dot(normed, sup_ref[...], preferred_element_type=jnp.float32)
    shared_hidden = (gate_part / (1.0 + jnp.exp(-gate_part)) * up_part).astype(jnp.bfloat16)
    shared_part = jnp.dot(
        shared_hidden, sdown_ref[...], preferred_element_type=jnp.float32
    ).astype(jnp.bfloat16)
    for v in range(y_count):
        for core in range(2):
            block = shared_part[(v * 2 + core) * own_rows : (v * 2 + core + 1) * own_rows]

            @pl.when(c == core)
            def _():
                pair_own[v, :own_rows, :] = block

            @pl.when(c != core)
            def _():
                pair_out[v, :own_rows, :] = block

    cross_copy.wait_recv()
    sent_rows = ext_in[:, :model]
    sent_mix = ext_in[:, model:]
    taken = (sent_mix[:, :half_slots].astype(jnp.float32) > 0.0).astype(jnp.float32)
    rel_slots[...] = lax.dot_general(
        taken.astype(jnp.bfloat16),
        sent_rows,
        (((0,), (0,)), ((), ())),
        preferred_element_type=jnp.float32,
    ).astype(jnp.bfloat16)

    def pass_on(j):
        to = lax.rem(place_me + j, half_count)
        rows = pl.ds(pl.multiple_of(to * capacity, capacity), capacity)
        return remote(
            rel_slots.at[rows],
            xbuf.at[t, across],
            k_send.at[to],
            d_recv.at[across],
            (near_first + to, t),
        )

    def start_pass(j, carry):
        pass_on(j).start()
        return carry

    lax.fori_loop(1, half_count, start_pass, 0)
    xbuf[t, across] = rel_slots[
        pl.ds(pl.multiple_of(place_me * capacity, capacity), capacity), :
    ]

    @pl.when(jnp.logical_not(at_once))
    def _():
        each_send((1, 2), start_send)
        each_send((0,), start_send)

    @pl.when(mine)
    def _():
        for which in range(3):
            own_copy(which).start()

    def spread(place, source, far):
        if far == 0:
            sends, recvs, where = g_send.at[source, 0], g_recv.at[source, 0], (e, partner)
        else:
            there = lax.rem(y + far, y_count)
            sends, recvs = g_send.at[source, far], g_recv.at[source, far]
            where = (e, there * 2 + c)
        return remote(place, place, sends, recvs, where)

    def hand_out(source):
        place = xbuf.at[t, source]
        for far in range(1, y_count):
            spread(place, source, far).start()
        spread(place, source, 0).start()

    hand_out(e)
    hand_out(across)

    def arrive_slots(j, carry):
        for source in (near(j), lax.rem(near(j) + half_count, ep_count)):
            place = xbuf.at[t, source]
            remote(
                place, place, d_send.at[source], d_recv.at[source], (e, partner)
            ).wait_recv()
            hand_out(source)
        return carry

    lax.fori_loop(1, half_count, arrive_slots, 0)

    def relay(source, far, core):
        from_y = lax.rem(y + y_count - far, y_count)
        place = xbuf.at[from_y * 2 + core, source]
        return remote(
            place, place, h_send.at[source, far - 1], h_recv.at[source, far - 1], (e, partner)
        )

    def arrive_far(j, carry):
        for source in (near(j), lax.rem(near(j) + half_count, ep_count)):
            for far in range(1, y_count):
                from_y = lax.rem(y + y_count - far, y_count)
                spread(xbuf.at[from_y * 2 + c, source], source, far).wait_recv()
                relay(source, far, c).start()
        return carry

    lax.fori_loop(0, half_count, arrive_far, 0)

    def arrive_relay(j, carry):
        source = lax.rem(e + j, ep_count)
        spread(xbuf.at[partner, source], source, 0).wait_recv()
        for far in range(1, y_count):
            relay(source, far, 1 - c).wait_recv()
        return carry

    lax.fori_loop(0, ep_count, arrive_relay, 0)

    for copy in weight_copies[3:6]:
        copy.wait()
    rows_in = xbuf[...].reshape(tp_count * slots, xbuf.shape[3])
    gate_part = jnp.dot(rows_in, gate_ref[...], preferred_element_type=jnp.float32)
    up_part = jnp.dot(rows_in, up_ref[...], preferred_element_type=jnp.float32)
    hidden[...] = (
        (gate_part / (1.0 + jnp.exp(-gate_part)) * up_part).astype(jnp.bfloat16)
    ).reshape(hidden.shape)

    def down_part(core, into):
        rows = jnp.concatenate([hidden[v * 2 + core] for v in range(y_count)], axis=0)
        product = jnp.dot(rows, down_ref[...], preferred_element_type=jnp.float32)
        product = product.astype(jnp.bfloat16)
        for v in range(y_count):
            into[v, own_rows:, :] = product[v * slots : (v + 1) * slots]

    down_part(1 - c, pair_out)
    near_copy = remote(pair_out, pair_in, p_sem.at[0], p_sem.at[1], (e, partner))
    near_copy.start()
    down_part(c, pair_own)
    near_copy.wait()
    pair_own[...] = (
        pair_own[...].astype(jnp.float32) + pair_in[...].astype(jnp.float32)
    ).astype(jnp.bfloat16)

    def far_copy(step):
        target = lax.rem(y + step, y_count)
        return remote(
            pair_own.at[target],
            far_in.at[step - 1],
            y_send.at[step - 1],
            y_recv.at[step - 1],
            (e, target * 2 + c),
        )

    for step in range(1, y_count):
        far_copy(step).start()

    def arrived(which, source):
        own = jnp.logical_and(source == e, mine)

        @pl.when(own)
        def _():
            own_copy(which).wait()

        @pl.when(jnp.logical_not(own))
        def _():
            place = landing(which, c, source)
            remote(
                place, place, f_send.at[0, source], s_recv.at[which, source], (e, partner)
            ).wait_recv()

    def arrive(j, carry):
        source = lax.rem(e + j, ep_count)
        for which in (1, 2):
            arrived(which, source)
            forward(which, source).start()
        return carry

    lax.fori_loop(0, ep_count, arrive, 0)

    def give_back(target):
        return remote(
            ret_out.at[target], ret_in.at[place_me], v_send.at[target], v_recv.at[place_me], (target, t)
        )

    def give_relay(target):
        beyond = lax.rem(target + half_count, ep_count)
        return remote(
            ret_out.at[beyond], gathered.at[place_me], u_send.at[target], u_recv.at[place_me], (target, t)
        )

    def finish_experts():
        for step in range(1, y_count):
            far_copy(step).wait_recv()
        expert_sum = pair_own[y].astype(jnp.float32)
        for step in range(1, y_count):
            expert_sum = expert_sum + far_in[step - 1].astype(jnp.float32)
        shared_sum[...] = expert_sum[:own_rows]
        ret_out[...] = expert_sum[own_rows:].astype(jnp.bfloat16).reshape(ret_out.shape)

        def start_back(j, carry):
            give_relay(near(j)).start()
            give_back(near(j)).start()
            return carry

        lax.fori_loop(1, half_count, start_back, 0)
        gathered[place_me] = ret_out[across]
        ret_in[place_me] = ret_out[e]

    def arrive_forward(j, carry):
        source = lax.rem(e + j, ep_count)
        for which in (1, 2):
            place = landing(which, 1 - c, source)
            remote(
                place,
                place,
                f_send.at[which - 1, source],
                f_recv.at[which - 1, source],
                (e, partner),
            ).wait_recv()
        return carry

    lax.fori_loop(0, ep_count, arrive_forward, 0)
    lam_copy.wait()
    small_copies[6].wait()

    lam = jnp.where(mine, lam_own[...], lam_other[...])[0:1, 0:1]
    gain = gain_ref[...]
    factor = head_dim ** (-0.5) * log2_e

    def back_place(v):
        return heads.at[h_me, v, c]

    def back_copy(target, v):
        return remote(
            obuf.at[target, v],
            back_place(v),
            o_send.at[target, v],
            o_recv.at[h_me, v, c],
            (target, y * 2 + s_me),
        )

    def back_own(v):
        return pltpu.make_async_copy(obuf.at[e, v], back_place(v), o_recv.at[h_me, v, c])

    def attend(v, at, first):
        targets = (at * 2, at * 2 + 1)

        @pl.when(first)
        def _():
            for target in targets:
                arrived(0, target)

        rows = pl.ds(pl.multiple_of(v * share, share), share)
        block = jnp.concatenate([qbuf[target, rows, :] for target in targets], axis=0)
        ratios = []
        for m in range(2):
            columns = slice(m * head_dim, (m + 1) * head_dim)
            scores = lax.dot_general(
                block[:, columns],
                kbuf[:, columns],
                (((1,), (1,)), ((), ())),
                preferred_element_type=jnp.float32,
            )
            top = jnp.max(scores, axis=-1, keepdims=True)
            weights = jnp.exp2((scores - top) * factor)
            denominator = jnp.sum(weights, axis=-1, keepdims=True)
            weighted = jnp.dot(
                weights.astype(jnp.bfloat16), vbuf[...], preferred_element_type=jnp.float32
            )
            ratios.append(weighted / denominator)
        mixed = ratios[0] - lam * ratios[1]
        mean_square = jnp.mean(mixed * mixed, axis=-1, keepdims=True)
        done = (mixed * lax.rsqrt(mean_square + head_eps) * gain).astype(jnp.bfloat16)
        for k, target in enumerate(targets):
            obuf[target, v] = done[k * share : (k + 1) * share]
        for target in targets:
            own = jnp.logical_and(target == e, mine)

            @pl.when(jnp.logical_not(own))
            def _():
                back_copy(target, v).start()

            @pl.when(own)
            def _():
                back_own(v).start()

    pair_first = s_me * near_pairs

    def beyond_pair(k):
        return (1 - s_me) * (pair_count - 1 - k) + s_me * k

    def near_pair(k):
        return pair_first + lax.rem(pair_me + k, near_pairs)

    def attend_rows(j, carry):
        v = lax.rem(y + 1 + j, y_count)
        attend(v, beyond_pair(0), j == 0)
        for k in range(near_pairs):
            attend(v, near_pair(k), j == 0)
        pl.when(j == 0)(finish_experts)
        for k in range(1, near_pairs):
            attend(v, beyond_pair(k), j == 0)
        return carry

    lax.fori_loop(0, y_count, attend_rows, 0)

    def arrive_gathered(j, carry):
        place = gathered.at[lax.rem(place_me + j, half_count)]
        remote(
            place, place, u_send.at[near(j)], u_recv.at[lax.rem(place_me + j, half_count)], (e, partner)
        ).wait_recv()
        return carry

    lax.fori_loop(1, half_count, arrive_gathered, 0)
    all_gathered = gathered[...].reshape(half_slots, model)
    cross_mix = ext_in[:, model:]
    part = jnp.dot(cross_mix[:, :half_slots], all_gathered, preferred_element_type=jnp.float32)
    part = part + jnp.dot(
        cross_mix[:, half_slots:], all_gathered, preferred_element_type=jnp.float32
    )
    part_out[...] = part.astype(jnp.bfloat16)
    part_copy = remote(part_out, part_in, m_sem.at[0], m_sem.at[1], (across, t))
    part_copy.start()

    weight_copies[6].wait()

    def pair_copy(at):
        return remote(sum_out.at[at], sum_in.at[at], r_send.at[at], r_recv.at[at], (e, partner))

    def project(at):
        v = lax.rem(y + 1 + at, y_count)

        def arrive_heads(h, carry):
            for side in range(2):
                own = jnp.logical_and(
                    jnp.logical_and(c * head_count + h == e, side == c), h == h_me
                )
                place = heads.at[h, v, side]

                @pl.when(own)
                def _():
                    back_own(v).wait()

                @pl.when(jnp.logical_not(own))
                def _():
                    remote(
                        place, place, o_send.at[0, 0], o_recv.at[h, v, side], (e, partner)
                    ).wait_recv()

            return carry

        lax.fori_loop(0, head_count, arrive_heads, 0)
        total = None
        for h in range(head_count):
            rows = jnp.concatenate([heads[h, v, 1 - c], heads[h, v, c]], axis=0)
            term = jnp.dot(
                rows,
                proj_ref[h * width : (h + 1) * width, :],
                preferred_element_type=jnp.float32,
            )
            total = term if total is None else total + term
        total = total.astype(jnp.bfloat16)
        sum_out[at] = total[:share]
        kept[at] = total[share:]
        pair_copy(at).start()

    def block_copy(step):
        target = lax.rem(y + step, y_count)
        return remote(
            block_out.at[step - 1],
            block_in.at[step - 1],
            b_send.at[step - 1],
            b_recv.at[step - 1],
            (e, target * 2 + c),
        )

    for step in range(1, y_count):
        project(step - 1)
        pair_copy(step - 1).wait()
        block_out[step - 1] = (
            kept[step - 1].astype(jnp.float32) + sum_in[step - 1].astype(jnp.float32)
        ).astype(jnp.bfloat16)
        block_copy(step).start()
    project(y_count - 1)

    def arrive_back(j, carry):
        at = lax.rem(place_me + j, half_count)
        place = ret_in.at[at]
        remote(place, place, v_send.at[near(j)], v_recv.at[at], (e, partner)).wait_recv()
        return carry

    lax.fori_loop(1, half_count, arrive_back, 0)
    wide = mix_ref[own_span, :]
    mix = jnp.where(s_me == 0, wide[:, :half_slots], wide[:, half_slots:])
    coarse = mix.astype(jnp.bfloat16)
    fine = (mix - coarse.astype(jnp.float32)).astype(jnp.bfloat16)
    returned = ret_in[...].reshape(half_slots, model)
    combined = jnp.dot(coarse, returned, preferred_element_type=jnp.float32)
    combined = combined + jnp.dot(fine, returned, preferred_element_type=jnp.float32)
    shared_sum[...] = shared_sum[...] + combined

    pair_copy(y_count - 1).wait()
    total = (
        kept[y_count - 1].astype(jnp.float32) + sum_in[y_count - 1].astype(jnp.float32)
    ).astype(jnp.bfloat16)
    total = total.astype(jnp.float32)
    for step in range(1, y_count):
        block_copy(step).wait()
        total = total + block_in[step - 1].astype(jnp.float32)
    out_ref[...] = total.astype(jnp.bfloat16)
    part_copy.wait()
    moe_ref[...] = (shared_sum[...] + part_in[...].astype(jnp.float32)).astype(jnp.bfloat16)

    def end_send(whiches, h, side, own):
        @pl.when(jnp.logical_not(own))
        def _():
            for which in whiches:
                first_copy(which, h, side).wait_send()

    each_send((0, 1, 2), end_send)

    for step in range(1, y_count):
        far_copy(step).wait_send()

    def end_rest(source, carry):
        for far in range(y_count):
            spread(xbuf.at[t, source], source, far).wait_send()
        for far in range(1, y_count):
            relay(source, far, c).wait_send()

        for which in (1, 2):
            forward(which, source).wait_send()

        @pl.when(jnp.logical_not(jnp.logical_and(source == e, mine)))
        def _():
            for v in range(y_count):
                back_copy(source, v).wait_send()

        return carry

    lax.fori_loop(0, ep_count, end_rest, 0)

    def end_near(j, carry):
        dispatch(near(j)).wait_send()
        pass_on(j).wait_send()
        give_back(near(j)).wait_send()
        give_relay(near(j)).wait_send()
        return carry

    lax.fori_loop(1, half_count, end_near, 0)
    cross_copy.wait_send()


def mixer(
    tables,
    sequence,
    lambdas,
    head_gain,
    out_proj,
    moe_inputs,
    expert_weights,
    ep_count,
    tp_count,
    capacity,
):
    moe_input, moe_gain, routes, route_weights = moe_inputs
    head_count = lambdas.shape[0]
    half = sequence[0].shape[0] // 2
    width = sequence[0].shape[1] // head_count
    slots = ep_count * capacity
    batch_rows, model = moe_input.shape
    own_rows = batch_rows // tp_count
    top_count = routes.shape[1]
    hidden_width = expert_weights[0].shape[2]
    shared_width = expert_weights[3].shape[1]
    tokens = ep_count * 2 * half
    share = 2 * half // tp_count
    y_count = tp_count // 2
    dma = pltpu.SemaphoreType.DMA
    bf16 = jnp.bfloat16
    return pl.pallas_call(
        functools.partial(mixer_kernel, ep_count, tp_count),
        out_shape=(
            pltpu.VMEM((share, model), bf16),
            pltpu.VMEM((own_rows, model), bf16),
        ),
        in_specs=[pl.BlockSpec(memory_space=pltpu.SMEM)]
        + [pl.BlockSpec(memory_space=pltpu.HBM)] * 17,
        out_specs=[pl.BlockSpec(memory_space=pltpu.VMEM)] * 2,
        scratch_shapes=[
            pltpu.VMEM(tables[0].shape, jnp.float32),
            pltpu.VMEM(tables[1].shape, jnp.float32),
            pltpu.VMEM(tables[0].shape[1:], jnp.float32),
            pltpu.VMEM(tables[0].shape[1:], jnp.float32),
            pltpu.VMEM((1, width), jnp.float32),
            pltpu.VMEM((1, model), jnp.float32),
            pltpu.VMEM((top_count, batch_rows), jnp.int32),
            pltpu.VMEM((top_count, batch_rows), jnp.float32),
            pltpu.VMEM((batch_rows, model), bf16),
            dma((7,)),
            pltpu.VMEM((batch_rows, model), bf16),
            pltpu.VMEM((slots, model), bf16),
            pltpu.VMEM((batch_rows, slots), jnp.float32),
            pltpu.VMEM((own_rows, model + slots), bf16),
            pltpu.VMEM((own_rows, model + slots), bf16),
            pltpu.VMEM((slots // 2, model), bf16),
            pltpu.VMEM((ep_count // 2, capacity, model), bf16),
            pltpu.VMEM((own_rows, model), bf16),
            pltpu.VMEM((own_rows, model), bf16),
            pltpu.VMEM((3,) + sequence[0].shape, bf16),
            pltpu.VMEM((3, head_count, 2, half, width), bf16),
            dma((3,)),
            pltpu.VMEM(out_proj.shape, bf16),
            pltpu.VMEM((model, hidden_width), bf16),
            pltpu.VMEM((model, hidden_width), bf16),
            pltpu.VMEM((hidden_width, model), bf16),
            pltpu.VMEM((model, shared_width), bf16),
            pltpu.VMEM((model, shared_width), bf16),
            pltpu.VMEM((shared_width, model), bf16),
            pltpu.VMEM((tp_count, ep_count, capacity, model), bf16),
            pltpu.VMEM((tp_count, slots, hidden_width), bf16),
            pltpu.VMEM((y_count, own_rows + slots, model), bf16),
            pltpu.VMEM((y_count, own_rows + slots, model), bf16),
            pltpu.VMEM((y_count, own_rows + slots, model), bf16),
            pltpu.VMEM((max(1, y_count - 1), own_rows + slots, model), bf16),
            pltpu.VMEM((own_rows, model), jnp.float32),
            pltpu.VMEM((ep_count, capacity, model), bf16),
            pltpu.VMEM((ep_count // 2, capacity, model), bf16),
            dma((7,)),
            dma((ep_count,)),
            dma((ep_count,)),
            dma((2,)),
            dma((ep_count // 2,)),
            dma((ep_count,)),
            dma((ep_count // 2,)),
            dma((2,)),
            dma((ep_count, y_count)),
            dma((ep_count, y_count)),
            dma((ep_count, max(1, y_count - 1))),
            dma((ep_count, max(1, y_count - 1))),
            dma((2,)),
            dma((max(1, y_count - 1),)),
            dma((max(1, y_count - 1),)),
            dma((ep_count,)),
            dma((ep_count,)),
            pltpu.VMEM((ep_count, half, width), bf16),
            pltpu.VMEM((tokens, width), bf16),
            pltpu.VMEM((tokens, width), bf16),
            pltpu.VMEM((8, 128), jnp.float32),
            pltpu.VMEM((8, 128), jnp.float32),
            pltpu.VMEM((ep_count, y_count, share, width), bf16),
            pltpu.VMEM((head_count, y_count, 2, share, width), bf16),
            pltpu.VMEM((y_count, share, model), bf16),
            pltpu.VMEM((y_count, share, model), bf16),
            pltpu.VMEM((y_count, share, model), bf16),
            pltpu.VMEM((max(1, y_count - 1), share, model), bf16),
            pltpu.VMEM((max(1, y_count - 1), share, model), bf16),
            dma((3, head_count, 2)),
            dma((3, ep_count)),
            dma((3,)),
            dma((2, ep_count)),
            dma((2, ep_count)),
            dma((2,)),
            dma((ep_count, y_count)),
            dma((head_count, y_count, 2)),
            dma((y_count,)),
            dma((y_count,)),
            dma((max(1, y_count - 1),)),
            dma((max(1, y_count - 1),)),
        ],
        compiler_params=pltpu.CompilerParams(
            has_side_effects=True, vmem_limit_bytes=62000000, collective_id=0
        ),
        name="mixer",
    )(
        lambdas,
        *tables,
        head_gain[None, :],
        moe_gain[None, :],
        jnp.transpose(routes),
        jnp.transpose(route_weights),
        moe_input,
        *sequence,
        out_proj,
        *expert_weights,
    )


def local(
    queries,
    key_rows,
    value_rows,
    lambdas,
    head_gain,
    out_proj,
    moe_input,
    moe_gain,
    routes,
    route_weights,
    expert_gate,
    expert_up,
    expert_down,
    shared_gate,
    shared_up,
    shared_down,
):
    query_rows = queries.shape[0]
    head_count = lambdas.shape[0]
    head_dim = queries.shape[1] // (2 * head_count)
    tp_count = lax.axis_size("tp")
    ep_count = lax.axis_size("ep")
    tp_place = lax.axis_index("tp")
    ep_place = lax.axis_index("ep")
    positions = ep_place * query_rows + jnp.arange(query_rows, dtype=jnp.int32)
    batch_rows = moe_input.shape[0]
    top_count = routes.shape[1]
    own_rows = batch_rows // tp_count
    local_experts = expert_gate.shape[0]
    expert_count = local_experts * ep_count
    capacity = (2 * own_rows * top_count + expert_count - 1) // expert_count
    one_head_each = ep_count == 2 * head_count and tp_count % 2 == 0 and local_experts == 1 and ep_count % 4 == 0 and expert_count * capacity % 128 == 0
    if one_head_each:
        tables = rotation_tables(query_rows, ep_count, head_dim)
        sequence = (queries, key_rows, value_rows)
        weights = (expert_gate, expert_up, expert_down, shared_gate, shared_up, shared_down)
        return mixer(
            tables,
            sequence,
            lambdas,
            head_gain,
            out_proj,
            (moe_input, moe_gain, routes, route_weights),
            weights,
            ep_count,
            tp_count,
            capacity,
        )
    else:
        rot_query = rotate(queries, positions, head_dim)
        rot_keys = rotate(key_rows, positions, head_dim)
        initial = (
            jnp.full((head_count, 2, query_rows), -1e30, jnp.float32),
            jnp.zeros((head_count, 2, query_rows), jnp.float32),
            jnp.zeros((head_count, 2, query_rows, 2 * head_dim), jnp.float32),
        )
        running_max, denominator, numerator = fold_keys(
            initial,
            (
                lax.all_gather(rot_keys, "ep", axis=0, tiled=True),
                lax.all_gather(value_rows, "ep", axis=0, tiled=True),
            ),
            rot_query,
            head_count,
            head_dim,
        )
        ratio = numerator / denominator[..., None]
        mixed_heads = ratio[:, 0] - lambdas[:, None, None] * ratio[:, 1]
        mean_square = jnp.mean(mixed_heads * mixed_heads, axis=-1, keepdims=True)
        normed_heads = (mixed_heads * lax.rsqrt(mean_square + head_eps) * head_gain).astype(
            jnp.bfloat16
        )
        head_out = jnp.transpose(normed_heads, (1, 0, 2)).reshape(query_rows, head_count * 2 * head_dim)
    normed = rms_rows(moe_input, moe_gain)
    shared_hidden = gated_hidden(normed, shared_gate, shared_up)
    own_routes = lax.dynamic_slice_in_dim(routes, tp_place * own_rows, own_rows, 0)
    own_weights = lax.dynamic_slice_in_dim(route_weights, tp_place * own_rows, own_rows, 0)
    own_source, own_filled, own_rank = slot_table(own_routes, expert_count, capacity)
    own_normed = lax.dynamic_slice_in_dim(normed, tp_place * own_rows, own_rows, 0)
    outgoing = fill_slots(own_normed, own_source, own_filled)
    arrived = lax.all_to_all(outgoing[:, None], "ep", split_axis=0, concat_axis=2, tiled=True)
    hidden = slot_hidden(lax.all_gather(arrived, "tp", axis=1, tiled=True), expert_gate, expert_up)
    slot_rows = local_experts * ep_count * capacity
    mixer_share = query_rows // tp_count
    expert_share = own_rows + slot_rows
    if not one_head_each:
        block_count = lax.axis_size("tp") * mixer_share // mixer_share
        product = jnp.dot(head_out, out_proj, preferred_element_type=jnp.float32)
        mixer_out = lax.psum_scatter(
            product.reshape(block_count, mixer_share, -1)
            .reshape(lax.axis_size("tp") * mixer_share, -1)
            .astype(jnp.bfloat16),
            "tp",
            scatter_dimension=0,
            tiled=True,
        )
    block_count = lax.axis_size("tp") * expert_share // expert_share
    shared_part = jnp.dot(shared_hidden, shared_down, preferred_element_type=jnp.float32).reshape(
        block_count, own_rows, -1
    )
    routed_part = jnp.einsum(
        "xnsf,xfd->nxsd", hidden, expert_down, preferred_element_type=jnp.float32
    )
    routed_part = routed_part.reshape(block_count, slot_rows, -1)
    expert_sum = lax.psum_scatter(
        jnp.concatenate([shared_part, routed_part], axis=1)
        .reshape(lax.axis_size("tp") * expert_share, -1)
        .astype(jnp.bfloat16),
        "tp",
        scatter_dimension=0,
        tiled=True,
    ).astype(jnp.float32)
    shared_sum = expert_sum[:own_rows]
    routed = (
        expert_sum[own_rows:].reshape(local_experts, ep_count * capacity, -1).astype(jnp.bfloat16)
    )
    returned = lax.all_to_all(routed, "ep", split_axis=1, concat_axis=0, tiled=True)
    flat_index = (own_routes * capacity + own_rank).reshape(-1)
    picked = jnp.take(returned.reshape(expert_count * capacity, -1), flat_index, axis=0).reshape(
        own_rows, top_count, -1
    )
    combined = shared_sum + jnp.sum(own_weights[..., None] * picked.astype(jnp.float32), axis=1)
    return (mixer_out, combined.astype(jnp.bfloat16))


def solution(mesh):
    in_specs = (
        P("ep", "tp"),
        P("ep", "tp"),
        P("ep", "tp"),
        P("tp"),
        P(),
        P("tp", None),
        P("ep", None),
        P(),
        P("ep", None),
        P("ep", None),
        P("ep", None, "tp"),
        P("ep", None, "tp"),
        P("ep", "tp", None),
        P(None, "tp"),
        P(None, "tp"),
        P("tp", None),
    )
    out_specs = (P(("ep", "tp"), None), P(("ep", "tp"), None))
    return jax.shard_map(local, mesh=mesh, in_specs=in_specs, out_specs=out_specs, check_vma=False)
```

```python
import functools
import jax
import jax.numpy as jnp
import numpy as np
from jax import lax
from jax.experimental import pallas as pl
from jax.experimental.pallas import tpu as pltpu
from jax.sharding import PartitionSpec as P

theta_base = 500000.0
norm_eps = 1e-06
head_eps = 1e-05
MESH = pl.DeviceIdType.MESH
log2_e = 1.4426950408889634


def rotate(matrix, positions, head_dim):
    row_count = matrix.shape[0]
    shaped = matrix.reshape(row_count, -1, head_dim).astype(jnp.float32)
    half_dim = head_dim // 2
    frequency = jnp.power(theta_base, -jnp.arange(half_dim, dtype=jnp.float32) * 2.0 / head_dim)
    angles = positions.astype(jnp.float32)[:, None] * frequency[None, :]
    cosine = jnp.cos(angles)[:, None, :]
    sines = jnp.sin(angles)[:, None, :]
    front_half = shaped[..., :half_dim]
    second = shaped[..., half_dim:]
    turned = jnp.concatenate(
        [front_half * cosine - second * sines, second * cosine + front_half * sines], axis=-1
    )
    return turned.reshape(matrix.shape).astype(jnp.bfloat16)


def rms_rows(values, gain):
    widened = values.astype(jnp.float32)
    mean_square = jnp.mean(widened * widened, axis=-1, keepdims=True)
    return (widened * lax.rsqrt(mean_square + norm_eps) * gain).astype(jnp.bfloat16)


def gated_hidden(rows_in, gate_weight, up_weight):
    gate_part = jnp.dot(rows_in, gate_weight, preferred_element_type=jnp.float32)
    up_part = jnp.dot(rows_in, up_weight, preferred_element_type=jnp.float32)
    return (jax.nn.silu(gate_part) * up_part).astype(jnp.bfloat16)


def slot_hidden(slot_rows, gate_weight, up_weight):
    gate_part = jnp.einsum(
        "xnsd,xdf->xnsf", slot_rows, gate_weight, preferred_element_type=jnp.float32
    )
    up_part = jnp.einsum("xnsd,xdf->xnsf", slot_rows, up_weight, preferred_element_type=jnp.float32)
    return (jax.nn.silu(gate_part) * up_part).astype(jnp.bfloat16)


def key_block_size(piece_rows):
    for candidate in (1024, 512):
        return candidate
    return piece_rows


def fold_keys(state_in, pieces, rot_query, head_count, head_dim):
    keys_piece, values_piece = pieces
    piece_rows = keys_piece.shape[0]
    block_rows = key_block_size(piece_rows)
    block_count = piece_rows // block_rows
    query_view = rot_query.reshape(rot_query.shape[0], head_count, 2, head_dim)
    score_scale = head_dim ** (-0.5)

    def one_block(running, key_block):
        running_max, denominator, numerator = running
        key_view = key_block[0].reshape(block_rows, head_count, 2, head_dim)
        value_view = key_block[1].reshape(block_rows, head_count, 2 * head_dim)
        scores = (
            jnp.einsum("qhmd,khmd->hmqk", query_view, key_view, preferred_element_type=jnp.float32)
            * score_scale
        )
        newest = jnp.maximum(running_max, jnp.max(scores, axis=-1))
        weights = jnp.exp(scores - newest[..., None])
        shrink = jnp.exp(running_max - newest)
        denominator = denominator * shrink + jnp.sum(weights, axis=-1)
        weighted = jnp.einsum(
            "hmqk,khe->hmqe",
            weights.astype(jnp.bfloat16),
            value_view,
            preferred_element_type=jnp.float32,
        )
        numerator = numerator * shrink[..., None] + weighted
        return ((newest, denominator, numerator), None)

    blocks = (
        keys_piece.reshape(block_count, block_rows, -1),
        values_piece.reshape(block_count, block_rows, -1),
    )
    result, _ = lax.scan(one_block, state_in, blocks)
    return result


def slot_table(route_block, expert_count, capacity):
    flat_routes = route_block.reshape(-1)
    route_total = flat_routes.shape[0]
    top_count = route_block.shape[1]
    experts_iota = jnp.arange(expert_count, dtype=jnp.int32)
    onehot = (flat_routes[:, None] == experts_iota[None, :]).astype(jnp.int32)
    before = jnp.cumsum(onehot, axis=0) - onehot
    slot_rank = jnp.sum(before * onehot, axis=1)
    slot_iota = jnp.arange(capacity, dtype=jnp.int32)
    matches = (flat_routes[None, None, :] == experts_iota[:, None, None]) & (
        slot_rank[None, None, :] == slot_iota[None, :, None]
    )
    source_row = jnp.arange(route_total, dtype=jnp.int32) // top_count
    source = jnp.sum(jnp.where(matches, source_row[None, None, :], 0), axis=2)
    filled = jnp.any(matches, axis=2)
    return (source, filled, slot_rank.reshape(route_block.shape))


def fill_slots(rows_src, source, filled):
    taken = jnp.take(rows_src, source.reshape(-1), axis=0).reshape(
        source.shape + (rows_src.shape[1],)
    )
    return jnp.where(filled[..., None], taken, jnp.zeros_like(taken))


def rotation_tables(row_count, block_count, head_dim):
    half_dim = head_dim // 2
    frequency = np.power(theta_base, -np.arange(half_dim) * 2.0 / head_dim)

    def table(positions):
        angles = positions[:, None] * frequency[None, :]
        cosine, sines = np.cos(angles), np.sin(angles)
        both = (np.concatenate([cosine, cosine], 1), np.concatenate([-sines, sines], 1))
        return np.stack(both).astype(np.float32)

    return (
        jnp.asarray(table(np.arange(row_count))),
        jnp.asarray(table(np.arange(block_count) * row_count)),
    )


def mixer_kernel(
    ep_count,
    tp_count,
    lam_hbm,
    turn_hbm,
    base_hbm,
    gain_hbm,
    mgain_hbm,
    routes_hbm,
    scale_hbm,
    rows_hbm,
    q_hbm,
    k_hbm,
    v_hbm,
    proj_hbm,
    gate_hbm,
    up_hbm,
    down_hbm,
    sgate_hbm,
    sup_hbm,
    sdown_hbm,
    out_ref,
    moe_ref,
    lam_ref,
    turn_ref,
    base_ref,
    cos_ref,
    sin_ref,
    gain_ref,
    mgain_ref,
    routes_ref,
    scale_ref,
    rows_ref,
    small_sem,
    norm_ref,
    slot_ref,
    mix_ref,
    ext_out,
    ext_in,
    rel_slots,
    gathered,
    part_out,
    part_in,
    raw,
    pack_ref,
    q_sem,
    proj_ref,
    gate_ref,
    up_ref,
    down_ref,
    sgate_ref,
    sup_ref,
    sdown_ref,
    xbuf,
    hidden,
    pair_out,
    pair_own,
    pair_in,
    far_in,
    shared_sum,
    ret_out,
    ret_in,
    w_sem,
    d_send,
    d_recv,
    c_sem,
    k_send,
    u_send,
    u_recv,
    m_sem,
    g_send,
    g_recv,
    h_send,
    h_recv,
    p_sem,
    y_send,
    y_recv,
    v_send,
    v_recv,
    qbuf,
    kbuf,
    vbuf,
    lam_own,
    lam_other,
    obuf,
    heads,
    sum_out,
    sum_in,
    kept,
    block_out,
    block_in,
    s_send,
    s_recv,
    s_local,
    f_send,
    f_recv,
    l_sem,
    o_send,
    o_recv,
    r_send,
    r_recv,
    b_send,
    b_recv,
):
    head_count = pack_ref.shape[1]
    half, width = pack_ref.shape[3], pack_ref.shape[4]
    head_dim = width // 2
    e = lax.axis_index("ep")
    t = lax.axis_index("tp")
    y, c = t // 2, lax.rem(t, 2)
    partner = y * 2 + 1 - c
    s_me, h_me = e // head_count, lax.rem(e, head_count)
    y_count = tp_count // 2
    share = half // y_count

    barrier = pltpu.get_barrier_semaphore()

    def greet(where):
        pl.semaphore_signal(barrier, inc=1, device_id=where, device_id_type=MESH)

    def greet_row(j, carry):
        there = lax.rem(e + j, ep_count)
        for core in range(2):
            greet((there, y * 2 + core))
        return carry

    lax.fori_loop(1, ep_count, greet_row, 0)
    greet((e, partner))
    for step in range(1, y_count):
        greet((e, lax.rem(y + step, y_count) * 2 + c))

    def remote(src, dst, send, recv, where):
        return pltpu.make_async_remote_copy(
            src_ref=src,
            dst_ref=dst,
            send_sem=send,
            recv_sem=recv,
            device_id=where,
            device_id_type=MESH,
        )

    small_copies = [
        pltpu.make_async_copy(a, b, small_sem.at[at])
        for at, (a, b) in enumerate(
            (
                (routes_hbm, routes_ref),
                (scale_hbm, scale_ref),
                (mgain_hbm, mgain_ref),
                (lam_hbm, lam_ref),
                (rows_hbm, rows_ref),
                (base_hbm, base_ref),
                (turn_hbm, turn_ref),
                (gain_hbm, gain_ref),
            )
        )
    ]
    for copy in small_copies:
        copy.start()
    raw_copies = [
        pltpu.make_async_copy(ref, raw.at[at], q_sem.at[at])
        for at, ref in enumerate((q_hbm, k_hbm, v_hbm))
    ]
    for copy in raw_copies:
        copy.start()
    weight_copies = [
        pltpu.make_async_copy(a, b, w_sem.at[at])
        for at, (a, b) in enumerate(
            (
                (sgate_hbm, sgate_ref),
                (sup_hbm, sup_ref),
                (sdown_hbm, sdown_ref),
                (gate_hbm.at[0], gate_ref),
                (up_hbm.at[0], up_ref),
                (down_hbm.at[0], down_ref),
                (proj_hbm, proj_ref),
            )
        )
    ]
    def landing(which, side, source):
        if which == 0:
            return qbuf.at[source]
        return (kbuf, vbuf)[which - 1].at[pl.ds((side * ep_count + source) * half, half)]

    def first_copy(which, h, side):
        return remote(
            pack_ref.at[which, h, side],
            landing(which, side, e),
            s_send.at[which, h, side],
            s_recv.at[which, e],
            (c * head_count + h, y * 2 + side),
        )

    def own_copy(which):
        return pltpu.make_async_copy(
            pack_ref.at[which, h_me, c], landing(which, c, e), s_local.at[which]
        )

    def forward(which, source):
        place = landing(which, c, source)
        return remote(
            place, place, f_send.at[which - 1, source], f_recv.at[which - 1, source], (e, partner)
        )

    capacity = xbuf.shape[2]
    own_rows = moe_ref.shape[0]
    slots = ep_count * capacity
    batch_rows = rows_ref.shape[0]
    model = rows_ref.shape[1]
    half_count = ep_count // 2
    half_slots = half_count * capacity
    across = lax.rem(e + half_count, ep_count)
    near_first = s_me * half_count
    place_me = lax.rem(e, half_count)

    def near(j):
        return near_first + lax.rem(place_me + j, half_count)

    for copy in small_copies[:5]:
        copy.wait()
    widened = rows_ref[...].astype(jnp.float32)
    mean_square = jnp.mean(widened * widened, axis=-1, keepdims=True)
    norm_ref[...] = (widened * lax.rsqrt(mean_square + norm_eps) * mgain_ref[...]).astype(
        jnp.bfloat16
    )
    slot_at = lax.broadcasted_iota(jnp.int32, (slots, batch_rows), 0)
    slot_expert, slot_rank = slot_at // capacity, lax.rem(slot_at, capacity)
    hits = [routes_ref[k : k + 1, :] == slot_expert for k in range(routes_ref.shape[0])]
    named = sum(hit.astype(jnp.float32) for hit in hits).astype(jnp.bfloat16)
    other_at = lax.broadcasted_iota(jnp.int32, (batch_rows, batch_rows), 0)
    row_at = lax.broadcasted_iota(jnp.int32, (batch_rows, batch_rows), 1)
    earlier = jnp.logical_and(other_at < row_at, other_at // own_rows == row_at // own_rows)
    before = jnp.dot(
        named, earlier.astype(jnp.float32).astype(jnp.bfloat16), preferred_element_type=jnp.float32
    ).astype(jnp.int32)
    chosen = [jnp.logical_and(hit, before == slot_rank).astype(jnp.float32) for hit in hits]
    token_block = lax.broadcasted_iota(jnp.int32, (slots, batch_rows), 1) // own_rows
    picked = jnp.where(token_block == t, sum(chosen), 0.0).astype(jnp.bfloat16)
    slot_ref[...] = jnp.dot(
        picked, norm_ref[...], preferred_element_type=jnp.float32
    ).astype(jnp.bfloat16)
    mixing = sum(scale_ref[k : k + 1, :] * chosen[k] for k in range(len(chosen)))
    mix_ref[...] = jnp.transpose(mixing)
    head_at = lax.broadcasted_iota(jnp.int32, lam_ref.shape, 1)
    lam_mine = jnp.sum(
        jnp.where(head_at == h_me, lam_ref[...], 0.0), axis=1, keepdims=True
    )
    lam_own[...] = jnp.broadcast_to(lam_mine, lam_own.shape)

    def fold(wide):
        return jnp.where(s_me == 0, wide[:, half_slots:], wide[:, :half_slots])

    own_span = pl.ds(pl.multiple_of(t * own_rows, own_rows), own_rows)
    away = fold(mix_ref[own_span, :])
    away_coarse = away.astype(jnp.bfloat16)
    away_fine = (away - away_coarse.astype(jnp.float32)).astype(jnp.bfloat16)
    ext_out[:, :model] = norm_ref[own_span, :]
    ext_out[:, model:] = jnp.concatenate([away_coarse, away_fine], axis=1)

    for copy in small_copies[5:7]:
        copy.wait()
    base_cos, base_sin = base_ref[0, pl.ds(e, 1), :], base_ref[1, pl.ds(e, 1), :]
    cos_ref[...] = base_cos * turn_ref[0] - base_sin * turn_ref[1]
    sin_ref[...] = base_sin * turn_ref[0] + base_cos * turn_ref[1]
    for copy in raw_copies:
        copy.wait()

    def pack_head(h, carry):
        cosine = cos_ref[...]
        sines = sin_ref[...]
        for which in range(2):
            for m in range(2):
                at = pl.multiple_of(h * width + m * head_dim, head_dim)
                part = raw[which, :, pl.ds(at, head_dim)].astype(jnp.float32)
                turned = part * cosine + pltpu.roll(part, head_dim // 2, 1) * sines
                turned = turned.astype(jnp.bfloat16)
                for v in range(y_count):
                    for side in range(2):
                        block = v * 2 + side
                        pack_ref[
                            which,
                            h,
                            side,
                            v * share : (v + 1) * share,
                            m * head_dim : (m + 1) * head_dim,
                        ] = turned[block * share : (block + 1) * share]
        at = pl.multiple_of(h * width, width)
        for v in range(y_count):
            for side in range(2):
                block = v * 2 + side
                pack_ref[2, h, side, v * share : (v + 1) * share] = raw[
                    2, block * share : (block + 1) * share, pl.ds(at, width)
                ]
        return carry

    lax.fori_loop(0, head_count, pack_head, 0)

    pl.semaphore_wait(barrier, (ep_count - 1) * 2 + 1 + (y_count - 1))

    for copy in weight_copies:
        copy.start()

    def dispatch(j):
        target, at = near(j), half_count - j
        rows = pl.ds(pl.multiple_of(target * capacity, capacity), capacity)
        return remote(
            slot_ref.at[rows], xbuf.at[t, at], d_send.at[target], d_recv.at[at], (target, t)
        )

    cross_copy = remote(ext_out, ext_in, c_sem.at[0], c_sem.at[1], (across, t))
    cross_copy.start()

    def start_dispatch(j, carry):
        dispatch(j).start()
        return carry

    lax.fori_loop(1, half_count, start_dispatch, 0)

    mine = s_me == c

    def each_send(whiches, act):
        def body(j, carry):
            h = lax.rem(h_me + 1 + j, head_count)
            for k in range(2):
                side = lax.rem(c + 1 + k, 2)
                own = jnp.logical_and(c * head_count + h == e, side == c)
                act(whiches, h, side, own)
            return carry

        lax.fori_loop(0, head_count, body, 0)

    def start_send(whiches, h, side, own):
        @pl.when(jnp.logical_not(own))
        def _():
            for which in whiches:
                first_copy(which, h, side).start()

    pair_count = ep_count // 2
    pair_me = e // 2
    near_pairs = pair_count // 2
    beside = jnp.logical_or(pair_me == near_pairs - 1, pair_me == near_pairs)
    at_once = jnp.logical_and(jnp.logical_not(mine), beside)

    @pl.when(at_once)
    def _():
        each_send((1, 2), start_send)
        each_send((0,), start_send)

    lam_copy = remote(lam_own, lam_other, l_sem.at[0], l_sem.at[1], (e, partner))
    lam_copy.start()
    xbuf[t, 0] = slot_ref[pl.ds(pl.multiple_of(e * capacity, capacity), capacity), :]

    def spread(place, source, far):
        if far == 0:
            sends, recvs, where = g_send.at[source, 0], g_recv.at[source, 0], (e, partner)
        else:
            there = lax.rem(y + far, y_count)
            sends, recvs = g_send.at[source, far], g_recv.at[source, far]
            where = (e, there * 2 + c)
        return remote(place, place, sends, recvs, where)

    def hand_out(source):
        place = xbuf.at[t, source]
        for far in range(1, y_count):
            spread(place, source, far).start()
        spread(place, source, 0).start()

    def relay(source, far, core):
        from_y = lax.rem(y + y_count - far, y_count)
        place = xbuf.at[from_y * 2 + core, source]
        return remote(
            place, place, h_send.at[source, far - 1], h_recv.at[source, far - 1], (e, partner)
        )

    def arrive_slots(at, carry):
        place = xbuf.at[t, at]
        remote(place, place, d_send.at[at], d_recv.at[at], (e, partner)).wait_recv()
        hand_out(at)
        return carry

    def arrive_far(source, carry):
        for far in range(1, y_count):
            from_y = lax.rem(y + y_count - far, y_count)
            spread(xbuf.at[from_y * 2 + c, source], source, far).wait_recv()
            relay(source, far, c).start()
        return carry

    def arrive_relay(source, carry):
        spread(xbuf.at[partner, source], source, 0).wait_recv()
        for far in range(1, y_count):
            relay(source, far, 1 - c).wait_recv()
        return carry

    hand_out(0)

    for copy in weight_copies[:3]:
        copy.wait()
    normed = norm_ref[...]
    gate_part = jnp.dot(normed, sgate_ref[...], preferred_element_type=jnp.float32)
    up_part = jnp.dot(normed, sup_ref[...], preferred_element_type=jnp.float32)
    shared_hidden = (gate_part / (1.0 + jnp.exp(-gate_part)) * up_part).astype(jnp.bfloat16)
    shared_part = jnp.dot(
        shared_hidden, sdown_ref[...], preferred_element_type=jnp.float32
    ).astype(jnp.bfloat16)
    for v in range(y_count):
        for core in range(2):
            block = shared_part[(v * 2 + core) * own_rows : (v * 2 + core + 1) * own_rows]

            @pl.when(c == core)
            def _():
                pair_own[v, :own_rows, :] = block

            @pl.when(c != core)
            def _():
                pair_out[v, :own_rows, :] = block

    lax.fori_loop(1, half_count, arrive_slots, 0)
    cross_copy.wait_recv()
    sent_rows = ext_in[:, :model]
    sent_mix = ext_in[:, model:]
    taken = (sent_mix[:, :half_slots].astype(jnp.float32) > 0.0).astype(jnp.float32)
    rel_slots[...] = lax.dot_general(
        taken.astype(jnp.bfloat16),
        sent_rows,
        (((0,), (0,)), ((), ())),
        preferred_element_type=jnp.float32,
    ).astype(jnp.bfloat16)

    def pass_on(j):
        to, at = lax.rem(place_me + j, half_count), half_count + (half_count - j)
        rows = pl.ds(pl.multiple_of(to * capacity, capacity), capacity)
        return remote(
            rel_slots.at[rows],
            xbuf.at[t, at],
            k_send.at[to],
            d_recv.at[at],
            (near_first + to, t),
        )

    def start_pass(j, carry):
        pass_on(j).start()
        return carry

    lax.fori_loop(1, half_count, start_pass, 0)
    xbuf[t, half_count] = rel_slots[
        pl.ds(pl.multiple_of(place_me * capacity, capacity), capacity), :
    ]

    @pl.when(jnp.logical_not(at_once))
    def _():
        each_send((1, 2), start_send)
        each_send((0,), start_send)

    @pl.when(mine)
    def _():
        for which in range(3):
            own_copy(which).start()

    hand_out(half_count)
    lax.fori_loop(0, half_count, arrive_far, 0)
    lax.fori_loop(half_count + 1, ep_count, arrive_slots, 0)

    def part_rows(part):
        first = own_rows + part * half_slots
        return slice(first if part else 0, first + half_slots)

    def down_part(core, into, part):
        rows = jnp.concatenate([hidden[v * 2 + core] for v in range(y_count)], axis=0)
        product = jnp.dot(rows, down_ref[...], preferred_element_type=jnp.float32)
        product = product.astype(jnp.bfloat16)
        first = own_rows + part * half_slots
        for v in range(y_count):
            into[v, first : first + half_slots, :] = product[v * half_slots : (v + 1) * half_slots]

    def far_copy(step, part):
        target = lax.rem(y + step, y_count)
        rows = part_rows(part)
        return remote(
            pair_own.at[target, rows],
            far_in.at[step - 1, rows],
            y_send.at[part, step - 1],
            y_recv.at[part, step - 1],
            (e, target * 2 + c),
        )

    for part in range(2):
        first, last = part * half_count, (part + 1) * half_count
        if part > 0:
            lax.fori_loop(first, last, arrive_far, 0)
        lax.fori_loop(first, last, arrive_relay, 0)
        if part == 0:
            for copy in weight_copies[3:6]:
                copy.wait()
        rows_in = xbuf[:, first:last].reshape(tp_count * half_slots, model)
        gate_part = jnp.dot(rows_in, gate_ref[...], preferred_element_type=jnp.float32)
        up_part = jnp.dot(rows_in, up_ref[...], preferred_element_type=jnp.float32)
        hidden[...] = (
            (gate_part / (1.0 + jnp.exp(-gate_part)) * up_part).astype(jnp.bfloat16)
        ).reshape(hidden.shape)
        down_part(1 - c, pair_out, part)
        rows = part_rows(part)
        near_copy = remote(
            pair_out.at[:, rows], pair_in.at[:, rows], p_sem.at[part, 0], p_sem.at[part, 1], (e, partner)
        )
        near_copy.start()
        down_part(c, pair_own, part)
        near_copy.wait()
        pair_own[:, rows] = (
            pair_own[:, rows].astype(jnp.float32) + pair_in[:, rows].astype(jnp.float32)
        ).astype(jnp.bfloat16)
        for step in range(1, y_count):
            far_copy(step, part).start()

    def give_back(j):
        return remote(
            ret_out.at[j], ret_in.at[place_me], v_send.at[j], v_recv.at[place_me], (near(j), t)
        )

    def give_relay(j):
        return remote(
            ret_out.at[half_count + j], gathered.at[place_me], u_send.at[j], u_recv.at[place_me], (near(j), t)
        )

    def finish_experts(part):
        rows = part_rows(part)
        for step in range(1, y_count):
            far_copy(step, part).wait_recv()
        expert_sum = pair_own[y, rows].astype(jnp.float32)
        for step in range(1, y_count):
            expert_sum = expert_sum + far_in[step - 1, rows].astype(jnp.float32)
        if part == 0:
            shared_sum[...] = expert_sum[:own_rows]
            expert_sum = expert_sum[own_rows:]
        first, last = part * half_count, (part + 1) * half_count
        ret_out[first:last] = expert_sum.astype(jnp.bfloat16).reshape(
            (half_count,) + ret_out.shape[1:]
        )
        give = (give_back, give_relay)[part]

        def start_give(j, carry):
            give(j).start()
            return carry

        lax.fori_loop(1, half_count, start_give, 0)
        (ret_in, gathered)[part][place_me] = ret_out[first]

    def arrived(which, source):
        own = jnp.logical_and(source == e, mine)

        @pl.when(own)
        def _():
            own_copy(which).wait()

        @pl.when(jnp.logical_not(own))
        def _():
            place = landing(which, c, source)
            remote(
                place, place, f_send.at[0, source], s_recv.at[which, source], (e, partner)
            ).wait_recv()

    def arrive(j, carry):
        source = lax.rem(e + j, ep_count)
        for which in (1, 2):
            arrived(which, source)
            forward(which, source).start()
        return carry

    lax.fori_loop(0, ep_count, arrive, 0)

    def arrive_forward(j, carry):
        source = lax.rem(e + j, ep_count)
        for which in (1, 2):
            place = landing(which, 1 - c, source)
            remote(
                place,
                place,
                f_send.at[which - 1, source],
                f_recv.at[which - 1, source],
                (e, partner),
            ).wait_recv()
        return carry

    lax.fori_loop(0, ep_count, arrive_forward, 0)
    lam_copy.wait()
    small_copies[7].wait()

    lam = jnp.where(mine, lam_own[...], lam_other[...])[0:1, 0:1]
    gain = gain_ref[...]
    factor = head_dim ** (-0.5) * log2_e

    def back_place(v):
        return heads.at[h_me, v, c]

    def back_copy(target, v):
        return remote(
            obuf.at[target, v],
            back_place(v),
            o_send.at[target, v],
            o_recv.at[h_me, v, c],
            (target, y * 2 + s_me),
        )

    def back_own(v):
        return pltpu.make_async_copy(obuf.at[e, v], back_place(v), o_recv.at[h_me, v, c])

    def attend(pieces):
        def rows_of(v):
            return pl.ds(pl.multiple_of(v * share, share), share)

        block = jnp.concatenate([qbuf[target, rows_of(v), :] for target, v in pieces], axis=0)
        ratios = []
        for m in range(2):
            columns = slice(m * head_dim, (m + 1) * head_dim)
            scores = lax.dot_general(
                block[:, columns],
                kbuf[:, columns],
                (((1,), (1,)), ((), ())),
                preferred_element_type=jnp.float32,
            )
            top = jnp.max(scores, axis=-1, keepdims=True)
            weights = jnp.exp2((scores - top) * factor)
            denominator = jnp.sum(weights, axis=-1, keepdims=True)
            weighted = jnp.dot(
                weights.astype(jnp.bfloat16), vbuf[...], preferred_element_type=jnp.float32
            )
            ratios.append(weighted / denominator)
        mixed = ratios[0] - lam * ratios[1]
        mean_square = jnp.mean(mixed * mixed, axis=-1, keepdims=True)
        done = (mixed * lax.rsqrt(mean_square + head_eps) * gain).astype(jnp.bfloat16)
        for k, (target, v) in enumerate(pieces):
            obuf[target, v] = done[k * share : (k + 1) * share]
        for target, v in pieces:
            own = jnp.logical_and(target == e, mine)

            @pl.when(jnp.logical_not(own))
            def _():
                back_copy(target, v).start()

            @pl.when(own)
            def _():
                back_own(v).start()

    pair_first = s_me * near_pairs

    def beyond_pair(k):
        return (1 - s_me) * (pair_count - 1 - k) + s_me * k

    def near_pair(k):
        return pair_first + lax.rem(pair_me + k, near_pairs)

    v_order = [lax.rem(y + 1 + j, y_count) for j in range(y_count)]

    def await_queries(pair):
        for k in range(2):
            arrived(0, pair * 2 + k)

    def both(pair, v):
        return [(pair * 2 + k, v) for k in range(2)]

    def attend_near(v):
        attend([piece for k in range(near_pairs) for piece in both(near_pair(k), v)])

    def attend_beyond(k):
        await_queries(beyond_pair(k))
        attend([piece for v in v_order for piece in both(beyond_pair(k), v)])

    for k in range(near_pairs):
        await_queries(near_pair(k))
    attend_near(v_order[0])
    finish_experts(0)
    attend_beyond(0)
    finish_experts(1)
    for v in v_order[1:]:
        attend_near(v)
    for k in range(1, near_pairs):
        attend_beyond(k)

    def arrive_gathered(j, carry):
        place = gathered.at[lax.rem(place_me + j, half_count)]
        remote(
            place, place, u_send.at[j], u_recv.at[lax.rem(place_me + j, half_count)], (e, partner)
        ).wait_recv()
        return carry

    part_copy = remote(part_out, part_in, m_sem.at[0], m_sem.at[1], (across, t))

    def mix_across():
        lax.fori_loop(1, half_count, arrive_gathered, 0)
        all_gathered = gathered[...].reshape(half_slots, model)
        cross_mix = ext_in[:, model:]
        part = jnp.dot(cross_mix[:, :half_slots], all_gathered, preferred_element_type=jnp.float32)
        part = part + jnp.dot(
            cross_mix[:, half_slots:], all_gathered, preferred_element_type=jnp.float32
        )
        part_out[...] = part.astype(jnp.bfloat16)
        part_copy.start()

    pl.when(beside)(mix_across)

    weight_copies[6].wait()

    def pair_copy(at):
        return remote(sum_out.at[at], sum_in.at[at], r_send.at[at], r_recv.at[at], (e, partner))

    def project(at):
        v = lax.rem(y + 1 + at, y_count)

        def arrive_heads(h, carry):
            for side in range(2):
                own = jnp.logical_and(
                    jnp.logical_and(c * head_count + h == e, side == c), h == h_me
                )
                place = heads.at[h, v, side]

                @pl.when(own)
                def _():
                    back_own(v).wait()

                @pl.when(jnp.logical_not(own))
                def _():
                    remote(
                        place, place, o_send.at[0, 0], o_recv.at[h, v, side], (e, partner)
                    ).wait_recv()

            return carry

        lax.fori_loop(0, head_count, arrive_heads, 0)
        total = None
        for h in range(head_count):
            rows = jnp.concatenate([heads[h, v, 1 - c], heads[h, v, c]], axis=0)
            term = jnp.dot(
                rows,
                proj_ref[h * width : (h + 1) * width, :],
                preferred_element_type=jnp.float32,
            )
            total = term if total is None else total + term
        total = total.astype(jnp.bfloat16)
        sum_out[at] = total[:share]
        kept[at] = total[share:]
        pair_copy(at).start()

    def block_copy(step):
        target = lax.rem(y + step, y_count)
        return remote(
            block_out.at[step - 1],
            block_in.at[step - 1],
            b_send.at[step - 1],
            b_recv.at[step - 1],
            (e, target * 2 + c),
        )

    for step in range(1, y_count):
        project(step - 1)
        pair_copy(step - 1).wait()
        block_out[step - 1] = (
            kept[step - 1].astype(jnp.float32) + sum_in[step - 1].astype(jnp.float32)
        ).astype(jnp.bfloat16)
        block_copy(step).start()
    pl.when(jnp.logical_not(beside))(mix_across)
    project(y_count - 1)

    def arrive_back(j, carry):
        at = lax.rem(place_me + j, half_count)
        place = ret_in.at[at]
        remote(place, place, v_send.at[j], v_recv.at[at], (e, partner)).wait_recv()
        return carry

    lax.fori_loop(1, half_count, arrive_back, 0)
    wide = mix_ref[own_span, :]
    mix = jnp.where(s_me == 0, wide[:, :half_slots], wide[:, half_slots:])
    coarse = mix.astype(jnp.bfloat16)
    fine = (mix - coarse.astype(jnp.float32)).astype(jnp.bfloat16)
    returned = ret_in[...].reshape(half_slots, model)
    combined = jnp.dot(coarse, returned, preferred_element_type=jnp.float32)
    combined = combined + jnp.dot(fine, returned, preferred_element_type=jnp.float32)
    shared_sum[...] = shared_sum[...] + combined

    pair_copy(y_count - 1).wait()
    total = (
        kept[y_count - 1].astype(jnp.float32) + sum_in[y_count - 1].astype(jnp.float32)
    ).astype(jnp.bfloat16)
    total = total.astype(jnp.float32)
    for step in range(1, y_count):
        block_copy(step).wait()
        total = total + block_in[step - 1].astype(jnp.float32)
    out_ref[...] = total.astype(jnp.bfloat16)
    part_copy.wait()
    moe_ref[...] = (shared_sum[...] + part_in[...].astype(jnp.float32)).astype(jnp.bfloat16)

    def end_send(whiches, h, side, own):
        @pl.when(jnp.logical_not(own))
        def _():
            for which in whiches:
                first_copy(which, h, side).wait_send()

    each_send((0, 1, 2), end_send)

    for step in range(1, y_count):
        for part in range(2):
            far_copy(step, part).wait_send()

    def end_rest(source, carry):
        for far in range(y_count):
            spread(xbuf.at[t, source], source, far).wait_send()
        for far in range(1, y_count):
            relay(source, far, c).wait_send()

        for which in (1, 2):
            forward(which, source).wait_send()

        @pl.when(jnp.logical_not(jnp.logical_and(source == e, mine)))
        def _():
            for v in range(y_count):
                back_copy(source, v).wait_send()

        return carry

    lax.fori_loop(0, ep_count, end_rest, 0)

    def end_near(j, carry):
        dispatch(j).wait_send()
        pass_on(j).wait_send()
        give_back(j).wait_send()
        give_relay(j).wait_send()
        return carry

    lax.fori_loop(1, half_count, end_near, 0)
    cross_copy.wait_send()


def mixer(
    tables,
    sequence,
    lambdas,
    head_gain,
    out_proj,
    moe_inputs,
    expert_weights,
    ep_count,
    tp_count,
    capacity,
):
    moe_input, moe_gain, routes, route_weights = moe_inputs
    head_count = lambdas.shape[0]
    half = sequence[0].shape[0] // 2
    width = sequence[0].shape[1] // head_count
    slots = ep_count * capacity
    batch_rows, model = moe_input.shape
    own_rows = batch_rows // tp_count
    top_count = routes.shape[1]
    hidden_width = expert_weights[0].shape[2]
    shared_width = expert_weights[3].shape[1]
    tokens = ep_count * 2 * half
    share = 2 * half // tp_count
    y_count = tp_count // 2
    dma = pltpu.SemaphoreType.DMA
    bf16 = jnp.bfloat16
    return pl.pallas_call(
        functools.partial(mixer_kernel, ep_count, tp_count),
        out_shape=(
            pltpu.VMEM((share, model), bf16),
            pltpu.VMEM((own_rows, model), bf16),
        ),
        in_specs=[pl.BlockSpec(memory_space=pltpu.HBM)] * 18,
        out_specs=[pl.BlockSpec(memory_space=pltpu.VMEM)] * 2,
        scratch_shapes=[
            pltpu.VMEM((1, head_count), jnp.float32),
            pltpu.VMEM(tables[0].shape, jnp.float32),
            pltpu.VMEM(tables[1].shape, jnp.float32),
            pltpu.VMEM(tables[0].shape[1:], jnp.float32),
            pltpu.VMEM(tables[0].shape[1:], jnp.float32),
            pltpu.VMEM((1, width), jnp.float32),
            pltpu.VMEM((1, model), jnp.float32),
            pltpu.VMEM((top_count, batch_rows), jnp.int32),
            pltpu.VMEM((top_count, batch_rows), jnp.float32),
            pltpu.VMEM((batch_rows, model), bf16),
            dma((8,)),
            pltpu.VMEM((batch_rows, model), bf16),
            pltpu.VMEM((slots, model), bf16),
            pltpu.VMEM((batch_rows, slots), jnp.float32),
            pltpu.VMEM((own_rows, model + slots), bf16),
            pltpu.VMEM((own_rows, model + slots), bf16),
            pltpu.VMEM((slots // 2, model), bf16),
            pltpu.VMEM((ep_count // 2, capacity, model), bf16),
            pltpu.VMEM((own_rows, model), bf16),
            pltpu.VMEM((own_rows, model), bf16),
            pltpu.VMEM((3,) + sequence[0].shape, bf16),
            pltpu.VMEM((3, head_count, 2, half, width), bf16),
            dma((3,)),
            pltpu.VMEM(out_proj.shape, bf16),
            pltpu.VMEM((model, hidden_width), bf16),
            pltpu.VMEM((model, hidden_width), bf16),
            pltpu.VMEM((hidden_width, model), bf16),
            pltpu.VMEM((model, shared_width), bf16),
            pltpu.VMEM((model, shared_width), bf16),
            pltpu.VMEM((shared_width, model), bf16),
            pltpu.VMEM((tp_count, ep_count, capacity, model), bf16),
            pltpu.VMEM((tp_count, slots // 2, hidden_width), bf16),
            pltpu.VMEM((y_count, own_rows + slots, model), bf16),
            pltpu.VMEM((y_count, own_rows + slots, model), bf16),
            pltpu.VMEM((y_count, own_rows + slots, model), bf16),
            pltpu.VMEM((max(1, y_count - 1), own_rows + slots, model), bf16),
            pltpu.VMEM((own_rows, model), jnp.float32),
            pltpu.VMEM((ep_count, capacity, model), bf16),
            pltpu.VMEM((ep_count // 2, capacity, model), bf16),
            dma((7,)),
            dma((ep_count,)),
            dma((ep_count,)),
            dma((2,)),
            dma((ep_count // 2,)),
            dma((ep_count,)),
            dma((ep_count // 2,)),
            dma((2,)),
            dma((ep_count, y_count)),
            dma((ep_count, y_count)),
            dma((ep_count, max(1, y_count - 1))),
            dma((ep_count, max(1, y_count - 1))),
            dma((2, 2)),
            dma((2, max(1, y_count - 1))),
            dma((2, max(1, y_count - 1))),
            dma((ep_count,)),
            dma((ep_count,)),
            pltpu.VMEM((ep_count, half, width), bf16),
            pltpu.VMEM((tokens, width), bf16),
            pltpu.VMEM((tokens, width), bf16),
            pltpu.VMEM((8, 128), jnp.float32),
            pltpu.VMEM((8, 128), jnp.float32),
            pltpu.VMEM((ep_count, y_count, share, width), bf16),
            pltpu.VMEM((head_count, y_count, 2, share, width), bf16),
            pltpu.VMEM((y_count, share, model), bf16),
            pltpu.VMEM((y_count, share, model), bf16),
            pltpu.VMEM((y_count, share, model), bf16),
            pltpu.VMEM((max(1, y_count - 1), share, model), bf16),
            pltpu.VMEM((max(1, y_count - 1), share, model), bf16),
            dma((3, head_count, 2)),
            dma((3, ep_count)),
            dma((3,)),
            dma((2, ep_count)),
            dma((2, ep_count)),
            dma((2,)),
            dma((ep_count, y_count)),
            dma((head_count, y_count, 2)),
            dma((y_count,)),
            dma((y_count,)),
            dma((max(1, y_count - 1),)),
            dma((max(1, y_count - 1),)),
        ],
        compiler_params=pltpu.CompilerParams(
            has_side_effects=True, vmem_limit_bytes=62000000, collective_id=0
        ),
        name="mixer",
    )(
        lambdas[None, :],
        *tables,
        head_gain[None, :],
        moe_gain[None, :],
        jnp.transpose(routes),
        jnp.transpose(route_weights),
        moe_input,
        *sequence,
        out_proj,
        *expert_weights,
    )


def local(
    queries,
    key_rows,
    value_rows,
    lambdas,
    head_gain,
    out_proj,
    moe_input,
    moe_gain,
    routes,
    route_weights,
    expert_gate,
    expert_up,
    expert_down,
    shared_gate,
    shared_up,
    shared_down,
):
    query_rows = queries.shape[0]
    head_count = lambdas.shape[0]
    head_dim = queries.shape[1] // (2 * head_count)
    tp_count = lax.axis_size("tp")
    ep_count = lax.axis_size("ep")
    tp_place = lax.axis_index("tp")
    ep_place = lax.axis_index("ep")
    positions = ep_place * query_rows + jnp.arange(query_rows, dtype=jnp.int32)
    batch_rows = moe_input.shape[0]
    top_count = routes.shape[1]
    own_rows = batch_rows // tp_count
    local_experts = expert_gate.shape[0]
    expert_count = local_experts * ep_count
    capacity = (2 * own_rows * top_count + expert_count - 1) // expert_count
    one_head_each = ep_count == 2 * head_count and tp_count % 2 == 0 and local_experts == 1 and ep_count % 4 == 0 and expert_count * capacity % 128 == 0
    if one_head_each:
        tables = rotation_tables(query_rows, ep_count, head_dim)
        sequence = (queries, key_rows, value_rows)
        weights = (expert_gate, expert_up, expert_down, shared_gate, shared_up, shared_down)
        return mixer(
            tables,
            sequence,
            lambdas,
            head_gain,
            out_proj,
            (moe_input, moe_gain, routes, route_weights),
            weights,
            ep_count,
            tp_count,
            capacity,
        )
    else:
        rot_query = rotate(queries, positions, head_dim)
        rot_keys = rotate(key_rows, positions, head_dim)
        initial = (
            jnp.full((head_count, 2, query_rows), -1e30, jnp.float32),
            jnp.zeros((head_count, 2, query_rows), jnp.float32),
            jnp.zeros((head_count, 2, query_rows, 2 * head_dim), jnp.float32),
        )
        running_max, denominator, numerator = fold_keys(
            initial,
            (
                lax.all_gather(rot_keys, "ep", axis=0, tiled=True),
                lax.all_gather(value_rows, "ep", axis=0, tiled=True),
            ),
            rot_query,
            head_count,
            head_dim,
        )
        ratio = numerator / denominator[..., None]
        mixed_heads = ratio[:, 0] - lambdas[:, None, None] * ratio[:, 1]
        mean_square = jnp.mean(mixed_heads * mixed_heads, axis=-1, keepdims=True)
        normed_heads = (mixed_heads * lax.rsqrt(mean_square + head_eps) * head_gain).astype(
            jnp.bfloat16
        )
        head_out = jnp.transpose(normed_heads, (1, 0, 2)).reshape(query_rows, head_count * 2 * head_dim)
    normed = rms_rows(moe_input, moe_gain)
    shared_hidden = gated_hidden(normed, shared_gate, shared_up)
    own_routes = lax.dynamic_slice_in_dim(routes, tp_place * own_rows, own_rows, 0)
    own_weights = lax.dynamic_slice_in_dim(route_weights, tp_place * own_rows, own_rows, 0)
    own_source, own_filled, own_rank = slot_table(own_routes, expert_count, capacity)
    own_normed = lax.dynamic_slice_in_dim(normed, tp_place * own_rows, own_rows, 0)
    outgoing = fill_slots(own_normed, own_source, own_filled)
    arrived = lax.all_to_all(outgoing[:, None], "ep", split_axis=0, concat_axis=2, tiled=True)
    hidden = slot_hidden(lax.all_gather(arrived, "tp", axis=1, tiled=True), expert_gate, expert_up)
    slot_rows = local_experts * ep_count * capacity
    mixer_share = query_rows // tp_count
    expert_share = own_rows + slot_rows
    if not one_head_each:
        block_count = lax.axis_size("tp") * mixer_share // mixer_share
        product = jnp.dot(head_out, out_proj, preferred_element_type=jnp.float32)
        mixer_out = lax.psum_scatter(
            product.reshape(block_count, mixer_share, -1)
            .reshape(lax.axis_size("tp") * mixer_share, -1)
            .astype(jnp.bfloat16),
            "tp",
            scatter_dimension=0,
            tiled=True,
        )
    block_count = lax.axis_size("tp") * expert_share // expert_share
    shared_part = jnp.dot(shared_hidden, shared_down, preferred_element_type=jnp.float32).reshape(
        block_count, own_rows, -1
    )
    routed_part = jnp.einsum(
        "xnsf,xfd->nxsd", hidden, expert_down, preferred_element_type=jnp.float32
    )
    routed_part = routed_part.reshape(block_count, slot_rows, -1)
    expert_sum = lax.psum_scatter(
        jnp.concatenate([shared_part, routed_part], axis=1)
        .reshape(lax.axis_size("tp") * expert_share, -1)
        .astype(jnp.bfloat16),
        "tp",
        scatter_dimension=0,
        tiled=True,
    ).astype(jnp.float32)
    shared_sum = expert_sum[:own_rows]
    routed = (
        expert_sum[own_rows:].reshape(local_experts, ep_count * capacity, -1).astype(jnp.bfloat16)
    )
    returned = lax.all_to_all(routed, "ep", split_axis=1, concat_axis=0, tiled=True)
    flat_index = (own_routes * capacity + own_rank).reshape(-1)
    picked = jnp.take(returned.reshape(expert_count * capacity, -1), flat_index, axis=0).reshape(
        own_rows, top_count, -1
    )
    combined = shared_sum + jnp.sum(own_weights[..., None] * picked.astype(jnp.float32), axis=1)
    return (mixer_out, combined.astype(jnp.bfloat16))


def solution(mesh):
    in_specs = (
        P("ep", "tp"),
        P("ep", "tp"),
        P("ep", "tp"),
        P("tp"),
        P(),
        P("tp", None),
        P("ep", None),
        P(),
        P("ep", None),
        P("ep", None),
        P("ep", None, "tp"),
        P("ep", None, "tp"),
        P("ep", "tp", None),
        P(None, "tp"),
        P(None, "tp"),
        P("tp", None),
    )
    out_specs = (P(("ep", "tp"), None), P(("ep", "tp"), None))
    return jax.shard_map(local, mesh=mesh, in_specs=in_specs, out_specs=out_specs, check_vma=False)
```

```python
import functools
import jax
import jax.numpy as jnp
import numpy as np
from jax import lax
from jax.experimental import pallas as pl
from jax.experimental.pallas import tpu as pltpu
from jax.sharding import PartitionSpec as P

theta_base = 500000.0
norm_eps = 1e-06
head_eps = 1e-05
MESH = pl.DeviceIdType.MESH
log2_e = 1.4426950408889634


def rotate(matrix, positions, head_dim):
    row_count = matrix.shape[0]
    shaped = matrix.reshape(row_count, -1, head_dim).astype(jnp.float32)
    half_dim = head_dim // 2
    frequency = jnp.power(theta_base, -jnp.arange(half_dim, dtype=jnp.float32) * 2.0 / head_dim)
    angles = positions.astype(jnp.float32)[:, None] * frequency[None, :]
    cosine = jnp.cos(angles)[:, None, :]
    sines = jnp.sin(angles)[:, None, :]
    front_half = shaped[..., :half_dim]
    second = shaped[..., half_dim:]
    turned = jnp.concatenate(
        [front_half * cosine - second * sines, second * cosine + front_half * sines], axis=-1
    )
    return turned.reshape(matrix.shape).astype(jnp.bfloat16)


def rms_rows(values, gain):
    widened = values.astype(jnp.float32)
    mean_square = jnp.mean(widened * widened, axis=-1, keepdims=True)
    return (widened * lax.rsqrt(mean_square + norm_eps) * gain).astype(jnp.bfloat16)


def gated_hidden(rows_in, gate_weight, up_weight):
    gate_part = jnp.dot(rows_in, gate_weight, preferred_element_type=jnp.float32)
    up_part = jnp.dot(rows_in, up_weight, preferred_element_type=jnp.float32)
    return (jax.nn.silu(gate_part) * up_part).astype(jnp.bfloat16)


def slot_hidden(slot_rows, gate_weight, up_weight):
    gate_part = jnp.einsum(
        "xnsd,xdf->xnsf", slot_rows, gate_weight, preferred_element_type=jnp.float32
    )
    up_part = jnp.einsum("xnsd,xdf->xnsf", slot_rows, up_weight, preferred_element_type=jnp.float32)
    return (jax.nn.silu(gate_part) * up_part).astype(jnp.bfloat16)


def key_block_size(piece_rows):
    for candidate in (1024, 512):
        return candidate
    return piece_rows


def fold_keys(state_in, pieces, rot_query, head_count, head_dim):
    keys_piece, values_piece = pieces
    piece_rows = keys_piece.shape[0]
    block_rows = key_block_size(piece_rows)
    block_count = piece_rows // block_rows
    query_view = rot_query.reshape(rot_query.shape[0], head_count, 2, head_dim)
    score_scale = head_dim ** (-0.5)

    def one_block(running, key_block):
        running_max, denominator, numerator = running
        key_view = key_block[0].reshape(block_rows, head_count, 2, head_dim)
        value_view = key_block[1].reshape(block_rows, head_count, 2 * head_dim)
        scores = (
            jnp.einsum("qhmd,khmd->hmqk", query_view, key_view, preferred_element_type=jnp.float32)
            * score_scale
        )
        newest = jnp.maximum(running_max, jnp.max(scores, axis=-1))
        weights = jnp.exp(scores - newest[..., None])
        shrink = jnp.exp(running_max - newest)
        denominator = denominator * shrink + jnp.sum(weights, axis=-1)
        weighted = jnp.einsum(
            "hmqk,khe->hmqe",
            weights.astype(jnp.bfloat16),
            value_view,
            preferred_element_type=jnp.float32,
        )
        numerator = numerator * shrink[..., None] + weighted
        return ((newest, denominator, numerator), None)

    blocks = (
        keys_piece.reshape(block_count, block_rows, -1),
        values_piece.reshape(block_count, block_rows, -1),
    )
    result, _ = lax.scan(one_block, state_in, blocks)
    return result


def slot_table(route_block, expert_count, capacity):
    flat_routes = route_block.reshape(-1)
    route_total = flat_routes.shape[0]
    top_count = route_block.shape[1]
    experts_iota = jnp.arange(expert_count, dtype=jnp.int32)
    onehot = (flat_routes[:, None] == experts_iota[None, :]).astype(jnp.int32)
    before = jnp.cumsum(onehot, axis=0) - onehot
    slot_rank = jnp.sum(before * onehot, axis=1)
    slot_iota = jnp.arange(capacity, dtype=jnp.int32)
    matches = (flat_routes[None, None, :] == experts_iota[:, None, None]) & (
        slot_rank[None, None, :] == slot_iota[None, :, None]
    )
    source_row = jnp.arange(route_total, dtype=jnp.int32) // top_count
    source = jnp.sum(jnp.where(matches, source_row[None, None, :], 0), axis=2)
    filled = jnp.any(matches, axis=2)
    return (source, filled, slot_rank.reshape(route_block.shape))


def fill_slots(rows_src, source, filled):
    taken = jnp.take(rows_src, source.reshape(-1), axis=0).reshape(
        source.shape + (rows_src.shape[1],)
    )
    return jnp.where(filled[..., None], taken, jnp.zeros_like(taken))


def rotation_tables(row_count, block_count, head_dim):
    half_dim = head_dim // 2
    frequency = np.power(theta_base, -np.arange(half_dim) * 2.0 / head_dim)

    def table(positions):
        angles = positions[:, None] * frequency[None, :]
        cosine, sines = np.cos(angles), np.sin(angles)
        both = (np.concatenate([cosine, cosine], 1), np.concatenate([-sines, sines], 1))
        return np.stack(both).astype(np.float32)

    return (
        jnp.asarray(table(np.arange(row_count))),
        jnp.asarray(table(np.arange(block_count) * row_count)),
    )


def mixer_kernel(
    ep_count,
    tp_count,
    lam_hbm,
    turn_hbm,
    base_hbm,
    gain_hbm,
    mgain_hbm,
    routes_hbm,
    scale_hbm,
    rows_hbm,
    q_hbm,
    k_hbm,
    v_hbm,
    proj_hbm,
    gate_hbm,
    up_hbm,
    down_hbm,
    sgate_hbm,
    sup_hbm,
    sdown_hbm,
    out_ref,
    moe_ref,
    lam_ref,
    turn_ref,
    base_ref,
    cos_ref,
    sin_ref,
    gain_ref,
    mgain_ref,
    routes_ref,
    scale_ref,
    rows_ref,
    small_sem,
    norm_ref,
    slot_ref,
    mix_ref,
    ext_out,
    ext_in,
    rel_slots,
    gathered,
    part_out,
    part_in,
    raw,
    pack_ref,
    q_sem,
    proj_ref,
    gate_ref,
    up_ref,
    down_ref,
    sgate_ref,
    sup_ref,
    sdown_ref,
    xbuf,
    hidden,
    pair_out,
    pair_own,
    pair_in,
    far_in,
    shared_sum,
    ret_out,
    ret_in,
    w_sem,
    d_send,
    d_recv,
    c_sem,
    k_send,
    u_send,
    u_recv,
    m_sem,
    g_send,
    g_recv,
    h_send,
    h_recv,
    p_sem,
    y_send,
    y_recv,
    v_send,
    v_recv,
    qbuf,
    kbuf,
    vbuf,
    lam_own,
    lam_other,
    obuf,
    heads,
    sum_out,
    sum_in,
    kept,
    block_out,
    block_in,
    s_send,
    s_recv,
    s_local,
    f_send,
    f_recv,
    l_sem,
    o_send,
    o_recv,
    r_send,
    r_recv,
    b_send,
    b_recv,
):
    head_count = pack_ref.shape[1]
    half, width = pack_ref.shape[3], pack_ref.shape[4]
    head_dim = width // 2
    e = lax.axis_index("ep")
    t = lax.axis_index("tp")
    y, c = t // 2, lax.rem(t, 2)
    partner = y * 2 + 1 - c
    s_me, h_me = e // head_count, lax.rem(e, head_count)
    y_count = tp_count // 2
    share = half // y_count

    barrier = pltpu.get_barrier_semaphore()

    def greet(where):
        pl.semaphore_signal(barrier, inc=1, device_id=where, device_id_type=MESH)

    def greet_row(j, carry):
        there = lax.rem(e + j, ep_count)
        for core in range(2):
            greet((there, y * 2 + core))
        return carry

    lax.fori_loop(1, ep_count, greet_row, 0)
    greet((e, partner))
    for step in range(1, y_count):
        greet((e, lax.rem(y + step, y_count) * 2 + c))

    def remote(src, dst, send, recv, where):
        return pltpu.make_async_remote_copy(
            src_ref=src,
            dst_ref=dst,
            send_sem=send,
            recv_sem=recv,
            device_id=where,
            device_id_type=MESH,
        )

    small_copies = [
        pltpu.make_async_copy(a, b, small_sem.at[at])
        for at, (a, b) in enumerate(
            (
                (routes_hbm, routes_ref),
                (scale_hbm, scale_ref),
                (mgain_hbm, mgain_ref),
                (lam_hbm, lam_ref),
                (rows_hbm, rows_ref),
                (base_hbm, base_ref),
                (turn_hbm, turn_ref),
                (gain_hbm, gain_ref),
            )
        )
    ]
    for copy in small_copies:
        copy.start()
    raw_copies = [
        pltpu.make_async_copy(ref, raw.at[at], q_sem.at[at])
        for at, ref in enumerate((q_hbm, k_hbm, v_hbm))
    ]
    for copy in raw_copies:
        copy.start()
    weight_copies = [
        pltpu.make_async_copy(a, b, w_sem.at[at])
        for at, (a, b) in enumerate(
            (
                (sgate_hbm, sgate_ref),
                (sup_hbm, sup_ref),
                (sdown_hbm, sdown_ref),
                (gate_hbm.at[0], gate_ref),
                (up_hbm.at[0], up_ref),
                (down_hbm.at[0], down_ref),
                (proj_hbm, proj_ref),
            )
        )
    ]
    def landing(which, side, source):
        if which == 0:
            return qbuf.at[source]
        return (kbuf, vbuf)[which - 1].at[pl.ds((side * ep_count + source) * half, half)]

    def first_copy(which, h, side):
        return remote(
            pack_ref.at[which, h, side],
            landing(which, side, e),
            s_send.at[which, h, side],
            s_recv.at[which, e],
            (c * head_count + h, y * 2 + side),
        )

    def own_copy(which):
        return pltpu.make_async_copy(
            pack_ref.at[which, h_me, c], landing(which, c, e), s_local.at[which]
        )

    def forward(which, source):
        place = landing(which, c, source)
        return remote(
            place, place, f_send.at[which - 1, source], f_recv.at[which - 1, source], (e, partner)
        )

    capacity = xbuf.shape[2]
    own_rows = moe_ref.shape[0]
    slots = ep_count * capacity
    batch_rows = rows_ref.shape[0]
    model = rows_ref.shape[1]
    half_count = ep_count // 2
    half_slots = half_count * capacity
    across = lax.rem(e + half_count, ep_count)
    near_first = s_me * half_count
    place_me = lax.rem(e, half_count)

    def near(j):
        return near_first + lax.rem(place_me + j, half_count)

    for copy in small_copies[:5]:
        copy.wait()
    widened = rows_ref[...].astype(jnp.float32)
    mean_square = jnp.mean(widened * widened, axis=-1, keepdims=True)
    norm_ref[...] = (widened * lax.rsqrt(mean_square + norm_eps) * mgain_ref[...]).astype(
        jnp.bfloat16
    )
    slot_at = lax.broadcasted_iota(jnp.int32, (slots, batch_rows), 0)
    slot_expert, slot_rank = slot_at // capacity, lax.rem(slot_at, capacity)
    hits = [routes_ref[k : k + 1, :] == slot_expert for k in range(routes_ref.shape[0])]
    named = sum(hit.astype(jnp.float32) for hit in hits).astype(jnp.bfloat16)
    other_at = lax.broadcasted_iota(jnp.int32, (batch_rows, batch_rows), 0)
    row_at = lax.broadcasted_iota(jnp.int32, (batch_rows, batch_rows), 1)
    earlier = jnp.logical_and(other_at < row_at, other_at // own_rows == row_at // own_rows)
    before = jnp.dot(
        named, earlier.astype(jnp.float32).astype(jnp.bfloat16), preferred_element_type=jnp.float32
    ).astype(jnp.int32)
    chosen = [jnp.logical_and(hit, before == slot_rank).astype(jnp.float32) for hit in hits]
    token_block = lax.broadcasted_iota(jnp.int32, (slots, batch_rows), 1) // own_rows
    picked = jnp.where(token_block == t, sum(chosen), 0.0).astype(jnp.bfloat16)
    slot_ref[...] = jnp.dot(
        picked, norm_ref[...], preferred_element_type=jnp.float32
    ).astype(jnp.bfloat16)
    mixing = sum(scale_ref[k : k + 1, :] * chosen[k] for k in range(len(chosen)))
    mix_ref[...] = jnp.transpose(mixing)
    head_at = lax.broadcasted_iota(jnp.int32, lam_ref.shape, 1)
    lam_mine = jnp.sum(
        jnp.where(head_at == h_me, lam_ref[...], 0.0), axis=1, keepdims=True
    )
    lam_own[...] = jnp.broadcast_to(lam_mine, lam_own.shape)

    def fold(wide):
        return jnp.where(s_me == 0, wide[:, half_slots:], wide[:, :half_slots])

    own_span = pl.ds(pl.multiple_of(t * own_rows, own_rows), own_rows)
    away = fold(mix_ref[own_span, :])
    away_coarse = away.astype(jnp.bfloat16)
    away_fine = (away - away_coarse.astype(jnp.float32)).astype(jnp.bfloat16)
    ext_out[:, :model] = norm_ref[own_span, :]
    ext_out[:, model:] = jnp.concatenate([away_coarse, away_fine], axis=1)

    for copy in small_copies[5:7]:
        copy.wait()
    base_cos, base_sin = base_ref[0, pl.ds(e, 1), :], base_ref[1, pl.ds(e, 1), :]
    cos_ref[...] = base_cos * turn_ref[0] - base_sin * turn_ref[1]
    sin_ref[...] = base_sin * turn_ref[0] + base_cos * turn_ref[1]
    for copy in raw_copies:
        copy.wait()

    def pack_head(h, carry):
        cosine = cos_ref[...]
        sines = sin_ref[...]
        for which in range(2):
            for m in range(2):
                at = pl.multiple_of(h * width + m * head_dim, head_dim)
                part = raw[which, :, pl.ds(at, head_dim)].astype(jnp.float32)
                turned = part * cosine + pltpu.roll(part, head_dim // 2, 1) * sines
                turned = turned.astype(jnp.bfloat16)
                for v in range(y_count):
                    for side in range(2):
                        block = v * 2 + side
                        pack_ref[
                            which,
                            h,
                            side,
                            v * share : (v + 1) * share,
                            m * head_dim : (m + 1) * head_dim,
                        ] = turned[block * share : (block + 1) * share]
        at = pl.multiple_of(h * width, width)
        for v in range(y_count):
            for side in range(2):
                block = v * 2 + side
                pack_ref[2, h, side, v * share : (v + 1) * share] = raw[
                    2, block * share : (block + 1) * share, pl.ds(at, width)
                ]
        return carry

    lax.fori_loop(0, head_count, pack_head, 0)

    pl.semaphore_wait(barrier, (ep_count - 1) * 2 + 1 + (y_count - 1))

    for copy in weight_copies:
        copy.start()

    def dispatch(j):
        target, at = near(j), half_count - j
        rows = pl.ds(pl.multiple_of(target * capacity, capacity), capacity)
        return remote(
            slot_ref.at[rows], xbuf.at[t, at], d_send.at[target], d_recv.at[at], (target, t)
        )

    cross_copy = remote(ext_out, ext_in, c_sem.at[0], c_sem.at[1], (across, t))
    cross_copy.start()

    def start_dispatch(j, carry):
        dispatch(j).start()
        return carry

    lax.fori_loop(1, half_count, start_dispatch, 0)

    mine = s_me == c

    def each_send(whiches, act):
        def body(j, carry):
            h = lax.rem(h_me + 1 + j, head_count)
            for k in range(2):
                side = lax.rem(c + 1 + k, 2)
                own = jnp.logical_and(c * head_count + h == e, side == c)
                act(whiches, h, side, own)
            return carry

        lax.fori_loop(0, head_count, body, 0)

    def start_send(whiches, h, side, own):
        @pl.when(jnp.logical_not(own))
        def _():
            for which in whiches:
                first_copy(which, h, side).start()

    pair_count = ep_count // 2
    pair_me = e // 2
    near_pairs = pair_count // 2
    beside = jnp.logical_or(pair_me == near_pairs - 1, pair_me == near_pairs)
    at_once = jnp.logical_and(jnp.logical_not(mine), beside)

    @pl.when(at_once)
    def _():
        each_send((1, 2), start_send)
        each_send((0,), start_send)

    lam_copy = remote(lam_own, lam_other, l_sem.at[0], l_sem.at[1], (e, partner))
    lam_copy.start()
    xbuf[t, 0] = slot_ref[pl.ds(pl.multiple_of(e * capacity, capacity), capacity), :]

    def spread(place, source, far):
        if far == 0:
            sends, recvs, where = g_send.at[source, 0], g_recv.at[source, 0], (e, partner)
        else:
            there = lax.rem(y + far, y_count)
            sends, recvs = g_send.at[source, far], g_recv.at[source, far]
            where = (e, there * 2 + c)
        return remote(place, place, sends, recvs, where)

    def hand_out(source):
        place = xbuf.at[t, source]
        for far in range(1, y_count):
            spread(place, source, far).start()
        spread(place, source, 0).start()

    def relay(source, far, core):
        from_y = lax.rem(y + y_count - far, y_count)
        place = xbuf.at[from_y * 2 + core, source]
        return remote(
            place, place, h_send.at[source, far - 1], h_recv.at[source, far - 1], (e, partner)
        )

    def arrive_slots(at, carry):
        place = xbuf.at[t, at]
        remote(place, place, d_send.at[at], d_recv.at[at], (e, partner)).wait_recv()
        hand_out(at)
        return carry

    def arrive_far(source, carry):
        for far in range(1, y_count):
            from_y = lax.rem(y + y_count - far, y_count)
            spread(xbuf.at[from_y * 2 + c, source], source, far).wait_recv()
            relay(source, far, c).start()
        return carry

    def arrive_relay(source, carry):
        spread(xbuf.at[partner, source], source, 0).wait_recv()
        for far in range(1, y_count):
            relay(source, far, 1 - c).wait_recv()
        return carry

    hand_out(0)

    for copy in weight_copies[:3]:
        copy.wait()
    normed = norm_ref[...]
    gate_part = jnp.dot(normed, sgate_ref[...], preferred_element_type=jnp.float32)
    up_part = jnp.dot(normed, sup_ref[...], preferred_element_type=jnp.float32)
    shared_hidden = (gate_part / (1.0 + jnp.exp(-gate_part)) * up_part).astype(jnp.bfloat16)
    shared_part = jnp.dot(
        shared_hidden, sdown_ref[...], preferred_element_type=jnp.float32
    ).astype(jnp.bfloat16)
    for v in range(y_count):
        for core in range(2):
            block = shared_part[(v * 2 + core) * own_rows : (v * 2 + core + 1) * own_rows]

            @pl.when(c == core)
            def _():
                pair_own[v, :own_rows, :] = block

            @pl.when(c != core)
            def _():
                pair_out[v, :own_rows, :] = block

    lax.fori_loop(1, half_count, arrive_slots, 0)
    cross_copy.wait_recv()
    sent_rows = ext_in[:, :model]
    sent_mix = ext_in[:, model:]
    taken = (sent_mix[:, :half_slots].astype(jnp.float32) > 0.0).astype(jnp.float32)
    rel_slots[...] = lax.dot_general(
        taken.astype(jnp.bfloat16),
        sent_rows,
        (((0,), (0,)), ((), ())),
        preferred_element_type=jnp.float32,
    ).astype(jnp.bfloat16)

    def pass_on(j):
        to, at = lax.rem(place_me + j, half_count), half_count + (half_count - j)
        rows = pl.ds(pl.multiple_of(to * capacity, capacity), capacity)
        return remote(
            rel_slots.at[rows],
            xbuf.at[t, at],
            k_send.at[to],
            d_recv.at[at],
            (near_first + to, t),
        )

    def start_pass(j, carry):
        pass_on(j).start()
        return carry

    lax.fori_loop(1, half_count, start_pass, 0)
    xbuf[t, half_count] = rel_slots[
        pl.ds(pl.multiple_of(place_me * capacity, capacity), capacity), :
    ]

    @pl.when(jnp.logical_not(at_once))
    def _():
        each_send((1, 2), start_send)
        each_send((0,), start_send)

    @pl.when(mine)
    def _():
        for which in range(3):
            own_copy(which).start()

    hand_out(half_count)
    lax.fori_loop(0, half_count, arrive_far, 0)
    lax.fori_loop(half_count + 1, ep_count, arrive_slots, 0)

    def part_rows(part):
        first = own_rows + part * half_slots
        return slice(first if part else 0, first + half_slots)

    def down_part(core, into, part):
        rows = jnp.concatenate([hidden[v * 2 + core] for v in range(y_count)], axis=0)
        product = jnp.dot(rows, down_ref[...], preferred_element_type=jnp.float32)
        product = product.astype(jnp.bfloat16)
        first = own_rows + part * half_slots
        for v in range(y_count):
            into[v, first : first + half_slots, :] = product[v * half_slots : (v + 1) * half_slots]

    def far_copy(step, part):
        target = lax.rem(y + step, y_count)
        rows = part_rows(part)
        return remote(
            pair_own.at[target, rows],
            far_in.at[step - 1, rows],
            y_send.at[part, step - 1],
            y_recv.at[part, step - 1],
            (e, target * 2 + c),
        )

    for part in range(2):
        first, last = part * half_count, (part + 1) * half_count
        if part > 0:
            lax.fori_loop(first, last, arrive_far, 0)
        lax.fori_loop(first, last, arrive_relay, 0)
        if part == 0:
            for copy in weight_copies[3:6]:
                copy.wait()
        rows_in = xbuf[:, first:last].reshape(tp_count * half_slots, model)
        gate_part = jnp.dot(rows_in, gate_ref[...], preferred_element_type=jnp.float32)
        up_part = jnp.dot(rows_in, up_ref[...], preferred_element_type=jnp.float32)
        hidden[...] = (
            (gate_part / (1.0 + jnp.exp(-gate_part)) * up_part).astype(jnp.bfloat16)
        ).reshape(hidden.shape)
        down_part(1 - c, pair_out, part)
        rows = part_rows(part)
        near_copy = remote(
            pair_out.at[:, rows], pair_in.at[:, rows], p_sem.at[part, 0], p_sem.at[part, 1], (e, partner)
        )
        near_copy.start()
        down_part(c, pair_own, part)
        near_copy.wait()
        pair_own[:, rows] = (
            pair_own[:, rows].astype(jnp.float32) + pair_in[:, rows].astype(jnp.float32)
        ).astype(jnp.bfloat16)
        for step in range(1, y_count):
            far_copy(step, part).start()

    def give_back(j):
        return remote(
            ret_out.at[j], ret_in.at[place_me], v_send.at[j], v_recv.at[place_me], (near(j), t)
        )

    def give_relay(j):
        return remote(
            ret_out.at[half_count + j], gathered.at[place_me], u_send.at[j], u_recv.at[place_me], (near(j), t)
        )

    def finish_experts(part):
        rows = part_rows(part)
        for step in range(1, y_count):
            far_copy(step, part).wait_recv()
        expert_sum = pair_own[y, rows].astype(jnp.float32)
        for step in range(1, y_count):
            expert_sum = expert_sum + far_in[step - 1, rows].astype(jnp.float32)
        if part == 0:
            shared_sum[...] = expert_sum[:own_rows]
            expert_sum = expert_sum[own_rows:]
        first, last = part * half_count, (part + 1) * half_count
        ret_out[first:last] = expert_sum.astype(jnp.bfloat16).reshape(
            (half_count,) + ret_out.shape[1:]
        )
        give = (give_back, give_relay)[part]

        def start_give(j, carry):
            give(j).start()
            return carry

        lax.fori_loop(1, half_count, start_give, 0)
        (ret_in, gathered)[part][place_me] = ret_out[first]

    def arrived(which, source):
        own = jnp.logical_and(source == e, mine)

        @pl.when(own)
        def _():
            own_copy(which).wait()

        @pl.when(jnp.logical_not(own))
        def _():
            place = landing(which, c, source)
            remote(
                place, place, f_send.at[0, source], s_recv.at[which, source], (e, partner)
            ).wait_recv()

    def arrive(j, carry):
        source = lax.rem(e + j, ep_count)
        for which in (1, 2):
            arrived(which, source)
            forward(which, source).start()
        return carry

    lax.fori_loop(0, ep_count, arrive, 0)

    def arrive_forward(j, carry):
        source = lax.rem(e + j, ep_count)
        for which in (1, 2):
            place = landing(which, 1 - c, source)
            remote(
                place,
                place,
                f_send.at[which - 1, source],
                f_recv.at[which - 1, source],
                (e, partner),
            ).wait_recv()
        return carry

    lax.fori_loop(0, ep_count, arrive_forward, 0)
    lam_copy.wait()
    small_copies[7].wait()

    lam = jnp.where(mine, lam_own[...], lam_other[...])[0:1, 0:1]
    gain = gain_ref[...]
    factor = head_dim ** (-0.5) * log2_e

    def back_place(v):
        return heads.at[h_me, v, c]

    def back_copy(target, v):
        return remote(
            obuf.at[target, v],
            back_place(v),
            o_send.at[target, v],
            o_recv.at[h_me, v, c],
            (target, y * 2 + s_me),
        )

    def back_own(v):
        return pltpu.make_async_copy(obuf.at[e, v], back_place(v), o_recv.at[h_me, v, c])

    def attend(pieces):
        def rows_of(v):
            return pl.ds(pl.multiple_of(v * share, share), share)

        block = jnp.concatenate([qbuf[target, rows_of(v), :] for target, v in pieces], axis=0)
        ratios = []
        for m in range(2):
            columns = slice(m * head_dim, (m + 1) * head_dim)
            scores = lax.dot_general(
                block[:, columns],
                kbuf[:, columns],
                (((1,), (1,)), ((), ())),
                preferred_element_type=jnp.float32,
            )
            top = jnp.max(scores, axis=-1, keepdims=True)
            weights = jnp.exp2((scores - top) * factor)
            denominator = jnp.sum(weights, axis=-1, keepdims=True)
            weighted = jnp.dot(
                weights.astype(jnp.bfloat16), vbuf[...], preferred_element_type=jnp.float32
            )
            ratios.append(weighted / denominator)
        mixed = ratios[0] - lam * ratios[1]
        mean_square = jnp.mean(mixed * mixed, axis=-1, keepdims=True)
        done = (mixed * lax.rsqrt(mean_square + head_eps) * gain).astype(jnp.bfloat16)
        for k, (target, v) in enumerate(pieces):
            obuf[target, v] = done[k * share : (k + 1) * share]
        for target, v in pieces:
            own = jnp.logical_and(target == e, mine)

            @pl.when(jnp.logical_not(own))
            def _():
                back_copy(target, v).start()

            @pl.when(own)
            def _():
                back_own(v).start()

    pair_first = s_me * near_pairs

    def beyond_pair(k):
        return (1 - s_me) * (pair_count - 1 - k) + s_me * k

    def near_pair(k):
        return pair_first + lax.rem(pair_me + k, near_pairs)

    v_order = [lax.rem(y + 1 + j, y_count) for j in range(y_count)]

    def await_queries(pair):
        for k in range(2):
            arrived(0, pair * 2 + k)

    def both(pair, v):
        return [(pair * 2 + k, v) for k in range(2)]

    def attend_near(v):
        attend([piece for k in range(near_pairs) for piece in both(near_pair(k), v)])

    def attend_beyond(k):
        await_queries(beyond_pair(k))
        attend([piece for v in v_order for piece in both(beyond_pair(k), v)])

    for k in range(near_pairs):
        await_queries(near_pair(k))
    attend_near(v_order[0])
    finish_experts(0)
    attend_beyond(0)
    finish_experts(1)
    for v in v_order[1:]:
        attend_near(v)
    for k in range(1, near_pairs):
        attend_beyond(k)

    def arrive_gathered(j, carry):
        place = gathered.at[lax.rem(place_me + j, half_count)]
        remote(
            place, place, u_send.at[j], u_recv.at[lax.rem(place_me + j, half_count)], (e, partner)
        ).wait_recv()
        return carry

    part_copy = remote(part_out, part_in, m_sem.at[0], m_sem.at[1], (across, t))

    def mix_across():
        lax.fori_loop(1, half_count, arrive_gathered, 0)
        all_gathered = gathered[...].reshape(half_slots, model)
        cross_mix = ext_in[:, model:]
        part = jnp.dot(cross_mix[:, :half_slots], all_gathered, preferred_element_type=jnp.float32)
        part = part + jnp.dot(
            cross_mix[:, half_slots:], all_gathered, preferred_element_type=jnp.float32
        )
        part_out[...] = part.astype(jnp.bfloat16)
        part_copy.start()

    pl.when(beside)(mix_across)

    weight_copies[6].wait()

    column_parts = 2
    part_width = model // column_parts

    def columns_of(part):
        return slice(part * part_width, (part + 1) * part_width)

    def pair_copy(at, part):
        columns = columns_of(part)
        return remote(
            sum_out.at[at, :, columns],
            sum_in.at[at, :, columns],
            r_send.at[at, part],
            r_recv.at[at, part],
            (e, partner),
        )

    def pair_sum(at, part):
        pair_copy(at, part).wait()
        columns = columns_of(part)
        mine_part = kept[at, :, columns].astype(jnp.float32)
        return (mine_part + sum_in[at, :, columns].astype(jnp.float32)).astype(jnp.bfloat16)

    def project(at):
        v = lax.rem(y + 1 + at, y_count)

        def arrive_heads(h, carry):
            for side in range(2):
                own = jnp.logical_and(
                    jnp.logical_and(c * head_count + h == e, side == c), h == h_me
                )
                place = heads.at[h, v, side]

                @pl.when(own)
                def _():
                    back_own(v).wait()

                @pl.when(jnp.logical_not(own))
                def _():
                    remote(
                        place, place, o_send.at[0, 0], o_recv.at[h, v, side], (e, partner)
                    ).wait_recv()

            return carry

        lax.fori_loop(0, head_count, arrive_heads, 0)
        rows = [
            jnp.concatenate([heads[h, v, 1 - c], heads[h, v, c]], axis=0)
            for h in range(head_count)
        ]
        for part in range(column_parts):
            columns = columns_of(part)
            total = None
            for h in range(head_count):
                term = jnp.dot(
                    rows[h],
                    proj_ref[h * width : (h + 1) * width, columns],
                    preferred_element_type=jnp.float32,
                )
                total = term if total is None else total + term
            total = total.astype(jnp.bfloat16)
            sum_out[at, :, columns] = total[:share]
            kept[at, :, columns] = total[share:]
            pair_copy(at, part).start()

    def block_copy(step, part):
        target = lax.rem(y + step, y_count)
        columns = columns_of(part)
        return remote(
            block_out.at[step - 1, :, columns],
            block_in.at[step - 1, :, columns],
            b_send.at[step - 1, part],
            b_recv.at[step - 1, part],
            (e, target * 2 + c),
        )

    for step in range(1, y_count):
        project(step - 1)
        for part in range(column_parts):
            block_out[step - 1, :, columns_of(part)] = pair_sum(step - 1, part)
            block_copy(step, part).start()
    pl.when(jnp.logical_not(beside))(mix_across)
    project(y_count - 1)

    def arrive_back(j, carry):
        at = lax.rem(place_me + j, half_count)
        place = ret_in.at[at]
        remote(place, place, v_send.at[j], v_recv.at[at], (e, partner)).wait_recv()
        return carry

    lax.fori_loop(1, half_count, arrive_back, 0)
    wide = mix_ref[own_span, :]
    mix = jnp.where(s_me == 0, wide[:, :half_slots], wide[:, half_slots:])
    coarse = mix.astype(jnp.bfloat16)
    fine = (mix - coarse.astype(jnp.float32)).astype(jnp.bfloat16)
    returned = ret_in[...].reshape(half_slots, model)
    combined = jnp.dot(coarse, returned, preferred_element_type=jnp.float32)
    combined = combined + jnp.dot(fine, returned, preferred_element_type=jnp.float32)
    shared_sum[...] = shared_sum[...] + combined

    for part in range(column_parts):
        columns = columns_of(part)
        total = pair_sum(y_count - 1, part).astype(jnp.float32)
        for step in range(1, y_count):
            block_copy(step, part).wait()
            total = total + block_in[step - 1, :, columns].astype(jnp.float32)
        out_ref[:, columns] = total.astype(jnp.bfloat16)
    part_copy.wait()
    moe_ref[...] = (shared_sum[...] + part_in[...].astype(jnp.float32)).astype(jnp.bfloat16)

    def end_send(whiches, h, side, own):
        @pl.when(jnp.logical_not(own))
        def _():
            for which in whiches:
                first_copy(which, h, side).wait_send()

    each_send((0, 1, 2), end_send)

    for step in range(1, y_count):
        for part in range(2):
            far_copy(step, part).wait_send()

    def end_rest(source, carry):
        for far in range(y_count):
            spread(xbuf.at[t, source], source, far).wait_send()
        for far in range(1, y_count):
            relay(source, far, c).wait_send()

        for which in (1, 2):
            forward(which, source).wait_send()

        @pl.when(jnp.logical_not(jnp.logical_and(source == e, mine)))
        def _():
            for v in range(y_count):
                back_copy(source, v).wait_send()

        return carry

    lax.fori_loop(0, ep_count, end_rest, 0)

    def end_near(j, carry):
        dispatch(j).wait_send()
        pass_on(j).wait_send()
        give_back(j).wait_send()
        give_relay(j).wait_send()
        return carry

    lax.fori_loop(1, half_count, end_near, 0)
    cross_copy.wait_send()


def place_kernel(first_ref, second_ref, first_hbm, second_hbm, sem):
    copies = [
        pltpu.make_async_copy(first_ref, first_hbm, sem.at[0]),
        pltpu.make_async_copy(second_ref, second_hbm, sem.at[1]),
    ]
    for copy in copies:
        copy.start()
    for copy in copies:
        copy.wait()


def place_results(results):
    return pl.pallas_call(
        place_kernel,
        out_shape=tuple(jax.ShapeDtypeStruct(r.shape, r.dtype) for r in results),
        in_specs=[pl.BlockSpec(memory_space=pltpu.VMEM)] * 2,
        out_specs=[pl.BlockSpec(memory_space=pltpu.HBM)] * 2,
        scratch_shapes=[pltpu.SemaphoreType.DMA((2,))],
        compiler_params=pltpu.CompilerParams(vmem_limit_bytes=1024 * 1024),
        name="place",
    )(*results)


def mixer(
    tables,
    sequence,
    lambdas,
    head_gain,
    out_proj,
    moe_inputs,
    expert_weights,
    ep_count,
    tp_count,
    capacity,
):
    moe_input, moe_gain, routes, route_weights = moe_inputs
    head_count = lambdas.shape[0]
    half = sequence[0].shape[0] // 2
    width = sequence[0].shape[1] // head_count
    slots = ep_count * capacity
    batch_rows, model = moe_input.shape
    own_rows = batch_rows // tp_count
    top_count = routes.shape[1]
    hidden_width = expert_weights[0].shape[2]
    shared_width = expert_weights[3].shape[1]
    tokens = ep_count * 2 * half
    share = 2 * half // tp_count
    y_count = tp_count // 2
    dma = pltpu.SemaphoreType.DMA
    bf16 = jnp.bfloat16
    return pl.pallas_call(
        functools.partial(mixer_kernel, ep_count, tp_count),
        out_shape=(
            pltpu.VMEM((share, model), bf16),
            pltpu.VMEM((own_rows, model), bf16),
        ),
        in_specs=[pl.BlockSpec(memory_space=pltpu.HBM)] * 18,
        out_specs=[pl.BlockSpec(memory_space=pltpu.VMEM)] * 2,
        scratch_shapes=[
            pltpu.VMEM((1, head_count), jnp.float32),
            pltpu.VMEM(tables[0].shape, jnp.float32),
            pltpu.VMEM(tables[1].shape, jnp.float32),
            pltpu.VMEM(tables[0].shape[1:], jnp.float32),
            pltpu.VMEM(tables[0].shape[1:], jnp.float32),
            pltpu.VMEM((1, width), jnp.float32),
            pltpu.VMEM((1, model), jnp.float32),
            pltpu.VMEM((top_count, batch_rows), jnp.int32),
            pltpu.VMEM((top_count, batch_rows), jnp.float32),
            pltpu.VMEM((batch_rows, model), bf16),
            dma((8,)),
            pltpu.VMEM((batch_rows, model), bf16),
            pltpu.VMEM((slots, model), bf16),
            pltpu.VMEM((batch_rows, slots), jnp.float32),
            pltpu.VMEM((own_rows, model + slots), bf16),
            pltpu.VMEM((own_rows, model + slots), bf16),
            pltpu.VMEM((slots // 2, model), bf16),
            pltpu.VMEM((ep_count // 2, capacity, model), bf16),
            pltpu.VMEM((own_rows, model), bf16),
            pltpu.VMEM((own_rows, model), bf16),
            pltpu.VMEM((3,) + sequence[0].shape, bf16),
            pltpu.VMEM((3, head_count, 2, half, width), bf16),
            dma((3,)),
            pltpu.VMEM(out_proj.shape, bf16),
            pltpu.VMEM((model, hidden_width), bf16),
            pltpu.VMEM((model, hidden_width), bf16),
            pltpu.VMEM((hidden_width, model), bf16),
            pltpu.VMEM((model, shared_width), bf16),
            pltpu.VMEM((model, shared_width), bf16),
            pltpu.VMEM((shared_width, model), bf16),
            pltpu.VMEM((tp_count, ep_count, capacity, model), bf16),
            pltpu.VMEM((tp_count, slots // 2, hidden_width), bf16),
            pltpu.VMEM((y_count, own_rows + slots, model), bf16),
            pltpu.VMEM((y_count, own_rows + slots, model), bf16),
            pltpu.VMEM((y_count, own_rows + slots, model), bf16),
            pltpu.VMEM((max(1, y_count - 1), own_rows + slots, model), bf16),
            pltpu.VMEM((own_rows, model), jnp.float32),
            pltpu.VMEM((ep_count, capacity, model), bf16),
            pltpu.VMEM((ep_count // 2, capacity, model), bf16),
            dma((7,)),
            dma((ep_count,)),
            dma((ep_count,)),
            dma((2,)),
            dma((ep_count // 2,)),
            dma((ep_count,)),
            dma((ep_count // 2,)),
            dma((2,)),
            dma((ep_count, y_count)),
            dma((ep_count, y_count)),
            dma((ep_count, max(1, y_count - 1))),
            dma((ep_count, max(1, y_count - 1))),
            dma((2, 2)),
            dma((2, max(1, y_count - 1))),
            dma((2, max(1, y_count - 1))),
            dma((ep_count,)),
            dma((ep_count,)),
            pltpu.VMEM((ep_count, half, width), bf16),
            pltpu.VMEM((tokens, width), bf16),
            pltpu.VMEM((tokens, width), bf16),
            pltpu.VMEM((8, 128), jnp.float32),
            pltpu.VMEM((8, 128), jnp.float32),
            pltpu.VMEM((ep_count, y_count, share, width), bf16),
            pltpu.VMEM((head_count, y_count, 2, share, width), bf16),
            pltpu.VMEM((y_count, share, model), bf16),
            pltpu.VMEM((y_count, share, model), bf16),
            pltpu.VMEM((y_count, share, model), bf16),
            pltpu.VMEM((max(1, y_count - 1), share, model), bf16),
            pltpu.VMEM((max(1, y_count - 1), share, model), bf16),
            dma((3, head_count, 2)),
            dma((3, ep_count)),
            dma((3,)),
            dma((2, ep_count)),
            dma((2, ep_count)),
            dma((2,)),
            dma((ep_count, y_count)),
            dma((head_count, y_count, 2)),
            dma((y_count, 2)),
            dma((y_count, 2)),
            dma((max(1, y_count - 1), 2)),
            dma((max(1, y_count - 1), 2)),
        ],
        compiler_params=pltpu.CompilerParams(
            has_side_effects=True, vmem_limit_bytes=62000000, collective_id=0
        ),
        name="mixer",
    )(
        lambdas[None, :],
        *tables,
        head_gain[None, :],
        moe_gain[None, :],
        jnp.transpose(routes),
        jnp.transpose(route_weights),
        moe_input,
        *sequence,
        out_proj,
        *expert_weights,
    )


def local(
    queries,
    key_rows,
    value_rows,
    lambdas,
    head_gain,
    out_proj,
    moe_input,
    moe_gain,
    routes,
    route_weights,
    expert_gate,
    expert_up,
    expert_down,
    shared_gate,
    shared_up,
    shared_down,
):
    query_rows = queries.shape[0]
    head_count = lambdas.shape[0]
    head_dim = queries.shape[1] // (2 * head_count)
    tp_count = lax.axis_size("tp")
    ep_count = lax.axis_size("ep")
    tp_place = lax.axis_index("tp")
    ep_place = lax.axis_index("ep")
    positions = ep_place * query_rows + jnp.arange(query_rows, dtype=jnp.int32)
    batch_rows = moe_input.shape[0]
    top_count = routes.shape[1]
    own_rows = batch_rows // tp_count
    local_experts = expert_gate.shape[0]
    expert_count = local_experts * ep_count
    capacity = (2 * own_rows * top_count + expert_count - 1) // expert_count
    one_head_each = ep_count == 2 * head_count and tp_count % 2 == 0 and local_experts == 1 and ep_count % 4 == 0 and expert_count * capacity % 128 == 0
    if one_head_each:
        tables = rotation_tables(query_rows, ep_count, head_dim)
        sequence = (queries, key_rows, value_rows)
        weights = (expert_gate, expert_up, expert_down, shared_gate, shared_up, shared_down)
        return place_results(mixer(
            tables,
            sequence,
            lambdas,
            head_gain,
            out_proj,
            (moe_input, moe_gain, routes, route_weights),
            weights,
            ep_count,
            tp_count,
            capacity,
        ))
    else:
        rot_query = rotate(queries, positions, head_dim)
        rot_keys = rotate(key_rows, positions, head_dim)
        initial = (
            jnp.full((head_count, 2, query_rows), -1e30, jnp.float32),
            jnp.zeros((head_count, 2, query_rows), jnp.float32),
            jnp.zeros((head_count, 2, query_rows, 2 * head_dim), jnp.float32),
        )
        running_max, denominator, numerator = fold_keys(
            initial,
            (
                lax.all_gather(rot_keys, "ep", axis=0, tiled=True),
                lax.all_gather(value_rows, "ep", axis=0, tiled=True),
            ),
            rot_query,
            head_count,
            head_dim,
        )
        ratio = numerator / denominator[..., None]
        mixed_heads = ratio[:, 0] - lambdas[:, None, None] * ratio[:, 1]
        mean_square = jnp.mean(mixed_heads * mixed_heads, axis=-1, keepdims=True)
        normed_heads = (mixed_heads * lax.rsqrt(mean_square + head_eps) * head_gain).astype(
            jnp.bfloat16
        )
        head_out = jnp.transpose(normed_heads, (1, 0, 2)).reshape(query_rows, head_count * 2 * head_dim)
    normed = rms_rows(moe_input, moe_gain)
    shared_hidden = gated_hidden(normed, shared_gate, shared_up)
    own_routes = lax.dynamic_slice_in_dim(routes, tp_place * own_rows, own_rows, 0)
    own_weights = lax.dynamic_slice_in_dim(route_weights, tp_place * own_rows, own_rows, 0)
    own_source, own_filled, own_rank = slot_table(own_routes, expert_count, capacity)
    own_normed = lax.dynamic_slice_in_dim(normed, tp_place * own_rows, own_rows, 0)
    outgoing = fill_slots(own_normed, own_source, own_filled)
    arrived = lax.all_to_all(outgoing[:, None], "ep", split_axis=0, concat_axis=2, tiled=True)
    hidden = slot_hidden(lax.all_gather(arrived, "tp", axis=1, tiled=True), expert_gate, expert_up)
    slot_rows = local_experts * ep_count * capacity
    mixer_share = query_rows // tp_count
    expert_share = own_rows + slot_rows
    if not one_head_each:
        block_count = lax.axis_size("tp") * mixer_share // mixer_share
        product = jnp.dot(head_out, out_proj, preferred_element_type=jnp.float32)
        mixer_out = lax.psum_scatter(
            product.reshape(block_count, mixer_share, -1)
            .reshape(lax.axis_size("tp") * mixer_share, -1)
            .astype(jnp.bfloat16),
            "tp",
            scatter_dimension=0,
            tiled=True,
        )
    block_count = lax.axis_size("tp") * expert_share // expert_share
    shared_part = jnp.dot(shared_hidden, shared_down, preferred_element_type=jnp.float32).reshape(
        block_count, own_rows, -1
    )
    routed_part = jnp.einsum(
        "xnsf,xfd->nxsd", hidden, expert_down, preferred_element_type=jnp.float32
    )
    routed_part = routed_part.reshape(block_count, slot_rows, -1)
    expert_sum = lax.psum_scatter(
        jnp.concatenate([shared_part, routed_part], axis=1)
        .reshape(lax.axis_size("tp") * expert_share, -1)
        .astype(jnp.bfloat16),
        "tp",
        scatter_dimension=0,
        tiled=True,
    ).astype(jnp.float32)
    shared_sum = expert_sum[:own_rows]
    routed = (
        expert_sum[own_rows:].reshape(local_experts, ep_count * capacity, -1).astype(jnp.bfloat16)
    )
    returned = lax.all_to_all(routed, "ep", split_axis=1, concat_axis=0, tiled=True)
    flat_index = (own_routes * capacity + own_rank).reshape(-1)
    picked = jnp.take(returned.reshape(expert_count * capacity, -1), flat_index, axis=0).reshape(
        own_rows, top_count, -1
    )
    combined = shared_sum + jnp.sum(own_weights[..., None] * picked.astype(jnp.float32), axis=1)
    return (mixer_out, combined.astype(jnp.bfloat16))


def solution(mesh):
    in_specs = (
        P("ep", "tp"),
        P("ep", "tp"),
        P("ep", "tp"),
        P("tp"),
        P(),
        P("tp", None),
        P("ep", None),
        P(),
        P("ep", None),
        P("ep", None),
        P("ep", None, "tp"),
        P("ep", None, "tp"),
        P("ep", "tp", None),
        P(None, "tp"),
        P(None, "tp"),
        P("tp", None),
    )
    out_specs = (P(("ep", "tp"), None), P(("ep", "tp"), None))
    return jax.shard_map(local, mesh=mesh, in_specs=in_specs, out_specs=out_specs, check_vma=False)
```

```python
import functools
import jax
import jax.numpy as jnp
import numpy as np
from jax import lax
from jax.experimental import pallas as pl
from jax.experimental.pallas import tpu as pltpu
from jax.sharding import PartitionSpec as P

theta_base = 500000.0
norm_eps = 1e-06
head_eps = 1e-05
MESH = pl.DeviceIdType.MESH
log2_e = 1.4426950408889634


def rotate(matrix, positions, head_dim):
    row_count = matrix.shape[0]
    shaped = matrix.reshape(row_count, -1, head_dim).astype(jnp.float32)
    half_dim = head_dim // 2
    frequency = jnp.power(theta_base, -jnp.arange(half_dim, dtype=jnp.float32) * 2.0 / head_dim)
    angles = positions.astype(jnp.float32)[:, None] * frequency[None, :]
    cosine = jnp.cos(angles)[:, None, :]
    sines = jnp.sin(angles)[:, None, :]
    front_half = shaped[..., :half_dim]
    second = shaped[..., half_dim:]
    turned = jnp.concatenate(
        [front_half * cosine - second * sines, second * cosine + front_half * sines], axis=-1
    )
    return turned.reshape(matrix.shape).astype(jnp.bfloat16)


def rms_rows(values, gain):
    widened = values.astype(jnp.float32)
    mean_square = jnp.mean(widened * widened, axis=-1, keepdims=True)
    return (widened * lax.rsqrt(mean_square + norm_eps) * gain).astype(jnp.bfloat16)


def gated_hidden(rows_in, gate_weight, up_weight):
    gate_part = jnp.dot(rows_in, gate_weight, preferred_element_type=jnp.float32)
    up_part = jnp.dot(rows_in, up_weight, preferred_element_type=jnp.float32)
    return (jax.nn.silu(gate_part) * up_part).astype(jnp.bfloat16)


def slot_hidden(slot_rows, gate_weight, up_weight):
    gate_part = jnp.einsum(
        "xnsd,xdf->xnsf", slot_rows, gate_weight, preferred_element_type=jnp.float32
    )
    up_part = jnp.einsum("xnsd,xdf->xnsf", slot_rows, up_weight, preferred_element_type=jnp.float32)
    return (jax.nn.silu(gate_part) * up_part).astype(jnp.bfloat16)


def key_block_size(piece_rows):
    for candidate in (1024, 512):
        return candidate
    return piece_rows


def fold_keys(state_in, pieces, rot_query, head_count, head_dim):
    keys_piece, values_piece = pieces
    piece_rows = keys_piece.shape[0]
    block_rows = key_block_size(piece_rows)
    block_count = piece_rows // block_rows
    query_view = rot_query.reshape(rot_query.shape[0], head_count, 2, head_dim)
    score_scale = head_dim ** (-0.5)

    def one_block(running, key_block):
        running_max, denominator, numerator = running
        key_view = key_block[0].reshape(block_rows, head_count, 2, head_dim)
        value_view = key_block[1].reshape(block_rows, head_count, 2 * head_dim)
        scores = (
            jnp.einsum("qhmd,khmd->hmqk", query_view, key_view, preferred_element_type=jnp.float32)
            * score_scale
        )
        newest = jnp.maximum(running_max, jnp.max(scores, axis=-1))
        weights = jnp.exp(scores - newest[..., None])
        shrink = jnp.exp(running_max - newest)
        denominator = denominator * shrink + jnp.sum(weights, axis=-1)
        weighted = jnp.einsum(
            "hmqk,khe->hmqe",
            weights.astype(jnp.bfloat16),
            value_view,
            preferred_element_type=jnp.float32,
        )
        numerator = numerator * shrink[..., None] + weighted
        return ((newest, denominator, numerator), None)

    blocks = (
        keys_piece.reshape(block_count, block_rows, -1),
        values_piece.reshape(block_count, block_rows, -1),
    )
    result, _ = lax.scan(one_block, state_in, blocks)
    return result


def slot_table(route_block, expert_count, capacity):
    flat_routes = route_block.reshape(-1)
    route_total = flat_routes.shape[0]
    top_count = route_block.shape[1]
    experts_iota = jnp.arange(expert_count, dtype=jnp.int32)
    onehot = (flat_routes[:, None] == experts_iota[None, :]).astype(jnp.int32)
    before = jnp.cumsum(onehot, axis=0) - onehot
    slot_rank = jnp.sum(before * onehot, axis=1)
    slot_iota = jnp.arange(capacity, dtype=jnp.int32)
    matches = (flat_routes[None, None, :] == experts_iota[:, None, None]) & (
        slot_rank[None, None, :] == slot_iota[None, :, None]
    )
    source_row = jnp.arange(route_total, dtype=jnp.int32) // top_count
    source = jnp.sum(jnp.where(matches, source_row[None, None, :], 0), axis=2)
    filled = jnp.any(matches, axis=2)
    return (source, filled, slot_rank.reshape(route_block.shape))


def fill_slots(rows_src, source, filled):
    taken = jnp.take(rows_src, source.reshape(-1), axis=0).reshape(
        source.shape + (rows_src.shape[1],)
    )
    return jnp.where(filled[..., None], taken, jnp.zeros_like(taken))


def rotation_tables(row_count, block_count, head_dim):
    half_dim = head_dim // 2
    frequency = np.power(theta_base, -np.arange(half_dim) * 2.0 / head_dim)

    def table(positions):
        angles = positions[:, None] * frequency[None, :]
        cosine, sines = np.cos(angles), np.sin(angles)
        both = (np.concatenate([cosine, cosine], 1), np.concatenate([-sines, sines], 1))
        return np.stack(both).astype(np.float32)

    return (
        jnp.asarray(table(np.arange(row_count))),
        jnp.asarray(table(np.arange(block_count) * row_count)),
    )


def mixer_kernel(
    ep_count,
    tp_count,
    lam_hbm,
    turn_hbm,
    base_hbm,
    gain_hbm,
    mgain_hbm,
    routes_hbm,
    scale_hbm,
    rows_hbm,
    q_hbm,
    k_hbm,
    v_hbm,
    proj_hbm,
    gate_hbm,
    up_hbm,
    down_hbm,
    sgate_hbm,
    sup_hbm,
    sdown_hbm,
    out_ref,
    moe_ref,
    lam_ref,
    turn_ref,
    base_ref,
    cos_ref,
    sin_ref,
    gain_ref,
    mgain_ref,
    routes_ref,
    scale_ref,
    rows_ref,
    small_sem,
    norm_ref,
    slot_ref,
    mix_ref,
    ext_out,
    ext_in,
    rel_slots,
    gathered,
    part_out,
    part_in,
    raw,
    pack_ref,
    q_sem,
    proj_ref,
    gate_ref,
    up_ref,
    down_ref,
    sgate_ref,
    sup_ref,
    sdown_ref,
    xbuf,
    hidden,
    pair_out,
    pair_own,
    pair_in,
    far_in,
    shared_sum,
    ret_out,
    ret_in,
    w_sem,
    d_send,
    d_recv,
    c_sem,
    k_send,
    u_send,
    u_recv,
    m_sem,
    g_send,
    g_recv,
    h_send,
    h_recv,
    p_sem,
    y_send,
    y_recv,
    v_send,
    v_recv,
    qbuf,
    kbuf,
    vbuf,
    lam_own,
    lam_other,
    obuf,
    heads,
    sum_out,
    sum_in,
    kept,
    block_out,
    block_in,
    s_send,
    s_recv,
    s_local,
    f_send,
    f_recv,
    l_sem,
    o_send,
    o_recv,
    r_send,
    r_recv,
    b_send,
    b_recv,
):
    head_count = pack_ref.shape[1]
    half, width = pack_ref.shape[3], pack_ref.shape[4]
    head_dim = width // 2
    e = lax.axis_index("ep")
    t = lax.axis_index("tp")
    y, c = t // 2, lax.rem(t, 2)
    partner = y * 2 + 1 - c
    s_me, h_me = e // head_count, lax.rem(e, head_count)
    y_count = tp_count // 2
    share = half // y_count

    barrier = pltpu.get_barrier_semaphore()

    def greet(where):
        pl.semaphore_signal(barrier, inc=1, device_id=where, device_id_type=MESH)

    def greet_row(j, carry):
        there = lax.rem(e + j, ep_count)
        for core in range(2):
            greet((there, y * 2 + core))
        return carry

    lax.fori_loop(1, ep_count, greet_row, 0)
    greet((e, partner))
    for step in range(1, y_count):
        greet((e, lax.rem(y + step, y_count) * 2 + c))

    def remote(src, dst, send, recv, where):
        return pltpu.make_async_remote_copy(
            src_ref=src,
            dst_ref=dst,
            send_sem=send,
            recv_sem=recv,
            device_id=where,
            device_id_type=MESH,
        )

    small_copies = [
        pltpu.make_async_copy(a, b, small_sem.at[at])
        for at, (a, b) in enumerate(
            (
                (routes_hbm, routes_ref),
                (scale_hbm, scale_ref),
                (mgain_hbm, mgain_ref),
                (lam_hbm, lam_ref),
                (rows_hbm, rows_ref),
                (base_hbm, base_ref),
                (turn_hbm, turn_ref),
                (gain_hbm, gain_ref),
            )
        )
    ]
    for copy in small_copies:
        copy.start()
    raw_copies = [
        pltpu.make_async_copy(ref, raw.at[at], q_sem.at[at])
        for at, ref in enumerate((q_hbm, k_hbm, v_hbm))
    ]
    for copy in raw_copies:
        copy.start()
    weight_copies = [
        pltpu.make_async_copy(a, b, w_sem.at[at])
        for at, (a, b) in enumerate(
            (
                (sgate_hbm, sgate_ref),
                (sup_hbm, sup_ref),
                (sdown_hbm, sdown_ref),
                (gate_hbm.at[0], gate_ref),
                (up_hbm.at[0], up_ref),
                (down_hbm.at[0], down_ref),
                (proj_hbm, proj_ref),
            )
        )
    ]
    def landing(which, side, source):
        if which == 0:
            return qbuf.at[source]
        return (kbuf, vbuf)[which - 1].at[pl.ds((side * ep_count + source) * half, half)]

    def first_copy(which, h, side):
        return remote(
            pack_ref.at[which, h, side],
            landing(which, side, e),
            s_send.at[which, h, side],
            s_recv.at[which, e],
            (c * head_count + h, y * 2 + side),
        )

    def own_copy(which):
        return pltpu.make_async_copy(
            pack_ref.at[which, h_me, c], landing(which, c, e), s_local.at[which]
        )

    def forward(which, source):
        place = landing(which, c, source)
        return remote(
            place, place, f_send.at[which - 1, source], f_recv.at[which - 1, source], (e, partner)
        )

    capacity = xbuf.shape[2]
    own_rows = moe_ref.shape[0]
    slots = ep_count * capacity
    batch_rows = rows_ref.shape[0]
    model = rows_ref.shape[1]
    half_count = ep_count // 2
    half_slots = half_count * capacity
    across = lax.rem(e + half_count, ep_count)
    near_first = s_me * half_count
    place_me = lax.rem(e, half_count)

    def near(j):
        return near_first + lax.rem(place_me + j, half_count)

    for copy in small_copies[:5]:
        copy.wait()
    widened = rows_ref[...].astype(jnp.float32)
    mean_square = jnp.mean(widened * widened, axis=-1, keepdims=True)
    norm_ref[...] = (widened * lax.rsqrt(mean_square + norm_eps) * mgain_ref[...]).astype(
        jnp.bfloat16
    )
    slot_at = lax.broadcasted_iota(jnp.int32, (slots, batch_rows), 0)
    slot_expert, slot_rank = slot_at // capacity, lax.rem(slot_at, capacity)
    hits = [routes_ref[k : k + 1, :] == slot_expert for k in range(routes_ref.shape[0])]
    named = sum(hit.astype(jnp.float32) for hit in hits).astype(jnp.bfloat16)
    other_at = lax.broadcasted_iota(jnp.int32, (batch_rows, batch_rows), 0)
    row_at = lax.broadcasted_iota(jnp.int32, (batch_rows, batch_rows), 1)
    earlier = jnp.logical_and(other_at < row_at, other_at // own_rows == row_at // own_rows)
    before = jnp.dot(
        named, earlier.astype(jnp.float32).astype(jnp.bfloat16), preferred_element_type=jnp.float32
    ).astype(jnp.int32)
    chosen = [jnp.logical_and(hit, before == slot_rank).astype(jnp.float32) for hit in hits]
    token_block = lax.broadcasted_iota(jnp.int32, (slots, batch_rows), 1) // own_rows
    picked = jnp.where(token_block == t, sum(chosen), 0.0).astype(jnp.bfloat16)
    slot_ref[...] = jnp.dot(
        picked, norm_ref[...], preferred_element_type=jnp.float32
    ).astype(jnp.bfloat16)
    mixing = sum(scale_ref[k : k + 1, :] * chosen[k] for k in range(len(chosen)))
    mix_ref[...] = jnp.transpose(mixing)
    head_at = lax.broadcasted_iota(jnp.int32, lam_ref.shape, 1)
    lam_mine = jnp.sum(
        jnp.where(head_at == h_me, lam_ref[...], 0.0), axis=1, keepdims=True
    )
    lam_own[...] = jnp.broadcast_to(lam_mine, lam_own.shape)

    def fold(wide):
        return jnp.where(s_me == 0, wide[:, half_slots:], wide[:, :half_slots])

    own_span = pl.ds(pl.multiple_of(t * own_rows, own_rows), own_rows)
    away = fold(mix_ref[own_span, :])
    away_coarse = away.astype(jnp.bfloat16)
    away_fine = (away - away_coarse.astype(jnp.float32)).astype(jnp.bfloat16)
    ext_out[:, :model] = norm_ref[own_span, :]
    ext_out[:, model:] = jnp.concatenate([away_coarse, away_fine], axis=1)

    for copy in small_copies[5:7]:
        copy.wait()
    base_cos, base_sin = base_ref[0, pl.ds(e, 1), :], base_ref[1, pl.ds(e, 1), :]
    cos_ref[...] = base_cos * turn_ref[0] - base_sin * turn_ref[1]
    sin_ref[...] = base_sin * turn_ref[0] + base_cos * turn_ref[1]
    for copy in raw_copies:
        copy.wait()

    def pack_head(h, carry):
        cosine = cos_ref[...]
        sines = sin_ref[...]
        for which in range(2):
            for m in range(2):
                at = pl.multiple_of(h * width + m * head_dim, head_dim)
                part = raw[which, :, pl.ds(at, head_dim)].astype(jnp.float32)
                turned = part * cosine + pltpu.roll(part, head_dim // 2, 1) * sines
                turned = turned.astype(jnp.bfloat16)
                for v in range(y_count):
                    for side in range(2):
                        block = v * 2 + side
                        pack_ref[
                            which,
                            h,
                            side,
                            v * share : (v + 1) * share,
                            m * head_dim : (m + 1) * head_dim,
                        ] = turned[block * share : (block + 1) * share]
        at = pl.multiple_of(h * width, width)
        for v in range(y_count):
            for side in range(2):
                block = v * 2 + side
                pack_ref[2, h, side, v * share : (v + 1) * share] = raw[
                    2, block * share : (block + 1) * share, pl.ds(at, width)
                ]
        return carry

    lax.fori_loop(0, head_count, pack_head, 0)

    pl.semaphore_wait(barrier, (ep_count - 1) * 2 + 1 + (y_count - 1))

    for copy in weight_copies:
        copy.start()

    def dispatch(j):
        target, at = near(j), half_count - j
        rows = pl.ds(pl.multiple_of(target * capacity, capacity), capacity)
        return remote(
            slot_ref.at[rows], xbuf.at[t, at], d_send.at[target], d_recv.at[at], (target, t)
        )

    cross_copy = remote(ext_out, ext_in, c_sem.at[0], c_sem.at[1], (across, t))
    cross_copy.start()

    def start_dispatch(j, carry):
        dispatch(j).start()
        return carry

    lax.fori_loop(1, half_count, start_dispatch, 0)

    mine = s_me == c

    def each_send(whiches, act):
        def body(j, carry):
            h = lax.rem(h_me + 1 + j, head_count)
            for k in range(2):
                side = lax.rem(c + 1 + k, 2)
                own = jnp.logical_and(c * head_count + h == e, side == c)
                act(whiches, h, side, own)
            return carry

        lax.fori_loop(0, head_count, body, 0)

    def start_send(whiches, h, side, own):
        @pl.when(jnp.logical_not(own))
        def _():
            for which in whiches:
                first_copy(which, h, side).start()

    pair_count = ep_count // 2
    pair_me = e // 2
    near_pairs = pair_count // 2
    beside = jnp.logical_or(pair_me == near_pairs - 1, pair_me == near_pairs)
    at_once = jnp.logical_and(jnp.logical_not(mine), beside)

    @pl.when(at_once)
    def _():
        each_send((1, 2), start_send)
        each_send((0,), start_send)

    lam_copy = remote(lam_own, lam_other, l_sem.at[0], l_sem.at[1], (e, partner))
    lam_copy.start()
    xbuf[t, 0] = slot_ref[pl.ds(pl.multiple_of(e * capacity, capacity), capacity), :]

    def spread(place, source, far):
        if far == 0:
            sends, recvs, where = g_send.at[source, 0], g_recv.at[source, 0], (e, partner)
        else:
            there = lax.rem(y + far, y_count)
            sends, recvs = g_send.at[source, far], g_recv.at[source, far]
            where = (e, there * 2 + c)
        return remote(place, place, sends, recvs, where)

    def hand_out(source):
        place = xbuf.at[t, source]
        for far in range(1, y_count):
            spread(place, source, far).start()
        spread(place, source, 0).start()

    def relay(source, far, core):
        from_y = lax.rem(y + y_count - far, y_count)
        place = xbuf.at[from_y * 2 + core, source]
        return remote(
            place, place, h_send.at[source, far - 1], h_recv.at[source, far - 1], (e, partner)
        )

    def arrive_slots(at, carry):
        place = xbuf.at[t, at]
        remote(place, place, d_send.at[at], d_recv.at[at], (e, partner)).wait_recv()
        hand_out(at)
        return carry

    def arrive_far(source, carry):
        for far in range(1, y_count):
            from_y = lax.rem(y + y_count - far, y_count)
            spread(xbuf.at[from_y * 2 + c, source], source, far).wait_recv()
            relay(source, far, c).start()
        return carry

    def arrive_relay(source, carry):
        spread(xbuf.at[partner, source], source, 0).wait_recv()
        for far in range(1, y_count):
            relay(source, far, 1 - c).wait_recv()
        return carry

    hand_out(0)

    for copy in weight_copies[:3]:
        copy.wait()
    normed = norm_ref[...]
    gate_part = jnp.dot(normed, sgate_ref[...], preferred_element_type=jnp.float32)
    up_part = jnp.dot(normed, sup_ref[...], preferred_element_type=jnp.float32)
    shared_hidden = (gate_part / (1.0 + jnp.exp(-gate_part)) * up_part).astype(jnp.bfloat16)
    shared_part = jnp.dot(
        shared_hidden, sdown_ref[...], preferred_element_type=jnp.float32
    ).astype(jnp.bfloat16)
    for v in range(y_count):
        for core in range(2):
            block = shared_part[(v * 2 + core) * own_rows : (v * 2 + core + 1) * own_rows]

            @pl.when(c == core)
            def _():
                pair_own[v, :own_rows, :] = block

            @pl.when(c != core)
            def _():
                pair_out[v, :own_rows, :] = block

    lax.fori_loop(1, half_count, arrive_slots, 0)
    cross_copy.wait_recv()
    sent_rows = ext_in[:, :model]
    sent_mix = ext_in[:, model:]
    taken = (sent_mix[:, :half_slots].astype(jnp.float32) > 0.0).astype(jnp.float32)
    rel_slots[...] = lax.dot_general(
        taken.astype(jnp.bfloat16),
        sent_rows,
        (((0,), (0,)), ((), ())),
        preferred_element_type=jnp.float32,
    ).astype(jnp.bfloat16)

    def pass_on(j):
        to, at = lax.rem(place_me + j, half_count), half_count + (half_count - j)
        rows = pl.ds(pl.multiple_of(to * capacity, capacity), capacity)
        return remote(
            rel_slots.at[rows],
            xbuf.at[t, at],
            k_send.at[to],
            d_recv.at[at],
            (near_first + to, t),
        )

    def start_pass(j, carry):
        pass_on(j).start()
        return carry

    lax.fori_loop(1, half_count, start_pass, 0)
    xbuf[t, half_count] = rel_slots[
        pl.ds(pl.multiple_of(place_me * capacity, capacity), capacity), :
    ]

    @pl.when(jnp.logical_not(at_once))
    def _():
        each_send((1, 2), start_send)
        each_send((0,), start_send)

    @pl.when(mine)
    def _():
        for which in range(3):
            own_copy(which).start()

    hand_out(half_count)
    lax.fori_loop(0, half_count, arrive_far, 0)
    lax.fori_loop(half_count + 1, ep_count, arrive_slots, 0)

    def part_rows(part):
        first = own_rows + part * half_slots
        return slice(first if part else 0, first + half_slots)

    def down_part(core, into, part):
        rows = jnp.concatenate([hidden[v * 2 + core] for v in range(y_count)], axis=0)
        product = jnp.dot(rows, down_ref[...], preferred_element_type=jnp.float32)
        product = product.astype(jnp.bfloat16)
        first = own_rows + part * half_slots
        for v in range(y_count):
            into[v, first : first + half_slots, :] = product[v * half_slots : (v + 1) * half_slots]

    def far_copy(step, part):
        target = lax.rem(y + step, y_count)
        rows = part_rows(part)
        return remote(
            pair_own.at[target, rows],
            far_in.at[step - 1, rows],
            y_send.at[part, step - 1],
            y_recv.at[part, step - 1],
            (e, target * 2 + c),
        )

    for part in range(2):
        first, last = part * half_count, (part + 1) * half_count
        if part > 0:
            lax.fori_loop(first, last, arrive_far, 0)
        lax.fori_loop(first, last, arrive_relay, 0)
        if part == 0:
            for copy in weight_copies[3:6]:
                copy.wait()
        rows_in = xbuf[:, first:last].reshape(tp_count * half_slots, model)
        gate_part = jnp.dot(rows_in, gate_ref[...], preferred_element_type=jnp.float32)
        up_part = jnp.dot(rows_in, up_ref[...], preferred_element_type=jnp.float32)
        hidden[...] = (
            (gate_part / (1.0 + jnp.exp(-gate_part)) * up_part).astype(jnp.bfloat16)
        ).reshape(hidden.shape)
        down_part(1 - c, pair_out, part)
        rows = part_rows(part)
        near_copy = remote(
            pair_out.at[:, rows], pair_in.at[:, rows], p_sem.at[part, 0], p_sem.at[part, 1], (e, partner)
        )
        near_copy.start()
        down_part(c, pair_own, part)
        near_copy.wait()
        pair_own[:, rows] = (
            pair_own[:, rows].astype(jnp.float32) + pair_in[:, rows].astype(jnp.float32)
        ).astype(jnp.bfloat16)
        for step in range(1, y_count):
            far_copy(step, part).start()

    def give_back(j):
        return remote(
            ret_out.at[j], ret_in.at[place_me], v_send.at[j], v_recv.at[place_me], (near(j), t)
        )

    def give_relay(j):
        return remote(
            ret_out.at[half_count + j], gathered.at[place_me], u_send.at[j], u_recv.at[place_me], (near(j), t)
        )

    def finish_experts(part):
        rows = part_rows(part)
        for step in range(1, y_count):
            far_copy(step, part).wait_recv()
        expert_sum = pair_own[y, rows].astype(jnp.float32)
        for step in range(1, y_count):
            expert_sum = expert_sum + far_in[step - 1, rows].astype(jnp.float32)
        if part == 0:
            shared_sum[...] = expert_sum[:own_rows]
            expert_sum = expert_sum[own_rows:]
        first, last = part * half_count, (part + 1) * half_count
        ret_out[first:last] = expert_sum.astype(jnp.bfloat16).reshape(
            (half_count,) + ret_out.shape[1:]
        )
        give = (give_back, give_relay)[part]

        def start_give(j, carry):
            give(j).start()
            return carry

        lax.fori_loop(1, half_count, start_give, 0)
        (ret_in, gathered)[part][place_me] = ret_out[first]

    def arrived(which, source):
        own = jnp.logical_and(source == e, mine)

        @pl.when(own)
        def _():
            own_copy(which).wait()

        @pl.when(jnp.logical_not(own))
        def _():
            place = landing(which, c, source)
            remote(
                place, place, f_send.at[0, source], s_recv.at[which, source], (e, partner)
            ).wait_recv()

    def arrive(j, carry):
        source = lax.rem(e + j, ep_count)
        for which in (1, 2):
            arrived(which, source)
            forward(which, source).start()
        return carry

    lax.fori_loop(0, ep_count, arrive, 0)

    def arrive_forward(j, carry):
        source = lax.rem(e + j, ep_count)
        for which in (1, 2):
            place = landing(which, 1 - c, source)
            remote(
                place,
                place,
                f_send.at[which - 1, source],
                f_recv.at[which - 1, source],
                (e, partner),
            ).wait_recv()
        return carry

    lax.fori_loop(0, ep_count, arrive_forward, 0)
    lam_copy.wait()
    small_copies[7].wait()

    lam = jnp.where(mine, lam_own[...], lam_other[...])[0:1, 0:1]
    gain = gain_ref[...]
    factor = head_dim ** (-0.5) * log2_e

    def back_place(v):
        return heads.at[h_me, v, c]

    def back_copy(target, v):
        return remote(
            obuf.at[target, v],
            back_place(v),
            o_send.at[target, v],
            o_recv.at[h_me, v, c],
            (target, y * 2 + s_me),
        )

    def back_own(v):
        return pltpu.make_async_copy(obuf.at[e, v], back_place(v), o_recv.at[h_me, v, c])

    def attend(pieces):
        def rows_of(v):
            return pl.ds(pl.multiple_of(v * share, share), share)

        block = jnp.concatenate([qbuf[target, rows_of(v), :] for target, v in pieces], axis=0)
        ratios = []
        for m in range(2):
            columns = slice(m * head_dim, (m + 1) * head_dim)
            scores = lax.dot_general(
                block[:, columns],
                kbuf[:, columns],
                (((1,), (1,)), ((), ())),
                preferred_element_type=jnp.float32,
            )
            top = jnp.max(scores, axis=-1, keepdims=True)
            weights = jnp.exp2((scores - top) * factor)
            denominator = jnp.sum(weights, axis=-1, keepdims=True)
            weighted = jnp.dot(
                weights.astype(jnp.bfloat16), vbuf[...], preferred_element_type=jnp.float32
            )
            ratios.append(weighted / denominator)
        mixed = ratios[0] - lam * ratios[1]
        mean_square = jnp.mean(mixed * mixed, axis=-1, keepdims=True)
        done = (mixed * lax.rsqrt(mean_square + head_eps) * gain).astype(jnp.bfloat16)
        for k, (target, v) in enumerate(pieces):
            obuf[target, v] = done[k * share : (k + 1) * share]
        for target, v in pieces:
            own = jnp.logical_and(target == e, mine)

            @pl.when(jnp.logical_not(own))
            def _():
                back_copy(target, v).start()

            @pl.when(own)
            def _():
                back_own(v).start()

    pair_first = s_me * near_pairs

    def beyond_pair(k):
        return (1 - s_me) * (pair_count - 1 - k) + s_me * k

    def near_pair(k):
        return pair_first + lax.rem(pair_me + k, near_pairs)

    v_order = [lax.rem(y + 1 + j, y_count) for j in range(y_count)]

    def await_queries(pair):
        for k in range(2):
            arrived(0, pair * 2 + k)

    def both(pair, v):
        return [(pair * 2 + k, v) for k in range(2)]

    def attend_near(v):
        attend([piece for k in range(near_pairs) for piece in both(near_pair(k), v)])

    def attend_beyond(k):
        await_queries(beyond_pair(k))
        attend([piece for v in v_order for piece in both(beyond_pair(k), v)])

    for k in range(near_pairs):
        await_queries(near_pair(k))
    attend_near(v_order[0])
    finish_experts(0)
    attend_beyond(0)
    finish_experts(1)
    for v in v_order[1:]:
        attend_near(v)
    for k in range(1, near_pairs):
        await_queries(beyond_pair(k))
        for v in v_order:
            attend(both(beyond_pair(k), v))

    def arrive_gathered(j, carry):
        place = gathered.at[lax.rem(place_me + j, half_count)]
        remote(
            place, place, u_send.at[j], u_recv.at[lax.rem(place_me + j, half_count)], (e, partner)
        ).wait_recv()
        return carry

    part_copy = remote(part_out, part_in, m_sem.at[0], m_sem.at[1], (across, t))

    def mix_across():
        lax.fori_loop(1, half_count, arrive_gathered, 0)
        all_gathered = gathered[...].reshape(half_slots, model)
        cross_mix = ext_in[:, model:]
        part = jnp.dot(cross_mix[:, :half_slots], all_gathered, preferred_element_type=jnp.float32)
        part = part + jnp.dot(
            cross_mix[:, half_slots:], all_gathered, preferred_element_type=jnp.float32
        )
        part_out[...] = part.astype(jnp.bfloat16)
        part_copy.start()

    pl.when(beside)(mix_across)

    weight_copies[6].wait()

    column_parts = 2
    part_width = model // column_parts

    def columns_of(part):
        return slice(part * part_width, (part + 1) * part_width)

    def pair_copy(at, part):
        columns = columns_of(part)
        return remote(
            sum_out.at[at, :, columns],
            sum_in.at[at, :, columns],
            r_send.at[at, part],
            r_recv.at[at, part],
            (e, partner),
        )

    def pair_sum(at, part):
        pair_copy(at, part).wait()
        columns = columns_of(part)
        mine_part = kept[at, :, columns].astype(jnp.float32)
        return (mine_part + sum_in[at, :, columns].astype(jnp.float32)).astype(jnp.bfloat16)

    def project(at):
        v = lax.rem(y + 1 + at, y_count)

        def arrive_heads(h, carry):
            for side in range(2):
                own = jnp.logical_and(
                    jnp.logical_and(c * head_count + h == e, side == c), h == h_me
                )
                place = heads.at[h, v, side]

                @pl.when(own)
                def _():
                    back_own(v).wait()

                @pl.when(jnp.logical_not(own))
                def _():
                    remote(
                        place, place, o_send.at[0, 0], o_recv.at[h, v, side], (e, partner)
                    ).wait_recv()

            return carry

        lax.fori_loop(0, head_count, arrive_heads, 0)
        rows = [
            jnp.concatenate([heads[h, v, 1 - c], heads[h, v, c]], axis=0)
            for h in range(head_count)
        ]
        for part in range(column_parts):
            columns = columns_of(part)
            total = None
            for h in range(head_count):
                term = jnp.dot(
                    rows[h],
                    proj_ref[h * width : (h + 1) * width, columns],
                    preferred_element_type=jnp.float32,
                )
                total = term if total is None else total + term
            total = total.astype(jnp.bfloat16)
            sum_out[at, :, columns] = total[:share]
            kept[at, :, columns] = total[share:]
            pair_copy(at, part).start()

    def block_copy(step, part):
        target = lax.rem(y + step, y_count)
        columns = columns_of(part)
        return remote(
            block_out.at[step - 1, :, columns],
            block_in.at[step - 1, :, columns],
            b_send.at[step - 1, part],
            b_recv.at[step - 1, part],
            (e, target * 2 + c),
        )

    for step in range(1, y_count):
        project(step - 1)
        for part in range(column_parts):
            block_out[step - 1, :, columns_of(part)] = pair_sum(step - 1, part)
            block_copy(step, part).start()
    pl.when(jnp.logical_not(beside))(mix_across)
    project(y_count - 1)

    def arrive_back(j, carry):
        at = lax.rem(place_me + j, half_count)
        place = ret_in.at[at]
        remote(place, place, v_send.at[j], v_recv.at[at], (e, partner)).wait_recv()
        return carry

    lax.fori_loop(1, half_count, arrive_back, 0)
    wide = mix_ref[own_span, :]
    mix = jnp.where(s_me == 0, wide[:, :half_slots], wide[:, half_slots:])
    coarse = mix.astype(jnp.bfloat16)
    fine = (mix - coarse.astype(jnp.float32)).astype(jnp.bfloat16)
    returned = ret_in[...].reshape(half_slots, model)
    combined = jnp.dot(coarse, returned, preferred_element_type=jnp.float32)
    combined = combined + jnp.dot(fine, returned, preferred_element_type=jnp.float32)
    shared_sum[...] = shared_sum[...] + combined

    for part in range(column_parts):
        columns = columns_of(part)
        total = pair_sum(y_count - 1, part).astype(jnp.float32)
        for step in range(1, y_count):
            block_copy(step, part).wait()
            total = total + block_in[step - 1, :, columns].astype(jnp.float32)
        out_ref[:, columns] = total.astype(jnp.bfloat16)
    part_copy.wait()
    moe_ref[...] = (shared_sum[...] + part_in[...].astype(jnp.float32)).astype(jnp.bfloat16)

    def end_send(whiches, h, side, own):
        @pl.when(jnp.logical_not(own))
        def _():
            for which in whiches:
                first_copy(which, h, side).wait_send()

    each_send((0, 1, 2), end_send)

    for step in range(1, y_count):
        for part in range(2):
            far_copy(step, part).wait_send()

    def end_rest(source, carry):
        for far in range(y_count):
            spread(xbuf.at[t, source], source, far).wait_send()
        for far in range(1, y_count):
            relay(source, far, c).wait_send()

        for which in (1, 2):
            forward(which, source).wait_send()

        @pl.when(jnp.logical_not(jnp.logical_and(source == e, mine)))
        def _():
            for v in range(y_count):
                back_copy(source, v).wait_send()

        return carry

    lax.fori_loop(0, ep_count, end_rest, 0)

    def end_near(j, carry):
        dispatch(j).wait_send()
        pass_on(j).wait_send()
        give_back(j).wait_send()
        give_relay(j).wait_send()
        return carry

    lax.fori_loop(1, half_count, end_near, 0)
    cross_copy.wait_send()


def place_kernel(first_ref, second_ref, first_hbm, second_hbm, sem):
    copies = [
        pltpu.make_async_copy(first_ref, first_hbm, sem.at[0]),
        pltpu.make_async_copy(second_ref, second_hbm, sem.at[1]),
    ]
    for copy in copies:
        copy.start()
    for copy in copies:
        copy.wait()


def place_results(results):
    return pl.pallas_call(
        place_kernel,
        out_shape=tuple(jax.ShapeDtypeStruct(r.shape, r.dtype) for r in results),
        in_specs=[pl.BlockSpec(memory_space=pltpu.VMEM)] * 2,
        out_specs=[pl.BlockSpec(memory_space=pltpu.HBM)] * 2,
        scratch_shapes=[pltpu.SemaphoreType.DMA((2,))],
        compiler_params=pltpu.CompilerParams(vmem_limit_bytes=1024 * 1024),
        name="place",
    )(*results)


def mixer(
    tables,
    sequence,
    lambdas,
    head_gain,
    out_proj,
    moe_inputs,
    expert_weights,
    ep_count,
    tp_count,
    capacity,
):
    moe_input, moe_gain, routes, route_weights = moe_inputs
    head_count = lambdas.shape[0]
    half = sequence[0].shape[0] // 2
    width = sequence[0].shape[1] // head_count
    slots = ep_count * capacity
    batch_rows, model = moe_input.shape
    own_rows = batch_rows // tp_count
    top_count = routes.shape[1]
    hidden_width = expert_weights[0].shape[2]
    shared_width = expert_weights[3].shape[1]
    tokens = ep_count * 2 * half
    share = 2 * half // tp_count
    y_count = tp_count // 2
    dma = pltpu.SemaphoreType.DMA
    bf16 = jnp.bfloat16
    return pl.pallas_call(
        functools.partial(mixer_kernel, ep_count, tp_count),
        out_shape=(
            pltpu.VMEM((share, model), bf16),
            pltpu.VMEM((own_rows, model), bf16),
        ),
        in_specs=[pl.BlockSpec(memory_space=pltpu.HBM)] * 18,
        out_specs=[pl.BlockSpec(memory_space=pltpu.VMEM)] * 2,
        scratch_shapes=[
            pltpu.VMEM((1, head_count), jnp.float32),
            pltpu.VMEM(tables[0].shape, jnp.float32),
            pltpu.VMEM(tables[1].shape, jnp.float32),
            pltpu.VMEM(tables[0].shape[1:], jnp.float32),
            pltpu.VMEM(tables[0].shape[1:], jnp.float32),
            pltpu.VMEM((1, width), jnp.float32),
            pltpu.VMEM((1, model), jnp.float32),
            pltpu.VMEM((top_count, batch_rows), jnp.int32),
            pltpu.VMEM((top_count, batch_rows), jnp.float32),
            pltpu.VMEM((batch_rows, model), bf16),
            dma((8,)),
            pltpu.VMEM((batch_rows, model), bf16),
            pltpu.VMEM((slots, model), bf16),
            pltpu.VMEM((batch_rows, slots), jnp.float32),
            pltpu.VMEM((own_rows, model + slots), bf16),
            pltpu.VMEM((own_rows, model + slots), bf16),
            pltpu.VMEM((slots // 2, model), bf16),
            pltpu.VMEM((ep_count // 2, capacity, model), bf16),
            pltpu.VMEM((own_rows, model), bf16),
            pltpu.VMEM((own_rows, model), bf16),
            pltpu.VMEM((3,) + sequence[0].shape, bf16),
            pltpu.VMEM((3, head_count, 2, half, width), bf16),
            dma((3,)),
            pltpu.VMEM(out_proj.shape, bf16),
            pltpu.VMEM((model, hidden_width), bf16),
            pltpu.VMEM((model, hidden_width), bf16),
            pltpu.VMEM((hidden_width, model), bf16),
            pltpu.VMEM((model, shared_width), bf16),
            pltpu.VMEM((model, shared_width), bf16),
            pltpu.VMEM((shared_width, model), bf16),
            pltpu.VMEM((tp_count, ep_count, capacity, model), bf16),
            pltpu.VMEM((tp_count, slots // 2, hidden_width), bf16),
            pltpu.VMEM((y_count, own_rows + slots, model), bf16),
            pltpu.VMEM((y_count, own_rows + slots, model), bf16),
            pltpu.VMEM((y_count, own_rows + slots, model), bf16),
            pltpu.VMEM((max(1, y_count - 1), own_rows + slots, model), bf16),
            pltpu.VMEM((own_rows, model), jnp.float32),
            pltpu.VMEM((ep_count, capacity, model), bf16),
            pltpu.VMEM((ep_count // 2, capacity, model), bf16),
            dma((7,)),
            dma((ep_count,)),
            dma((ep_count,)),
            dma((2,)),
            dma((ep_count // 2,)),
            dma((ep_count,)),
            dma((ep_count // 2,)),
            dma((2,)),
            dma((ep_count, y_count)),
            dma((ep_count, y_count)),
            dma((ep_count, max(1, y_count - 1))),
            dma((ep_count, max(1, y_count - 1))),
            dma((2, 2)),
            dma((2, max(1, y_count - 1))),
            dma((2, max(1, y_count - 1))),
            dma((ep_count,)),
            dma((ep_count,)),
            pltpu.VMEM((ep_count, half, width), bf16),
            pltpu.VMEM((tokens, width), bf16),
            pltpu.VMEM((tokens, width), bf16),
            pltpu.VMEM((8, 128), jnp.float32),
            pltpu.VMEM((8, 128), jnp.float32),
            pltpu.VMEM((ep_count, y_count, share, width), bf16),
            pltpu.VMEM((head_count, y_count, 2, share, width), bf16),
            pltpu.VMEM((y_count, share, model), bf16),
            pltpu.VMEM((y_count, share, model), bf16),
            pltpu.VMEM((y_count, share, model), bf16),
            pltpu.VMEM((max(1, y_count - 1), share, model), bf16),
            pltpu.VMEM((max(1, y_count - 1), share, model), bf16),
            dma((3, head_count, 2)),
            dma((3, ep_count)),
            dma((3,)),
            dma((2, ep_count)),
            dma((2, ep_count)),
            dma((2,)),
            dma((ep_count, y_count)),
            dma((head_count, y_count, 2)),
            dma((y_count, 2)),
            dma((y_count, 2)),
            dma((max(1, y_count - 1), 2)),
            dma((max(1, y_count - 1), 2)),
        ],
        compiler_params=pltpu.CompilerParams(
            has_side_effects=True, vmem_limit_bytes=62000000, collective_id=0
        ),
        name="mixer",
    )(
        lambdas[None, :],
        *tables,
        head_gain[None, :],
        moe_gain[None, :],
        jnp.transpose(routes),
        jnp.transpose(route_weights),
        moe_input,
        *sequence,
        out_proj,
        *expert_weights,
    )


def local(
    queries,
    key_rows,
    value_rows,
    lambdas,
    head_gain,
    out_proj,
    moe_input,
    moe_gain,
    routes,
    route_weights,
    expert_gate,
    expert_up,
    expert_down,
    shared_gate,
    shared_up,
    shared_down,
):
    query_rows = queries.shape[0]
    head_count = lambdas.shape[0]
    head_dim = queries.shape[1] // (2 * head_count)
    tp_count = lax.axis_size("tp")
    ep_count = lax.axis_size("ep")
    tp_place = lax.axis_index("tp")
    ep_place = lax.axis_index("ep")
    positions = ep_place * query_rows + jnp.arange(query_rows, dtype=jnp.int32)
    batch_rows = moe_input.shape[0]
    top_count = routes.shape[1]
    own_rows = batch_rows // tp_count
    local_experts = expert_gate.shape[0]
    expert_count = local_experts * ep_count
    capacity = (2 * own_rows * top_count + expert_count - 1) // expert_count
    one_head_each = ep_count == 2 * head_count and tp_count % 2 == 0 and local_experts == 1 and ep_count % 4 == 0 and expert_count * capacity % 128 == 0
    if one_head_each:
        tables = rotation_tables(query_rows, ep_count, head_dim)
        sequence = (queries, key_rows, value_rows)
        weights = (expert_gate, expert_up, expert_down, shared_gate, shared_up, shared_down)
        return place_results(mixer(
            tables,
            sequence,
            lambdas,
            head_gain,
            out_proj,
            (moe_input, moe_gain, routes, route_weights),
            weights,
            ep_count,
            tp_count,
            capacity,
        ))
    else:
        rot_query = rotate(queries, positions, head_dim)
        rot_keys = rotate(key_rows, positions, head_dim)
        initial = (
            jnp.full((head_count, 2, query_rows), -1e30, jnp.float32),
            jnp.zeros((head_count, 2, query_rows), jnp.float32),
            jnp.zeros((head_count, 2, query_rows, 2 * head_dim), jnp.float32),
        )
        running_max, denominator, numerator = fold_keys(
            initial,
            (
                lax.all_gather(rot_keys, "ep", axis=0, tiled=True),
                lax.all_gather(value_rows, "ep", axis=0, tiled=True),
            ),
            rot_query,
            head_count,
            head_dim,
        )
        ratio = numerator / denominator[..., None]
        mixed_heads = ratio[:, 0] - lambdas[:, None, None] * ratio[:, 1]
        mean_square = jnp.mean(mixed_heads * mixed_heads, axis=-1, keepdims=True)
        normed_heads = (mixed_heads * lax.rsqrt(mean_square + head_eps) * head_gain).astype(
            jnp.bfloat16
        )
        head_out = jnp.transpose(normed_heads, (1, 0, 2)).reshape(query_rows, head_count * 2 * head_dim)
    normed = rms_rows(moe_input, moe_gain)
    shared_hidden = gated_hidden(normed, shared_gate, shared_up)
    own_routes = lax.dynamic_slice_in_dim(routes, tp_place * own_rows, own_rows, 0)
    own_weights = lax.dynamic_slice_in_dim(route_weights, tp_place * own_rows, own_rows, 0)
    own_source, own_filled, own_rank = slot_table(own_routes, expert_count, capacity)
    own_normed = lax.dynamic_slice_in_dim(normed, tp_place * own_rows, own_rows, 0)
    outgoing = fill_slots(own_normed, own_source, own_filled)
    arrived = lax.all_to_all(outgoing[:, None], "ep", split_axis=0, concat_axis=2, tiled=True)
    hidden = slot_hidden(lax.all_gather(arrived, "tp", axis=1, tiled=True), expert_gate, expert_up)
    slot_rows = local_experts * ep_count * capacity
    mixer_share = query_rows // tp_count
    expert_share = own_rows + slot_rows
    if not one_head_each:
        block_count = lax.axis_size("tp") * mixer_share // mixer_share
        product = jnp.dot(head_out, out_proj, preferred_element_type=jnp.float32)
        mixer_out = lax.psum_scatter(
            product.reshape(block_count, mixer_share, -1)
            .reshape(lax.axis_size("tp") * mixer_share, -1)
            .astype(jnp.bfloat16),
            "tp",
            scatter_dimension=0,
            tiled=True,
        )
    block_count = lax.axis_size("tp") * expert_share // expert_share
    shared_part = jnp.dot(shared_hidden, shared_down, preferred_element_type=jnp.float32).reshape(
        block_count, own_rows, -1
    )
    routed_part = jnp.einsum(
        "xnsf,xfd->nxsd", hidden, expert_down, preferred_element_type=jnp.float32
    )
    routed_part = routed_part.reshape(block_count, slot_rows, -1)
    expert_sum = lax.psum_scatter(
        jnp.concatenate([shared_part, routed_part], axis=1)
        .reshape(lax.axis_size("tp") * expert_share, -1)
        .astype(jnp.bfloat16),
        "tp",
        scatter_dimension=0,
        tiled=True,
    ).astype(jnp.float32)
    shared_sum = expert_sum[:own_rows]
    routed = (
        expert_sum[own_rows:].reshape(local_experts, ep_count * capacity, -1).astype(jnp.bfloat16)
    )
    returned = lax.all_to_all(routed, "ep", split_axis=1, concat_axis=0, tiled=True)
    flat_index = (own_routes * capacity + own_rank).reshape(-1)
    picked = jnp.take(returned.reshape(expert_count * capacity, -1), flat_index, axis=0).reshape(
        own_rows, top_count, -1
    )
    combined = shared_sum + jnp.sum(own_weights[..., None] * picked.astype(jnp.float32), axis=1)
    return (mixer_out, combined.astype(jnp.bfloat16))


def solution(mesh):
    in_specs = (
        P("ep", "tp"),
        P("ep", "tp"),
        P("ep", "tp"),
        P("tp"),
        P(),
        P("tp", None),
        P("ep", None),
        P(),
        P("ep", None),
        P("ep", None),
        P("ep", None, "tp"),
        P("ep", None, "tp"),
        P("ep", "tp", None),
        P(None, "tp"),
        P(None, "tp"),
        P("tp", None),
    )
    out_specs = (P(("ep", "tp"), None), P(("ep", "tp"), None))
    return jax.shard_map(local, mesh=mesh, in_specs=in_specs, out_specs=out_specs, check_vma=False)
```
